512 devices in a mesh: sp: 64 (over z, y), tp: 8 (over x, core).
Axes of the slice: x: 4, y: 8, z: 8, core: 2. Of those that a mesh axis runs over, the one named last changes fastest.
Arguments:
- tokens: bfloat16 [24576, 2048], P('sp', 'tp'), may hold values from -40 to 40
- mix_gain: float32 [2048], replicated, may hold values from 0.1 to 1.9
- w_pool_in: bfloat16 [2048, 1024], P(None, 'tp'), may hold values from -0.125 to 0.125
- w_qlat: bfloat16 [2048, 512], P(None, 'tp'), may hold values from -0.125 to 0.125
- w_kvlat: bfloat16 [2048, 512], P(None, 'tp'), may hold values from -0.125 to 0.125
- w_krope: bfloat16 [2048, 64], replicated, may hold values from -0.125 to 0.125
- q_gain: float32 [512], replicated, may hold values from 1 to 60
- kv_gain: float32 [512], replicated, may hold values from 0.1 to 1.9
- w_q_content: bfloat16 [512, 2048], P(None, 'tp'), may hold values from -0.25 to 0.25
- w_q_rotary: bfloat16 [512, 1024], P(None, 'tp'), may hold values from -0.25 to 0.25
- w_key: bfloat16 [512, 2048], P(None, 'tp'), may hold values from -0.25 to 0.25
- w_value: bfloat16 [512, 2048], P(None, 'tp'), may hold values from -0.25 to 0.25
- pool_mix: bfloat16 [8, 128, 128], replicated, may hold values from -0.5 to 0.5
- pool_scale: float32 [1024], replicated, may hold values from 0.1 to 1.9
- w_out_pool: bfloat16 [1024, 2048], P('tp'), may hold values from -0.109375 to 0.109375
- w_out_attn: bfloat16 [2048, 2048], P('tp'), may hold values from -0.25 to 0.25
Outputs:
- layer_out: bfloat16 [24576, 2048], P(('sp', 'tp'))
- log_total: float32 [24576, 16], P('sp', 'tp')
The draws below stay inside these ranges and needn't reach their ends.
All inputs are finite; a program needn't handle non-finite values.
Results may differ from the reference program's by a relative error of at most 0.015.
The reference program's roundings to bfloat16 on the way (of `scaled`, `weights`, `attended`, `pooled` and `pool_out`) count: a program that leaves them out, or rounds other values in their place, can miss the bound.
Values may be sent and summed in bfloat16 or wider, within the bound.
A program may use at most 64 MiB of HBM per device.

```python
import jax
import jax.numpy as jnp
from jax import lax

D = 2048
HEADS = 16
NOPE = 128
ROPE = 64
VDIM = 128
QLAT = 512
KVLAT = 512
GROUPS = 8
GROUP_DIM = 128
WIDEST = 16
SPAN = 16
TOK_DEV = 384
POOL = 1024
MIX = 3072
SEQ_LEN = 6144
SEQS = 4
TOKENS = 24576


def draw_tokens(key, part):
    base_key, column_key = jax.random.split(jax.random.fold_in(key, 11), 2)
    base = jnp.clip(jax.random.normal(base_key, (TOKENS, D), jnp.float32), -6.0, 6.0)
    ramp = jnp.arange(D, dtype=jnp.float32) / D
    column_scale = jnp.exp(jnp.log(4.0) * ramp + jax.random.uniform(column_key, (D,), jnp.float32, -0.5, 0.5))
    return jnp.clip(base * column_scale[None, :], -40.0, 40.0).astype(jnp.bfloat16)


def draw_q_gain(key, part):
    gain_key = jax.random.fold_in(key, 23)
    logs = jax.random.uniform(gain_key, (QLAT,), jnp.float32, 0.0, jnp.log(4.0))
    return jnp.exp(logs)


def steps_of(own_key, shape, cuts, least, high):
    gain, own = 1.0, jax.random.fold_in(own_key, 6)
    for axis_at, parts in cuts:
        heights = jnp.exp(jax.random.uniform(jax.random.fold_in(own, axis_at), (parts,), jnp.float32, least / len(cuts), high / len(cuts)))
        gain = gain * jnp.repeat(heights, shape[axis_at] // parts).reshape([-1 if axis == axis_at else 1 for axis in range(len(shape))])
    return gain


def normal_values(key, extent, spread, most, shards=(), kind=jnp.bfloat16):
    drawn = jax.random.normal(key, extent, jnp.float32) * spread
    if len(shards) > 0:
        drawn = steps_of(key, extent, shards, -0.22, 0.18) * drawn
    return jnp.clip(drawn, min=-most, max=most).astype(kind)


def setup_inputs(seed: int = 0) -> dict:
    keys = jax.random.split(jax.random.key(seed), 17)
    tokens = draw_tokens(jax.random.fold_in(keys[16], 71), 0)
    mix_gain = jnp.clip(1.0 + 0.18 * jax.random.normal(keys[1], (D,), jnp.float32), 0.1, 1.9)
    w_pool_in = normal_values(keys[2], (D, POOL), D ** -0.5, 0.125, ((1, 8),))
    w_qlat = normal_values(keys[3], (D, QLAT), D ** -0.5, 0.125, ((1, 8),))
    w_kvlat = normal_values(keys[4], (D, KVLAT), D ** -0.5, 0.125, ((1, 8),))
    w_krope = normal_values(keys[5], (D, ROPE), D ** -0.5, 0.125)
    q_gain = draw_q_gain(jax.random.fold_in(keys[16], 71), 0)
    kv_gain = jnp.clip(1.0 + 0.18 * jax.random.normal(keys[7], (KVLAT,), jnp.float32), 0.1, 1.9)
    w_q_content = normal_values(keys[8], (QLAT, HEADS * NOPE), QLAT ** -0.5, 0.25, ((1, 8),))
    w_q_rotary = normal_values(keys[9], (QLAT, HEADS * ROPE), QLAT ** -0.5, 0.25, ((1, 8),))
    w_key = normal_values(keys[10], (KVLAT, HEADS * NOPE), KVLAT ** -0.5, 0.25, ((1, 8),))
    w_value = normal_values(keys[11], (KVLAT, HEADS * VDIM), KVLAT ** -0.5, 0.25, ((1, 8),))
    pool_mix = normal_values(keys[12], (GROUPS, GROUP_DIM, GROUP_DIM), GROUP_DIM ** -0.5, 0.5)
    pool_scale = jnp.clip(1.0 + 0.18 * jax.random.normal(keys[13], (POOL,), jnp.float32), 0.1, 1.9)
    w_out_pool = normal_values(keys[14], (POOL, D), MIX ** -0.5, 0.109375, ((0, 8),))
    w_out_attn = normal_values(keys[15], (HEADS * VDIM, D), (HEADS * VDIM // 4) ** -0.5, 0.25, ((0, 8),))
    return {"tokens": tokens, "mix_gain": mix_gain, "w_pool_in": w_pool_in, "w_qlat": w_qlat, "w_kvlat": w_kvlat, "w_krope": w_krope, "q_gain": q_gain, "kv_gain": kv_gain, "w_q_content": w_q_content, "w_q_rotary": w_q_rotary, "w_key": w_key, "w_value": w_value, "pool_mix": pool_mix, "pool_scale": pool_scale, "w_out_pool": w_out_pool, "w_out_attn": w_out_attn}


eps_norm = 1e-06
rope_base = 10000.0
masked_score = -1e+30

def tables(positions, rotary_width):
    half_width = rotary_width // 2
    frequency = rope_base ** (-jnp.arange(half_width, dtype=jnp.float32) * 2.0 / rotary_width)
    angles = positions.astype(jnp.float32)[:, None] * frequency[None, :]
    return (jnp.cos(angles), jnp.sin(angles))

def rotate(vectors, cosine, sine_table):
    half_width = vectors.shape[-1] // 2
    first_half = vectors[..., :half_width]
    second_half = vectors[..., half_width:]
    return jnp.concatenate([first_half * cosine - second_half * sine_table, second_half * cosine + first_half * sine_table], axis=-1)

def latent_norm(latent, gain_vector):
    latent_values = latent.astype(jnp.float32)
    inverse = lax.rsqrt(lax.optimization_barrier(jnp.mean(latent_values * latent_values, axis=-1, keepdims=True)) + eps_norm)
    return (latent_values * inverse * gain_vector).astype(jnp.bfloat16)

def one_sequence(seq_tokens, mix_gain, w_pool_in, w_qlat, w_kvlat, w_krope, q_gain, kv_gain, w_q_content, w_q_rotary, w_key, w_value, pool_mix, pool_scale, w_out_pool, w_out_attn):
    length = seq_tokens.shape[0]
    positions = jnp.arange(length, dtype=jnp.int32)
    raw_values = seq_tokens.astype(jnp.float32)
    inverse_rms = lax.rsqrt(lax.optimization_barrier(jnp.mean(raw_values * raw_values, axis=1, keepdims=True)) + eps_norm)
    scaled = (raw_values * mix_gain).astype(jnp.bfloat16)

    def project(weight):
        return (jnp.dot(scaled, weight, preferred_element_type=jnp.float32) * inverse_rms).astype(jnp.bfloat16)
    pool_pre = project(w_pool_in)
    query_latent = project(w_qlat)
    kv_latent = project(w_kvlat)
    rotary_raw = project(w_krope)
    query_normed = latent_norm(query_latent, q_gain)
    key_normed = latent_norm(kv_latent, kv_gain)
    cosine, sine_table = tables(positions, ROPE)
    query_content = jnp.dot(query_normed, w_q_content, preferred_element_type=jnp.float32).astype(jnp.bfloat16).reshape(length, HEADS, NOPE)
    key_content = jnp.dot(key_normed, w_key, preferred_element_type=jnp.float32).astype(jnp.bfloat16).reshape(length, HEADS, NOPE)
    values = jnp.dot(key_normed, w_value, preferred_element_type=jnp.float32).astype(jnp.bfloat16).reshape(length, HEADS, VDIM)
    query_rotary = rotate(jnp.dot(query_normed, w_q_rotary, preferred_element_type=jnp.float32).reshape(length, HEADS, ROPE), cosine[:, None, :], sine_table[:, None, :]).astype(jnp.bfloat16)
    key_rotary = rotate(rotary_raw.astype(jnp.float32), cosine, sine_table).astype(jnp.bfloat16)
    score_scale = (NOPE + ROPE) ** (-0.5)
    key_content_wide = key_content.astype(jnp.float32)
    key_rotary_wide = key_rotary.astype(jnp.float32)
    values_wide = values.astype(jnp.float32)

    def query_block(block_index):
        row_start = block_index * TOK_DEV
        block_content = lax.dynamic_slice_in_dim(query_content, row_start, TOK_DEV, 0).astype(jnp.float32)
        block_rotary = lax.dynamic_slice_in_dim(query_rotary, row_start, TOK_DEV, 0).astype(jnp.float32)
        scores = jnp.einsum('qhd,khd->qhk', block_content, key_content_wide, precision=lax.Precision.HIGHEST)
        scores = scores + jnp.einsum('qhr,kr->qhk', block_rotary, key_rotary_wide, precision=lax.Precision.HIGHEST)
        query_positions = row_start + jnp.arange(TOK_DEV, dtype=jnp.int32)
        allowed = positions[None, None, :] <= query_positions[:, None, None]
        scores = jnp.where(allowed, scores * score_scale, masked_score)
        row_max = lax.optimization_barrier(jnp.max(scores, axis=-1))
        expo = jnp.exp(scores - row_max[..., None])
        row_total = lax.optimization_barrier(jnp.sum(expo, axis=-1))
        weights = lax.optimization_barrier(expo.astype(jnp.bfloat16))
        summed = jnp.einsum('qhk,khd->qhd', weights.astype(jnp.float32), values_wide, precision=lax.Precision.HIGHEST)
        attended = (summed / row_total[..., None]).astype(jnp.bfloat16).reshape(TOK_DEV, HEADS * VDIM)
        return (attended, row_max + jnp.log(row_total))
    attended, log_total = lax.map(query_block, jnp.arange(length // TOK_DEV))
    attended = attended.reshape(length, HEADS * VDIM)
    log_total = log_total.reshape(length, HEADS)
    pool_values = pool_pre.astype(jnp.float32)
    extended = jnp.concatenate([jnp.zeros((WIDEST - 1, POOL), jnp.float32), pool_values], axis=0)
    groups = jnp.arange(POOL, dtype=jnp.int32) // GROUP_DIM
    windows = jnp.left_shift(jnp.int32(2), groups % 4)
    window_sums = jnp.zeros((length, POOL), jnp.float32)
    for distance in range(WIDEST):
        window_sums = window_sums + jnp.where(distance < windows[None, :], extended[WIDEST - 1 - distance:WIDEST - 1 - distance + length], 0.0)
    counts = jnp.minimum(positions[:, None] + 1, windows[None, :]).astype(jnp.float32)
    pooled = lax.optimization_barrier((window_sums / counts - pool_values).astype(jnp.bfloat16))
    mixed_pool = jnp.einsum('sgc,gcd->sgd', pooled.astype(jnp.float32).reshape(length, GROUPS, GROUP_DIM), pool_mix.astype(jnp.float32), precision=lax.Precision.HIGHEST).reshape(length, POOL)
    pool_out = (mixed_pool * pool_scale).astype(jnp.bfloat16)
    layer_out = jnp.dot(pool_out, w_out_pool, preferred_element_type=jnp.float32)
    layer_out = layer_out + jnp.dot(attended, w_out_attn, preferred_element_type=jnp.float32)
    return (layer_out.astype(jnp.bfloat16), log_total)

def reference(tokens, mix_gain, w_pool_in, w_qlat, w_kvlat, w_krope, q_gain, kv_gain, w_q_content, w_q_rotary, w_key, w_value, pool_mix, pool_scale, w_out_pool, w_out_attn):
    sequences = tokens.reshape(SPAN, SEQS, TOK_DEV, D).transpose(1, 0, 2, 3).reshape(SEQS, SEQ_LEN, D)

    def per_sequence(seq_tokens):
        return one_sequence(seq_tokens, mix_gain, w_pool_in, w_qlat, w_kvlat, w_krope, q_gain, kv_gain, w_q_content, w_q_rotary, w_key, w_value, pool_mix, pool_scale, w_out_pool, w_out_attn)
    outputs, log_sums = lax.map(per_sequence, sequences)
    outputs = outputs.reshape(SEQS, SPAN, TOK_DEV, D).transpose(1, 0, 2, 3).reshape(TOKENS, D)
    log_sums = log_sums.reshape(SEQS, SPAN, TOK_DEV, HEADS).transpose(1, 0, 2, 3).reshape(TOKENS, HEADS)
    return (outputs, log_sums)
```

```python
import functools
import math

import jax
import jax.numpy as jnp
import numpy as np
from jax import lax
from jax.experimental import pallas as pl
from jax.experimental.pallas import tpu as pltpu
from jax.sharding import PartitionSpec as P

NOPE = 128
ROPE = 64
VDIM = 128
GROUP_DIM = 128
SPAN = 16
CHIPS = 4
PEERS = 8

eps_norm = 1e-06
rope_base = 10000.0
masked_score = -1e30

MESH = pl.DeviceIdType.MESH
F32 = jnp.float32
BF16 = jnp.bfloat16
NT = (((1,), (1,)), ((), ()))


def event_list(ring):
    up, down = ring // 2, ring - 1 - ring // 2
    timed = []
    for column in (0, 1):
        first = 0.0 if column == 0 else 4.7
        timed.append((first, (column, 0, 0)))
        base = 0.0 if column == 0 else 5.2
        for k in range(1, up + 1):
            timed.append((base + 2 * k, (column, 0, k)))
        for k in range(1, down + 1):
            timed.append((base + 2 * k + 0.5, (column, 1, k)))
    order = [e for _, e in sorted(timed)]
    at = {e: i for i, e in enumerate(order)}
    next_up, next_down = [], []
    for column, direction, k in order:
        next_up.append(at.get((column, 0, k + 1), 0) if k == 0 or direction == 0 else 0)
        next_down.append(at.get((column, 1, k + 1), 0) if k == 0 or direction == 1 else 0)
    shift = [k if direction == 1 else -k for _, direction, k in order]
    return order, next_up, next_down, shift, at[(1, 0, 0)]


def table(index, entries):
    out = jnp.int32(entries[0])
    for i, entry in enumerate(entries):
        if i > 0 and entry != entries[0]:
            out = jnp.where(index == i, jnp.int32(entry), out)
    return out


def remote(src, dst, send, recv, sp, tp):
    return pltpu.make_async_remote_copy(
        src_ref=src,
        dst_ref=dst,
        send_sem=send,
        recv_sem=recv,
        device_id={"sp": sp, "tp": tp},
        device_id_type=MESH,
    )


def dot(a, b, dims=(((1,), (0,)), ((), ()))):
    return lax.dot_general(a, b, dims, preferred_element_type=F32)


def kernel(
    sp_size,
    tokens,
    mix_gain,
    w_pool_in,
    w_qlat,
    w_kvlat,
    w_krope,
    q_gain,
    kv_gain,
    w_qc,
    w_qr,
    w_key,
    w_value,
    pool_mix,
    pool_scale,
    w_out_pool,
    w_out_attn,
    base_tab,
    rank_tab,
    out,
    logt,
    tok,
    wp,
    wl,
    wqc,
    wqr,
    wk,
    wv,
    mix,
    wo,
    tab,
    proj,
    pool_own,
    halo,
    pool_out,
    kvz,
    kvx,
    qbuf,
    qn,
    qs,
    wk2,
    wv2,
    gk,
    acc,
    stat,
    stat_in,
    stat_wide,
    osum,
    osum_in,
    part,
    rs,
    sem_local,
    sem_ws,
    sem_wr,
    sem_ts,
    sem_tr,
    sem_zs,
    sem_zr,
    sem_xs,
    sem_xr,
    sem_qs,
    sem_qr,
    sem_one_s,
    sem_one_r,
    sem_rs_s,
    sem_rs_r,
):
    sp = lax.axis_index("sp")
    tp = lax.axis_index("tp")
    count = sp_size // SPAN
    ring = SPAN // 2
    x, c = tp // 2, tp % 2
    rank = sp // count
    z, yh = rank // 2, rank % 2
    order, next_up, next_down, shift, y_event = event_list(ring)
    total_events = len(order)
    rows = tokens.shape[0]
    half = rows // 2
    width = tokens.shape[1]
    quarter = half // 4
    own_half = pl.multiple_of(half * c, half)
    other_half = pl.multiple_of(half * (1 - c), half)

    def tp_of(chip, core):
        return lax.rem(chip + CHIPS, CHIPS) * 2 + core

    partner = tp_of(x, 1 - c)
    right, left, across = tp_of(x + 1, c), tp_of(x - 1, c), tp_of(x + 2, c)
    ring_step = 2 * count
    above = lax.rem(sp + ring_step, sp_size)
    below = lax.rem(sp + sp_size - ring_step, sp_size)
    beside = sp + count * (1 - 2 * yh)
    halo_sp = lax.rem(sp + count * c, sp_size)
    halo_greet = lax.rem(sp + sp_size + count * (2 * c - 1), sp_size)

    core64 = pl.multiple_of(64 * c, 64)
    wl_q, wl_kv = core64, pl.multiple_of(128 + 64 * c, 64)
    wo_pool = pl.multiple_of(128 * c, 128)
    wo_attn = pl.multiple_of(256 + 256 * c, 256)
    shared = [
        (w_pool_in, lambda: wp.at[c]),
        (w_qlat, lambda: wl.at[pl.ds(wl_q, 64)]),
        (w_kvlat, lambda: wl.at[pl.ds(wl_kv, 64)]),
        (w_key, lambda: wk.at[c]),
        (w_value, lambda: wv.at[c]),
        (w_qc, lambda: wqc.at[c]),
        (w_qr, lambda: wqr.at[c]),
        (w_out_pool, lambda: wo.at[pl.ds(wo_pool, 128)]),
        (w_out_attn, lambda: wo.at[pl.ds(wo_attn, 256)]),
    ]
    n_shared = len(shared)
    local = [(src, dst()) for src, dst in shared]
    local += [
        (tokens.at[pl.ds(own_half, half)], tok.at[tp]),
        (w_krope, wl.at[pl.ds(256, 64)]),
        (w_krope, wl.at[pl.ds(320, 64)]),
        (base_tab, tab),
        (pool_mix.at[pl.ds(2 * x, 2)], mix),
    ]
    local = [pltpu.make_async_copy(s, d, sem_local.at[i]) for i, (s, d) in enumerate(local)]
    given = [
        remote(s, d(), sem_ws.at[i], sem_wr.at[i], sp, partner) for i, (s, d) in enumerate(shared)
    ]
    for i in [9, 10, 11, 0, 1, 2, 12, 3, 4, 5, 6, 13, 7, 8]:
        local[i].start()

    barrier = pltpu.get_barrier_semaphore()
    for i in range(1, PEERS):
        pl.semaphore_signal(
            barrier, inc=1, device_id={"sp": sp, "tp": lax.rem(tp + i, PEERS)}, device_id_type=MESH
        )
    for other_sp, other_tp in (
        (beside, tp),
        (above, tp),
        (below, tp),
        (halo_greet, partner),
    ):
        pl.semaphore_signal(
            barrier, inc=1, device_id={"sp": other_sp, "tp": other_tp}, device_id_type=MESH
        )
    pl.semaphore_wait(barrier, PEERS - 1 + 4)

    def token_copy(i):
        chip = x + (2, 2, 1, 1, 3, 3, 0)[i]
        core = (0, 1, 0, 1, 0, 1, 1 - c)[i]
        start = pl.multiple_of(half * core, half) if i == 6 else half * core
        return remote(
            tokens.at[pl.ds(start, half)],
            tok.at[tp],
            sem_ts.at[i],
            sem_tr.at[tp],
            sp,
            tp_of(chip, core),
        )

    token_copies = [token_copy(i) for i in range(7)]
    for i in (2, 4, 3, 5, 0, 1, 6):
        token_copies[i].start()
    for g in given:
        g.start()

    local[12].wait()
    lane = lax.broadcasted_iota(jnp.int32, (1, 128), 1)
    low_part = (lane % 64) < 32
    sign = jnp.where(low_part, -1.0, 1.0).astype(F32)
    cos_rank = rank_tab[0, pl.ds(rank, 1), :]
    sin_rank = rank_tab[1, pl.ds(rank, 1), :]
    cos_row, sin_row = tab[0], tab[1]
    tab[0] = cos_row * cos_rank - sin_row * sin_rank
    tab[1] = (sin_row * cos_rank + cos_row * sin_rank) * sign

    def rotate(v, cosine, signed_sine):
        swapped = jnp.where(low_part, pltpu.roll(v, 96, 1), pltpu.roll(v, 32, 1))
        return v * cosine + swapped * signed_sine

    for i in (0, 1, 2, 9, 10, 11):
        local[i].wait()
    for i in (0, 1, 2):
        given[i].wait_recv()

    def slab(j, squares):
        hop = j // 2
        chip = x + jnp.where(hop == 2, 3, jnp.where(hop == 3, 2, hop))
        source = tp_of(chip, (c + j) % 2)

        @pl.when(j > 0)
        def _():
            remote(tok.at[source], tok.at[source], sem_ts.at[0], sem_tr.at[source], sp, partner).wait_recv()

        at = pl.ds(pl.multiple_of(source * width, width), width)
        raw = tok[source].astype(F32)
        scaled = (raw * mix_gain[:, at]).astype(BF16)
        raw = raw * raw
        new = jnp.concatenate(
            [dot(scaled, wp[0, at, :]), dot(scaled, wp[1, at, :]), dot(scaled, wl[:, at], NT)],
            axis=1,
        )

        @pl.when(j == 0)
        def _():
            proj[...] = new

        @pl.when(j > 0)
        def _():
            proj[...] += new

        return squares + raw[:, :128] + raw[:, 128:]

    squares = lax.fori_loop(0, PEERS, slab, jnp.zeros((half, 128), F32))
    inverse = lax.rsqrt(jnp.sum(squares, axis=1, keepdims=True) / (width * PEERS) + eps_norm)
    done = (proj[...] * inverse).astype(BF16)
    own = kvz.at[rank]
    own[:half, :] = done[:, 384:512]
    qbuf[x] = done[:, 256:384]
    pool_own[...] = done[:, :256]
    rope = done[:, 512:640].astype(F32)
    rope = rotate(rope, tab[0, pl.ds(own_half, half), :], tab[1, pl.ds(own_half, half), :])
    rope = jnp.where(lane < 64, rope[: half // 2], rope[half // 2 :])
    own[2 * half :, :] = rope.astype(BF16)

    first = own.at[pl.ds(0, half)]
    to_left = remote(first, own.at[pl.ds(half, half)], sem_zs.at[0], sem_zr.at[0], sp, left)
    to_right = remote(first, kvx.at[rank, 1], sem_xs.at[0, 1], sem_xr.at[0, 1], sp, right)
    to_across = remote(first, kvx.at[rank, 0], sem_xs.at[0, 0], sem_xr.at[0, 0], sp, across)
    q_copies = [
        remote(qbuf.at[x], qbuf.at[x], sem_qs.at[i], sem_qr.at[i], sp, who)
        for i, who in enumerate((left, right, across))
    ]
    q_from = [lax.rem(x + 1, CHIPS), lax.rem(x + 3, CHIPS), lax.rem(x + 2, CHIPS)]
    to_left.start()
    to_right.start()
    to_across.start()
    for q_copy in q_copies:
        q_copy.start()
    halo_copy = remote(
        pool_own.at[pl.ds(half - 16, 16)],
        halo,
        sem_one_s.at[0],
        sem_one_r.at[0],
        halo_sp,
        partner,
    )
    halo_copy.start()

    for i in (3, 4, 5, 6):
        local[i].wait()
        given[i].wait_recv()
    for r in range(CHIPS):
        at = pl.ds(pl.multiple_of(lax.rem(x + r, CHIPS) * 128, 128), 128)
        gk[:, 128 * r : 128 * r + 128] = kv_gain[:, at]
        for core in (0, 1):
            wk2[128 * r : 128 * r + 128, 256 * core : 256 * core + 256] = wk[core, at, :]
            wv2[256 * core : 256 * core + 256, 128 * r : 128 * r + 128] = wv[core, at, :].T

    def block_copy(event, block, to):
        return remote(
            kvz.at[block], kvz.at[block], sem_zs.at[event], sem_zr.at[event], to, tp
        )

    to_left.wait_recv()
    block_copy(next_up[0], rank, above).start()
    if next_down[0]:
        block_copy(next_down[0], rank, below).start()
    block_copy(y_event, rank, beside).start()

    for i, piece in enumerate(q_from):
        remote(
            qbuf.at[piece], qbuf.at[piece], sem_qs.at[i], sem_qr.at[i], sp, left
        ).wait_recv()
    latent = [qbuf[i].astype(F32) for i in range(CHIPS)]
    squares = latent[0] * latent[0]
    for i in range(1, CHIPS):
        squares = squares + latent[i] * latent[i]
    inverse = lax.rsqrt(jnp.sum(squares, axis=1, keepdims=True) / (128 * CHIPS) + eps_norm)
    for i in range(CHIPS):
        gain = q_gain[:, 128 * i : 128 * i + 128]
        qn[pl.ds(own_half, half), 128 * i : 128 * i + 128] = (latent[i] * inverse * gain).astype(BF16)
    qn_copy = remote(
        qn.at[pl.ds(own_half, half)],
        qn.at[pl.ds(own_half, half)],
        sem_one_s.at[1],
        sem_one_r.at[1],
        sp,
        partner,
    )
    qn_copy.start()
    qn_other = qn.at[pl.ds(other_half, half)]
    remote(qn_other, qn_other, sem_one_s.at[1], sem_one_r.at[1], sp, partner).wait_recv()
    normed = qn[...]
    for core in (0, 1):
        content = dot(normed, wqc[core]).astype(BF16)
        rotary = rotate(dot(normed, wqr[core]), tab[0], tab[1])
        for h in (0, 1):
            qs[2 * core + h, :, :128] = content[:, 128 * h : 128 * h + 128]
            mine = (lane < 64) if h == 0 else (lane >= 64)
            qs[2 * core + h, :, 128:] = jnp.where(mine, rotary, 0.0).astype(BF16)

    stat[0:8, :] = jnp.full((8, rows), masked_score, F32)
    stat[8:16, :] = jnp.zeros((8, rows), F32)
    acc[...] = jnp.zeros_like(acc)
    to_log2 = (NOPE + ROPE) ** (-0.5) * math.log2(math.e)

    def rank_of(t):
        column = table(t, [e[0] for e in order])
        moved = table(t, shift)
        return lax.rem(z + moved + ring, ring) * 2 + lax.rem(yh + column, 2)

    def attend(block):
        piece = [
            kvz[block, :half, :].astype(F32),
            kvz[block, half : 2 * half, :].astype(F32),
            kvx[block, 0].astype(F32),
            kvx[block, 1].astype(F32),
        ]
        squares = piece[0] * piece[0]
        for i in range(1, CHIPS):
            squares = squares + piece[i] * piece[i]
        inverse = lax.rsqrt(jnp.sum(squares, axis=1, keepdims=True) / (128 * CHIPS) + eps_norm)
        normed = jnp.concatenate(
            [
                (piece[i] * inverse * gk[:, 128 * i : 128 * i + 128]).astype(BF16)
                for i in range(CHIPS)
            ],
            axis=1,
        )
        content = dot(normed, wk2[...]).astype(BF16)
        values = dot(wv2[...], normed, NT).astype(BF16)
        packed = kvz[block, 2 * half :, :].astype(F32)
        turned = pltpu.roll(packed, 64, 1)
        rotary = jnp.concatenate(
            [jnp.where(lane < 64, packed, turned), jnp.where(lane < 64, turned, packed)], axis=0
        ).astype(BF16)
        ahead = (block - rank) * rows + half * c
        key_at = lax.broadcasted_iota(jnp.int32, (half, rows), 0) + ahead
        allowed = key_at <= lax.broadcasted_iota(jnp.int32, (half, rows), 1)
        for h in range(4):
            keys = jnp.concatenate([content[:, 128 * h : 128 * h + 128], rotary], axis=1)
            scores = dot(keys, qs[h], NT) * to_log2
            scores = jnp.where(allowed, scores, masked_score)
            old = stat[h : h + 1, :]
            new = jnp.maximum(old, jnp.max(scores, axis=0, keepdims=True))
            factor = jnp.exp2(old - new)
            expo = jnp.exp2(scores - new)
            stat[h : h + 1, :] = new
            stat[8 + h : 9 + h, :] = stat[8 + h : 9 + h, :] * factor + jnp.sum(
                expo, axis=0, keepdims=True
            )
            acc[h] = acc[h] * factor + dot(values[128 * h : 128 * h + 128], expo.astype(BF16))

    def pooling():
        remote(halo, halo, sem_one_s.at[0], sem_one_r.at[0], sp, partner).wait_recv()
        local[13].wait()
        before = halo[...].astype(F32)
        before = jnp.where(jnp.logical_and(rank == 0, c == 0), 0.0, before)
        row = lax.broadcasted_iota(jnp.int32, (half, 128), 0) + (rank * rows + own_half)
        odd = x % 2
        for g in (0, 1):
            at = slice(128 * g, 128 * g + 128)
            values = pool_own[:, at].astype(F32)
            extended = jnp.concatenate([before[:, at], values], axis=0)
            sums = [extended]
            for step in (1, 2, 4, 8):
                sums.append(sums[-1] + pltpu.roll(sums[-1], step, 0))
            window = jnp.where(odd == 1, (8, 16)[g], (2, 4)[g])
            chosen = jnp.where(odd == 1, sums[3 + g][16:], sums[1 + g][16:])
            counts = jnp.minimum(row + 1, window).astype(F32)
            pooled = (chosen / counts - values).astype(BF16)
            scale = pool_scale[:, pl.ds(pl.multiple_of(256 * x + 128 * g, 128), 128)]
            pool_out[:, at] = (dot(pooled, mix[g]) * scale).astype(BF16)

    def visit(t, carry):
        @pl.when(t < total_events)
        def _():
            block = rank_of(t)
            block_copy(t, block, above).wait_recv()
            up = table(t, next_up)
            down = table(t, next_down)

            @pl.when(up > 0)
            def _():
                block_copy(up, block, above).start()

            @pl.when(down > 0)
            def _():
                block_copy(down, block, below).start()

            x_copy(t, block, 0).start()
            x_copy(t, block, 1).start()

        earlier = rank_of(t - 1)
        x_copy(t - 1, earlier, 0).wait_recv()
        x_copy(t - 1, earlier, 1).wait_recv()

        @pl.when(earlier <= rank)
        def _():
            attend(earlier)

        @pl.when(t == 2)
        def _():
            pooling()

        return carry

    def x_copy(t, block, which):
        piece = kvz.at[block, pl.ds(half if which == 0 else 0, half)]
        return remote(
            piece,
            kvx.at[block, which],
            sem_xs.at[t, which],
            sem_xr.at[t, which],
            sp,
            left if which == 0 else right,
        )

    lax.fori_loop(1, total_events + 1, visit, 0)

    for h in range(4):
        osum[:, 128 * h : 128 * h + 128] = acc[h].T
    stat_wide[0:16, :] = stat[...]
    stat_wide[16:128, :] = jnp.zeros((112, rows), F32)
    osum[:, 512:640] = stat_wide[...].T
    osum_copy = remote(
        osum.at[pl.ds(other_half, half)], osum_in, sem_one_s.at[2], sem_one_r.at[2], sp, partner
    )
    stat_copy = remote(stat, stat_in, sem_one_s.at[3], sem_one_r.at[3], sp, partner)
    osum_copy.start()
    stat_copy.start()
    for i in (7, 8):
        local[i].wait()
        given[i].wait_recv()
    stat_copy.wait_recv()
    most = jnp.maximum(stat[0:8, :], stat_in[0:8, :])
    sums = stat[8:16, :] * jnp.exp2(stat[0:8, :] - most) + stat_in[8:16, :] * jnp.exp2(
        stat_in[0:8, :] - most
    )
    logs = most * math.log(2.0) + jnp.log(sums)
    logt[...] = jnp.where(c == 0, logs[0:2, :], logs[2:4, :])
    osum_copy.wait_recv()
    own_rows = pl.ds(own_half, half)
    mixed = [pool_out[...]]
    own_stat, other_stat = osum[own_rows, 512:640], osum_in[:, 512:640]
    for h in range(4):
        at = slice(128 * h, 128 * h + 128)
        own_max, other_max = own_stat[:, h : h + 1], other_stat[:, h : h + 1]
        most = jnp.maximum(own_max, other_max)
        own_factor, other_factor = jnp.exp2(own_max - most), jnp.exp2(other_max - most)
        sums = (
            own_stat[:, 8 + h : 9 + h] * own_factor + other_stat[:, 8 + h : 9 + h] * other_factor
        )
        mixed.append(
            (
                (osum[own_rows, at] * own_factor + osum_in[:, at] * other_factor) / sums
            ).astype(BF16)
        )
    mixed = jnp.concatenate(mixed, axis=1)

    columns = wo.shape[1]
    chunks = sem_rs_s.shape[1]
    chunk = columns // chunks
    mine = x // 2 == c

    def part_copy(i, n):
        at = pl.ds(n * chunk, chunk)
        return remote(
            part.at[pl.ds(quarter * i, quarter), at],
            rs.at[x, :, at],
            sem_rs_s.at[i, n],
            sem_rs_r.at[x, n],
            sp,
            4 * c + i,
        )

    own_at = pl.multiple_of(quarter * lax.rem(tp, 4), quarter)

    def part_keep(n):
        at = pl.ds(n * chunk, chunk)
        return pltpu.make_async_copy(
            part.at[pl.ds(own_at, quarter), at], rs.at[x, :, at], sem_local.at[14 + n]
        )

    for n in range(chunks):
        at = slice(n * chunk, (n + 1) * chunk)
        part[:, at] = dot(mixed, wo[:, at]).astype(BF16)
        for i in range(4):

            @pl.when(4 * c + i != tp)
            def _():
                part_copy(i, n).start()

        @pl.when(mine)
        def _():
            part_keep(n).start()

    for n in range(chunks):
        at = slice(n * chunk, (n + 1) * chunk)
        for chip in range(CHIPS):

            @pl.when(jnp.logical_and(mine, x == chip))
            def _():
                part_keep(n).wait()

            @pl.when(jnp.logical_not(jnp.logical_and(mine, x == chip)))
            def _():
                ref = rs.at[chip, :, pl.ds(n * chunk, chunk)]
                remote(ref, ref, sem_rs_s.at[0, n], sem_rs_r.at[chip, n], sp, partner).wait_recv()

        out[:, at] = (
            rs[0, :, at].astype(F32)
            + rs[1, :, at].astype(F32)
            + rs[2, :, at].astype(F32)
            + rs[3, :, at].astype(F32)
        ).astype(BF16)

    for cp in token_copies + given + q_copies:
        cp.wait_send()
    to_left.wait_send()
    to_right.wait_send()
    to_across.wait_send()
    for cp in (halo_copy, qn_copy, osum_copy, stat_copy):
        cp.wait_send()

    def drain(t, carry):
        block_copy(t, 0, above).wait_send()
        x_copy(t, 0, 0).wait_send()
        x_copy(t, 0, 1).wait_send()
        return carry

    lax.fori_loop(1, total_events, drain, 0)
    for n in range(chunks):
        for i in range(4):

            @pl.when(4 * c + i != tp)
            def _():
                part_copy(i, n).wait_send()


def rotary_tables(rows, ranks):
    frequency = rope_base ** (-np.arange(ROPE // 2, dtype=np.float64) * 2.0 / ROPE)
    frequency = np.tile(frequency, 128 // (ROPE // 2))
    by_row = np.arange(rows)[:, None] * frequency[None, :]
    by_rank = (np.arange(ranks) * rows)[:, None] * frequency[None, :]
    return (
        np.stack([np.cos(by_row), np.sin(by_row)]).astype(np.float32),
        np.stack([np.cos(by_rank), np.sin(by_rank)]).astype(np.float32),
    )


def per_device(
    sp_size,
    tokens,
    mix_gain,
    w_pool_in,
    w_qlat,
    w_kvlat,
    w_krope,
    q_gain,
    kv_gain,
    w_q_content,
    w_q_rotary,
    w_key,
    w_value,
    pool_mix,
    pool_scale,
    w_out_pool,
    w_out_attn,
):
    rows, width = tokens.shape
    half = rows // 2
    columns = w_out_attn.shape[1]
    features = width * PEERS
    base_tab, rank_tab = rotary_tables(rows, SPAN)
    total_events = len(event_list(SPAN // 2)[0])
    chunks = 2
    anywhere = pl.BlockSpec(memory_space=pl.ANY)
    near = pl.BlockSpec(memory_space=pltpu.VMEM)
    dma = lambda *shape: pltpu.SemaphoreType.DMA(shape)
    vmem = pltpu.VMEM
    out, logt = pl.pallas_call(
        functools.partial(kernel, sp_size),
        out_shape=(
            jax.ShapeDtypeStruct((rows // PEERS, columns), BF16),
            jax.ShapeDtypeStruct((2, rows), F32),
        ),
        in_specs=[
            anywhere,
            near,
            anywhere,
            anywhere,
            anywhere,
            anywhere,
            near,
            near,
            anywhere,
            anywhere,
            anywhere,
            anywhere,
            anywhere,
            near,
            anywhere,
            anywhere,
            anywhere,
            near,
        ],
        out_specs=(near, near),
        scratch_shapes=[
            vmem((PEERS, half, width), BF16),
            vmem((2, features, 128), BF16),
            vmem((384, features), BF16),
            vmem((2, 512, 256), BF16),
            vmem((2, 512, 128), BF16),
            vmem((2, 512, 256), BF16),
            vmem((2, 512, 256), BF16),
            vmem((2, 128, 128), BF16),
            vmem((768, columns), BF16),
            vmem((2, rows, 128), F32),
            vmem((half, 640), F32),
            vmem((half, 256), BF16),
            vmem((16, 256), BF16),
            vmem((half, 256), BF16),
            vmem((SPAN, 2 * half + half // 2, 128), BF16),
            vmem((SPAN, 2, half, 128), BF16),
            vmem((CHIPS, half, 128), BF16),
            vmem((rows, 512), BF16),
            vmem((4, rows, 256), BF16),
            vmem((512, 512), BF16),
            vmem((512, 512), BF16),
            vmem((1, 512), F32),
            vmem((4, 128, rows), F32),
            vmem((16, rows), F32),
            vmem((16, rows), F32),
            vmem((128, rows), F32),
            vmem((rows, 640), F32),
            vmem((half, 640), F32),
            vmem((half, columns), BF16),
            vmem((CHIPS, rows // PEERS, columns), BF16),
            dma(14 + chunks),
            dma(9),
            dma(9),
            dma(7),
            dma(PEERS),
            dma(total_events),
            dma(total_events),
            dma(total_events, 2),
            dma(total_events, 2),
            dma(3),
            dma(3),
            dma(4),
            dma(4),
            dma(4, chunks),
            dma(CHIPS, chunks),
        ],
        compiler_params=pltpu.CompilerParams(
            collective_id=0, has_side_effects=True, vmem_limit_bytes=56 * 1024 * 1024
        ),
    )(
        tokens,
        mix_gain.reshape(1, -1),
        w_pool_in,
        w_qlat.T,
        w_kvlat.T,
        w_krope.T,
        q_gain.reshape(1, -1),
        kv_gain.reshape(1, -1),
        w_q_content,
        w_q_rotary,
        w_key,
        w_value,
        pool_mix,
        pool_scale.reshape(1, -1),
        w_out_pool,
        w_out_attn,
        jnp.asarray(base_tab),
        jnp.asarray(rank_tab),
    )
    return out, logt.T


def solution(mesh):
    in_specs = (
        P("sp", "tp"),
        P(),
        P(None, "tp"),
        P(None, "tp"),
        P(None, "tp"),
        P(),
        P(),
        P(),
        P(None, "tp"),
        P(None, "tp"),
        P(None, "tp"),
        P(None, "tp"),
        P(),
        P(),
        P("tp", None),
        P("tp", None),
    )
    out_specs = (P(("sp", "tp"), None), P("sp", "tp"))
    return jax.shard_map(
        functools.partial(per_device, mesh.shape["sp"]),
        mesh=mesh,
        in_specs=in_specs,
        out_specs=out_specs,
        check_vma=False,
    )
```

```python
import functools
import math

import jax
import jax.numpy as jnp
import numpy as np
from jax import lax
from jax.experimental import pallas as pl
from jax.experimental.pallas import tpu as pltpu
from jax.sharding import PartitionSpec as P

NOPE = 128
ROPE = 64
VDIM = 128
GROUP_DIM = 128
SPAN = 16
CHIPS = 4
PEERS = 8

eps_norm = 1e-06
rope_base = 10000.0
masked_score = -1e30

MESH = pl.DeviceIdType.MESH
F32 = jnp.float32
BF16 = jnp.bfloat16
NT = (((1,), (1,)), ((), ()))


def event_list(ring):
    far = ring // 2
    timed = []
    for column in (0, 1):
        first, pace = (0.0, 4.5) if column == 0 else (10.0, 4.7)
        timed.append((first, (column, 0, 0)))
        for k in range(1, far):
            timed.append((first + pace * k, (column, 0, k)))
            timed.append((first + pace * k + 0.1, (column, 1, k)))
        timed.append((first + pace * far, (column, 2, far)))
    order = [e for _, e in sorted(timed)]
    at = {e: i for i, e in enumerate(order)}
    follow = {}
    for going in (0, 1):
        for which in (0, 1):
            entries = []
            for column, direction, k in order:
                entry = 0
                if k == 0 or direction == going:
                    if k + 1 < far:
                        entry = at[(column, going, k + 1)]
                    elif which == going:
                        entry = at[(column, 2, far)]
                entries.append(entry)
            follow[going, which] = entries
    shift = [k if direction == 1 else -k for _, direction, k in order]
    return order, follow, shift, at[(1, 0, 0)]


def table(index, entries):
    out = jnp.int32(entries[0])
    for i, entry in enumerate(entries):
        if i > 0 and entry != entries[0]:
            out = jnp.where(index == i, jnp.int32(entry), out)
    return out


def remote(src, dst, send, recv, sp, tp):
    return pltpu.make_async_remote_copy(
        src_ref=src,
        dst_ref=dst,
        send_sem=send,
        recv_sem=recv,
        device_id={"sp": sp, "tp": tp},
        device_id_type=MESH,
    )


def dot(a, b, dims=(((1,), (0,)), ((), ()))):
    return lax.dot_general(a, b, dims, preferred_element_type=F32)


def kernel(
    sp_size,
    tokens,
    mix_gain,
    w_pool_in,
    w_qlat,
    w_kvlat,
    w_krope,
    q_gain,
    kv_gain,
    w_qc,
    w_qr,
    w_key,
    w_value,
    pool_mix,
    pool_scale,
    w_out_pool,
    w_out_attn,
    base_tab,
    rank_tab,
    out,
    logt,
    tok,
    wp,
    wl,
    wqc,
    wqr,
    wk,
    wv,
    mix,
    wo,
    tab,
    proj,
    pool_own,
    halo,
    pool_out,
    kvz,
    kvx,
    qbuf,
    qn,
    qs,
    wk2,
    wv2,
    gk,
    content_at,
    values_at,
    rotary_at,
    acc,
    stat,
    stat_in,
    most_at,
    sum_at,
    acc_in,
    part,
    rs,
    sem_local,
    sem_ws,
    sem_wr,
    sem_ts,
    sem_tr,
    sem_zs,
    sem_zr,
    sem_xs,
    sem_xr,
    sem_qs,
    sem_qr,
    sem_one_s,
    sem_one_r,
    sem_rs_s,
    sem_rs_r,
):
    sp = lax.axis_index("sp")
    tp = lax.axis_index("tp")
    count = sp_size // SPAN
    ring = SPAN // 2
    x, c = tp // 2, tp % 2
    rank = sp // count
    z, yh = rank // 2, rank % 2
    order, follow, shift, y_event = event_list(ring)
    total_events = len(order)
    rows = tokens.shape[0]
    half = rows // 2
    width = tokens.shape[1]
    quarter = half // 4
    own_half = pl.multiple_of(half * c, half)
    other_half = pl.multiple_of(half * (1 - c), half)

    def tp_of(chip, core):
        return lax.rem(chip + CHIPS, CHIPS) * 2 + core

    partner = tp_of(x, 1 - c)
    right, left, across = tp_of(x + 1, c), tp_of(x - 1, c), tp_of(x + 2, c)
    ring_step = 2 * count
    above = lax.rem(sp + ring_step, sp_size)
    below = lax.rem(sp + sp_size - ring_step, sp_size)
    beside = sp + count * (1 - 2 * yh)
    halo_sp = lax.rem(sp + count * c, sp_size)
    halo_greet = lax.rem(sp + sp_size + count * (2 * c - 1), sp_size)

    core64 = pl.multiple_of(64 * c, 64)
    wl_q, wl_kv = core64, pl.multiple_of(128 + 64 * c, 64)
    wo_pool = pl.multiple_of(128 * c, 128)
    wo_attn = pl.multiple_of(256 + 256 * c, 256)
    shared = [
        (w_pool_in, lambda: wp.at[c]),
        (w_qlat, lambda: wl.at[pl.ds(wl_q, 64)]),
        (w_kvlat, lambda: wl.at[pl.ds(wl_kv, 64)]),
        (w_key, lambda: wk.at[c]),
        (w_value, lambda: wv.at[c]),
        (w_qc, lambda: wqc.at[c]),
        (w_qr, lambda: wqr.at[c]),
        (w_out_pool, lambda: wo.at[pl.ds(wo_pool, 128)]),
        (w_out_attn, lambda: wo.at[pl.ds(wo_attn, 256)]),
    ]
    n_shared = len(shared)
    local = [(src, dst()) for src, dst in shared]
    local += [
        (tokens.at[pl.ds(own_half, half)], tok.at[tp]),
        (w_krope, wl.at[pl.ds(256, 64)]),
        (w_krope, wl.at[pl.ds(320, 64)]),
        (base_tab, tab),
        (pool_mix.at[pl.ds(2 * x, 2)], mix),
    ]
    local = [pltpu.make_async_copy(s, d, sem_local.at[i]) for i, (s, d) in enumerate(local)]
    given = [
        remote(s, d(), sem_ws.at[i], sem_wr.at[i], sp, partner) for i, (s, d) in enumerate(shared)
    ]
    for i in [9, 10, 11, 0, 1, 2, 12, 3, 4, 5, 6, 13, 7, 8]:
        local[i].start()

    barrier = pltpu.get_barrier_semaphore()
    for i in range(1, PEERS):
        pl.semaphore_signal(
            barrier, inc=1, device_id={"sp": sp, "tp": lax.rem(tp + i, PEERS)}, device_id_type=MESH
        )
    for other_sp, other_tp in (
        (beside, tp),
        (above, tp),
        (below, tp),
        (halo_greet, partner),
    ):
        pl.semaphore_signal(
            barrier, inc=1, device_id={"sp": other_sp, "tp": other_tp}, device_id_type=MESH
        )
    pl.semaphore_wait(barrier, PEERS - 1 + 4)

    def token_copy(i):
        chip = x + (2, 2, 1, 1, 3, 3, 0)[i]
        core = (0, 1, 0, 1, 0, 1, 1 - c)[i]
        start = pl.multiple_of(half * core, half) if i == 6 else half * core
        return remote(
            tokens.at[pl.ds(start, half)],
            tok.at[tp],
            sem_ts.at[i],
            sem_tr.at[tp],
            sp,
            tp_of(chip, core),
        )

    token_copies = [token_copy(i) for i in range(7)]
    for i in (2, 4, 3, 5, 0, 1, 6):
        token_copies[i].start()
    for g in given:
        g.start()

    local[12].wait()
    lane = lax.broadcasted_iota(jnp.int32, (1, 128), 1)
    low_part = (lane % 64) < 32
    sign = jnp.where(low_part, -1.0, 1.0).astype(F32)
    cos_rank = rank_tab[0, pl.ds(rank, 1), :]
    sin_rank = rank_tab[1, pl.ds(rank, 1), :]
    cos_row, sin_row = tab[0], tab[1]
    tab[0] = cos_row * cos_rank - sin_row * sin_rank
    tab[1] = (sin_row * cos_rank + cos_row * sin_rank) * sign

    def rotate(v, cosine, signed_sine):
        swapped = jnp.where(low_part, pltpu.roll(v, 96, 1), pltpu.roll(v, 32, 1))
        return v * cosine + swapped * signed_sine

    for i in (0, 1, 2, 9, 10, 11):
        local[i].wait()
    for i in (0, 1, 2):
        given[i].wait_recv()

    def slab(j, squares):
        hop = j // 2
        chip = x + jnp.where(hop == 2, 3, jnp.where(hop == 3, 2, hop))
        source = tp_of(chip, (c + j) % 2)

        @pl.when(j > 0)
        def _():
            remote(tok.at[source], tok.at[source], sem_ts.at[0], sem_tr.at[source], sp, partner).wait_recv()

        at = pl.ds(pl.multiple_of(source * width, width), width)
        raw = tok[source].astype(F32)
        scaled = (raw * mix_gain[:, at]).astype(BF16)
        raw = raw * raw
        new = jnp.concatenate(
            [dot(scaled, wp[0, at, :]), dot(scaled, wp[1, at, :]), dot(scaled, wl[:, at], NT)],
            axis=1,
        )

        @pl.when(j == 0)
        def _():
            proj[...] = new

        @pl.when(j > 0)
        def _():
            proj[...] += new

        return squares + raw[:, :128] + raw[:, 128:]

    squares = lax.fori_loop(0, PEERS, slab, jnp.zeros((half, 128), F32))
    inverse = lax.rsqrt(jnp.sum(squares, axis=1, keepdims=True) / (width * PEERS) + eps_norm)
    done = (proj[...] * inverse).astype(BF16)
    own = kvz.at[rank]
    own[:half, :] = done[:, 384:512]
    qbuf[x] = done[:, 256:384]
    pool_own[...] = done[:, :256]
    rope = done[:, 512:640].astype(F32)
    rope = rotate(rope, tab[0, pl.ds(own_half, half), :], tab[1, pl.ds(own_half, half), :])
    rope = jnp.where(lane < 64, rope[: half // 2], rope[half // 2 :])
    own[half : half + half // 2, :] = rope.astype(BF16)

    first_part = pl.ds(0, half + half // 2)
    second = pl.ds(half + half // 2, half)

    def block_copy(event, which, block, to):
        piece = kvz.at[block, first_part if which == 0 else second]
        return remote(piece, piece, sem_zs.at[event, which], sem_zr.at[event, which], to, tp)

    def start_own(which):
        for going, to in ((0, above), (1, below)):
            if follow[going, which][0]:
                block_copy(follow[going, which][0], which, rank, to).start()
        block_copy(y_event, which, rank, beside).start()

    first = own.at[pl.ds(0, half)]
    to_left = remote(first, own.at[second], sem_zs.at[0, 1], sem_zr.at[0, 1], sp, left)
    to_right = remote(first, kvx.at[rank, 1], sem_xs.at[0, 1], sem_xr.at[0, 1], sp, right)
    to_across = remote(first, kvx.at[rank, 0], sem_xs.at[0, 0], sem_xr.at[0, 0], sp, across)
    q_copies = [
        remote(qbuf.at[x], qbuf.at[x], sem_qs.at[i], sem_qr.at[i], sp, who)
        for i, who in enumerate((left, right, across))
    ]
    q_from = [lax.rem(x + 1, CHIPS), lax.rem(x + 3, CHIPS), lax.rem(x + 2, CHIPS)]
    to_left.start()
    start_own(0)
    to_right.start()
    to_across.start()
    for q_copy in q_copies:
        q_copy.start()
    halo_copy = remote(
        pool_own.at[pl.ds(half - 16, 16)],
        halo,
        sem_one_s.at[0],
        sem_one_r.at[0],
        halo_sp,
        partner,
    )
    halo_copy.start()

    for i in (3, 4, 5, 6):
        local[i].wait()
        given[i].wait_recv()
    for r in range(CHIPS):
        at = pl.ds(pl.multiple_of(lax.rem(x + r, CHIPS) * 128, 128), 128)
        gk[:, 128 * r : 128 * r + 128] = kv_gain[:, at]
        for core in (0, 1):
            wk2[128 * r : 128 * r + 128, 256 * core : 256 * core + 256] = wk[core, at, :]
            wv2[128 * r : 128 * r + 128, 256 * core : 256 * core + 256] = wv[core, at, :]

    def rank_of(t):
        column = table(t, [e[0] for e in order])
        moved = table(t, shift)
        return lax.rem(z + moved + ring, ring) * 2 + lax.rem(yh + column, 2)

    def x_copy(t, block, which):
        piece = kvz.at[block, second if which == 0 else pl.ds(0, half)]
        return remote(
            piece,
            kvx.at[block, which],
            sem_xs.at[t, which],
            sem_xr.at[t, which],
            sp,
            left if which == 0 else right,
        )

    def forward(t):
        block = rank_of(t)
        for which in (0, 1):
            block_copy(t, which, block, above).wait_recv()
            for going, to in ((0, above), (1, below)):
                entry = table(t, follow[going, which])

                @pl.when(entry > 0)
                def _():
                    block_copy(entry, which, block, to).start()

            x_copy(t, block, 1 - which).start()

    def arrived(t, block):
        x_copy(t, block, 0).wait_recv()
        x_copy(t, block, 1).wait_recv()

    to_left.wait_recv()
    start_own(1)

    forward(jnp.int32(1))
    forward(jnp.int32(2))
    for i, piece in enumerate(q_from):
        remote(
            qbuf.at[piece], qbuf.at[piece], sem_qs.at[i], sem_qr.at[i], sp, left
        ).wait_recv()
    latent = [qbuf[i].astype(F32) for i in range(CHIPS)]
    squares = latent[0] * latent[0]
    for i in range(1, CHIPS):
        squares = squares + latent[i] * latent[i]
    inverse = lax.rsqrt(jnp.sum(squares, axis=1, keepdims=True) / (128 * CHIPS) + eps_norm)
    for i in range(CHIPS):
        gain = q_gain[:, 128 * i : 128 * i + 128]
        qn[pl.ds(own_half, half), 128 * i : 128 * i + 128] = (latent[i] * inverse * gain).astype(BF16)
    qn_copy = remote(
        qn.at[pl.ds(own_half, half)],
        qn.at[pl.ds(own_half, half)],
        sem_one_s.at[1],
        sem_one_r.at[1],
        sp,
        partner,
    )
    qn_copy.start()
    qn_other = qn.at[pl.ds(other_half, half)]
    remote(qn_other, qn_other, sem_one_s.at[1], sem_one_r.at[1], sp, partner).wait_recv()
    normed = qn[...]
    to_log2 = (NOPE + ROPE) ** (-0.5) * math.log2(math.e)
    for core in (0, 1):
        content = (dot(normed, wqc[core]) * to_log2).astype(BF16)
        rotary = rotate(dot(normed, wqr[core]), tab[0], tab[1]) * to_log2
        for h in (0, 1):
            qs[2 * core + h, :, :128] = content[:, 128 * h : 128 * h + 128]
            turned = rotary if h == 0 else pltpu.roll(rotary, 64, 1)
            spare = jnp.where(lane == 64, 1.0, 0.0)
            qs[2 * core + h, :, 128:] = jnp.where(lane < 64, turned, spare).astype(BF16)

    most_at[...] = jnp.full(most_at.shape, masked_score, F32)
    sum_at[...] = jnp.zeros_like(sum_at)
    acc[...] = jnp.zeros_like(acc)

    def expand(blocks):
        parts = (pl.ds(0, half), second)
        piece = [
            jnp.concatenate([kvz[b, at, :].astype(F32) for b in blocks], axis=0) for at in parts
        ]
        piece += [
            jnp.concatenate([kvx[b, i].astype(F32) for b in blocks], axis=0) for i in (0, 1)
        ]
        squares = piece[0] * piece[0]
        for i in range(1, CHIPS):
            squares = squares + piece[i] * piece[i]
        inverse = lax.rsqrt(jnp.sum(squares, axis=1, keepdims=True) / (128 * CHIPS) + eps_norm)
        normed = jnp.concatenate(
            [
                (piece[i] * inverse * gk[:, 128 * i : 128 * i + 128]).astype(BF16)
                for i in range(CHIPS)
            ],
            axis=1,
        )
        content = dot(normed, wk2[...]).astype(BF16)
        values = dot(normed, wv2[...]).astype(BF16)
        rotary = []
        for b in blocks:
            packed = kvz[b, half : half + half // 2, :].astype(F32)
            hidden = jnp.where(b <= rank, 0.0, masked_score).astype(F32)
            spare = jnp.where(lane == 64, hidden, 0.0)
            rotary.append(jnp.where(lane < 64, packed, spare))
            rotary.append(jnp.where(lane < 64, pltpu.roll(packed, 64, 1), spare))
        rotary = jnp.concatenate(rotary, axis=0).astype(BF16)
        content_at[...] = content
        values_at[...] = values
        rotary_at[...] = rotary

    def attend_heads(heads, masked):
        if masked:
            column = lax.broadcasted_iota(jnp.int32, (rows, rows), 1)
            row = lax.broadcasted_iota(jnp.int32, (rows, rows), 0)
            allowed = jnp.logical_or(column >= half, column + half * c <= row)
        for h in heads:
            at = slice(128 * h, 128 * h + 128)
            keys = jnp.concatenate([content_at[:, at], rotary_at[...]], axis=1)
            scores = dot(qs[h], keys, NT)
            if masked:
                scores = jnp.where(allowed, scores, masked_score)
            old = most_at[h]
            new = jnp.maximum(old, jnp.max(scores, axis=1, keepdims=True))
            factor = jnp.exp2(old - new)
            expo = [jnp.exp2(scores[:, i : i + 128] - new) for i in range(0, rows, 128)]
            most_at[h] = new
            sum_at[h] = sum_at[h] * factor + sum(expo[1:], expo[0])
            expo = jnp.concatenate([e.astype(BF16) for e in expo], axis=1)
            acc[h] = acc[h] * factor + dot(expo, values_at[:, at])

    def pooling():
        remote(halo, halo, sem_one_s.at[0], sem_one_r.at[0], sp, partner).wait_recv()
        local[13].wait()
        before = halo[...].astype(F32)
        before = jnp.where(jnp.logical_and(rank == 0, c == 0), 0.0, before)
        row = lax.broadcasted_iota(jnp.int32, (half, 128), 0) + (rank * rows + own_half)
        odd = x % 2
        for g in (0, 1):
            at = slice(128 * g, 128 * g + 128)
            values = pool_own[:, at].astype(F32)
            extended = jnp.concatenate([before[:, at], values], axis=0)
            sums = [extended]
            for step in (1, 2, 4, 8):
                sums.append(sums[-1] + pltpu.roll(sums[-1], step, 0))
            window = jnp.where(odd == 1, (8, 16)[g], (2, 4)[g])
            chosen = jnp.where(odd == 1, sums[3 + g][16:], sums[1 + g][16:])
            counts = jnp.minimum(row + 1, window).astype(F32)
            pooled = (chosen / counts - values).astype(BF16)
            scale = pool_scale[:, pl.ds(pl.multiple_of(256 * x + 128 * g, 128), 128)]
            pool_out[:, at] = (dot(pooled, mix[g]) * scale).astype(BF16)

    forward(jnp.int32(3))
    arrived(0, rank)
    arrived(1, rank_of(jnp.int32(1)))
    expand([rank, rank_of(jnp.int32(1))])
    attend_heads((0, 1), True)
    forward(jnp.int32(4))
    attend_heads((2, 3), True)

    def visit(i, carry):
        @pl.when(2 * i + 3 < total_events)
        def _():
            forward(2 * i + 3)

        earlier = [rank_of(2 * i), rank_of(2 * i + 1)]
        seen = jnp.logical_or(earlier[0] < rank, earlier[1] < rank)
        arrived(2 * i, earlier[0])
        arrived(2 * i + 1, earlier[1])

        @pl.when(seen)
        def _():
            expand(earlier)
            attend_heads((0, 1), False)


        @pl.when(2 * i + 4 < total_events)
        def _():
            forward(2 * i + 4)


        @pl.when(seen)
        def _():
            attend_heads((2, 3), False)

        @pl.when(i == 1)
        def _():
            pooling()

        return carry

    lax.fori_loop(1, total_events // 2, visit, 0)

    acc_copy = remote(
        acc.at[:, pl.ds(other_half, half), :], acc_in, sem_one_s.at[2], sem_one_r.at[2], sp, partner
    )
    acc_copy.start()
    packed = jnp.zeros((rows, 128), F32)
    for h in range(4):
        packed = jnp.where(lane == h, most_at[h], packed)
        packed = jnp.where(lane == 8 + h, jnp.sum(sum_at[h], axis=1, keepdims=True), packed)
    stat[...] = packed
    stat_copy = remote(stat, stat_in, sem_one_s.at[3], sem_one_r.at[3], sp, partner)
    stat_copy.start()
    for i in (7, 8):
        local[i].wait()
        given[i].wait_recv()
    stat_copy.wait_recv()
    acc_copy.wait_recv()
    own_rows = pl.ds(own_half, half)
    mine_now, other_now = stat[...], stat_in[...]
    most = jnp.maximum(mine_now, other_now)
    sum_at[0] = jnp.exp2(mine_now - most)
    sum_at[1] = jnp.exp2(other_now - most)
    sums = pltpu.roll(mine_now, 120, 1) * sum_at[0] + pltpu.roll(other_now, 120, 1) * sum_at[1]
    sums = jnp.where(lane < 4, sums, 1.0)
    logs = jnp.where(lane < 4, most, 0.0) * math.log(2.0) + jnp.log(sums)
    logs = logs.T
    logt[...] = jnp.where(c == 0, logs[0:2, :], logs[2:4, :])
    most_at[0] = 1.0 / sums
    mixed = [pool_out[...]]
    for h in range(4):
        share = most_at[0, own_rows, h : h + 1]
        own_share = sum_at[0, own_rows, h : h + 1] * share
        other_share = sum_at[1, own_rows, h : h + 1] * share
        mixed.append((acc[h, own_rows, :] * own_share + acc_in[h] * other_share).astype(BF16))
    mixed = jnp.concatenate(mixed, axis=1)

    columns = wo.shape[1]
    chunks = sem_rs_s.shape[1]
    chunk = columns // chunks
    mine = x // 2 == c

    def part_copy(i, n):
        at = pl.ds(n * chunk, chunk)
        return remote(
            part.at[pl.ds(quarter * i, quarter), at],
            rs.at[x, :, at],
            sem_rs_s.at[i, n],
            sem_rs_r.at[x, n],
            sp,
            4 * c + i,
        )

    own_at = pl.multiple_of(quarter * lax.rem(tp, 4), quarter)

    def part_keep(n):
        at = pl.ds(n * chunk, chunk)
        return pltpu.make_async_copy(
            part.at[pl.ds(own_at, quarter), at], rs.at[x, :, at], sem_local.at[14 + n]
        )

    for n in range(chunks):
        at = slice(n * chunk, (n + 1) * chunk)
        part[:, at] = dot(mixed, wo[:, at]).astype(BF16)
        for i in range(4):

            @pl.when(4 * c + i != tp)
            def _():
                part_copy(i, n).start()

        @pl.when(mine)
        def _():
            part_keep(n).start()

    for n in range(chunks):
        at = slice(n * chunk, (n + 1) * chunk)
        for chip in range(CHIPS):

            @pl.when(jnp.logical_and(mine, x == chip))
            def _():
                part_keep(n).wait()

            @pl.when(jnp.logical_not(jnp.logical_and(mine, x == chip)))
            def _():
                ref = rs.at[chip, :, pl.ds(n * chunk, chunk)]
                remote(ref, ref, sem_rs_s.at[0, n], sem_rs_r.at[chip, n], sp, partner).wait_recv()

        out[:, at] = (
            rs[0, :, at].astype(F32)
            + rs[1, :, at].astype(F32)
            + rs[2, :, at].astype(F32)
            + rs[3, :, at].astype(F32)
        ).astype(BF16)

    for cp in token_copies + given + q_copies:
        cp.wait_send()
    to_left.wait_send()
    to_right.wait_send()
    to_across.wait_send()
    for cp in (halo_copy, qn_copy, acc_copy, stat_copy):
        cp.wait_send()

    def drain(t, carry):
        block_copy(t, 0, 0, above).wait_send()
        block_copy(t, 1, 0, above).wait_send()
        x_copy(t, 0, 0).wait_send()
        x_copy(t, 0, 1).wait_send()
        return carry

    lax.fori_loop(1, total_events, drain, 0)
    for n in range(chunks):
        for i in range(4):

            @pl.when(4 * c + i != tp)
            def _():
                part_copy(i, n).wait_send()


def rotary_tables(rows, ranks):
    frequency = rope_base ** (-np.arange(ROPE // 2, dtype=np.float64) * 2.0 / ROPE)
    frequency = np.tile(frequency, 128 // (ROPE // 2))
    by_row = np.arange(rows)[:, None] * frequency[None, :]
    by_rank = (np.arange(ranks) * rows)[:, None] * frequency[None, :]
    return (
        np.stack([np.cos(by_row), np.sin(by_row)]).astype(np.float32),
        np.stack([np.cos(by_rank), np.sin(by_rank)]).astype(np.float32),
    )


def per_device(
    sp_size,
    tokens,
    mix_gain,
    w_pool_in,
    w_qlat,
    w_kvlat,
    w_krope,
    q_gain,
    kv_gain,
    w_q_content,
    w_q_rotary,
    w_key,
    w_value,
    pool_mix,
    pool_scale,
    w_out_pool,
    w_out_attn,
):
    rows, width = tokens.shape
    half = rows // 2
    columns = w_out_attn.shape[1]
    features = width * PEERS
    base_tab, rank_tab = rotary_tables(rows, SPAN)
    total_events = len(event_list(SPAN // 2)[0])
    chunks = 2
    anywhere = pl.BlockSpec(memory_space=pl.ANY)
    near = pl.BlockSpec(memory_space=pltpu.VMEM)
    dma = lambda *shape: pltpu.SemaphoreType.DMA(shape)
    vmem = pltpu.VMEM
    out, logt = pl.pallas_call(
        functools.partial(kernel, sp_size),
        out_shape=(
            jax.ShapeDtypeStruct((rows // PEERS, columns), BF16),
            jax.ShapeDtypeStruct((2, rows), F32),
        ),
        in_specs=[
            anywhere,
            near,
            anywhere,
            anywhere,
            anywhere,
            anywhere,
            near,
            near,
            anywhere,
            anywhere,
            anywhere,
            anywhere,
            anywhere,
            near,
            anywhere,
            anywhere,
            anywhere,
            near,
        ],
        out_specs=(near, near),
        scratch_shapes=[
            vmem((PEERS, half, width), BF16),
            vmem((2, features, 128), BF16),
            vmem((384, features), BF16),
            vmem((2, 512, 256), BF16),
            vmem((2, 512, 128), BF16),
            vmem((2, 512, 256), BF16),
            vmem((2, 512, 256), BF16),
            vmem((2, 128, 128), BF16),
            vmem((768, columns), BF16),
            vmem((2, rows, 128), F32),
            vmem((half, 640), F32),
            vmem((half, 256), BF16),
            vmem((16, 256), BF16),
            vmem((half, 256), BF16),
            vmem((SPAN, 2 * half + half // 2, 128), BF16),
            vmem((SPAN, 2, half, 128), BF16),
            vmem((CHIPS, half, 128), BF16),
            vmem((rows, 512), BF16),
            vmem((4, rows, 256), BF16),
            vmem((512, 512), BF16),
            vmem((512, 512), BF16),
            vmem((1, 512), F32),
            vmem((rows, 512), BF16),
            vmem((rows, 512), BF16),
            vmem((rows, 128), BF16),
            vmem((4, rows, 128), F32),
            vmem((rows, 128), F32),
            vmem((rows, 128), F32),
            vmem((4, rows, 128), F32),
            vmem((4, rows, 128), F32),
            vmem((4, half, 128), F32),
            vmem((half, columns), BF16),
            vmem((CHIPS, rows // PEERS, columns), BF16),
            dma(14 + chunks),
            dma(9),
            dma(9),
            dma(7),
            dma(PEERS),
            dma(total_events, 2),
            dma(total_events, 2),
            dma(total_events, 2),
            dma(total_events, 2),
            dma(3),
            dma(3),
            dma(4),
            dma(4),
            dma(4, chunks),
            dma(CHIPS, chunks),
        ],
        compiler_params=pltpu.CompilerParams(
            collective_id=0, has_side_effects=True, vmem_limit_bytes=56 * 1024 * 1024
        ),
    )(
        tokens,
        mix_gain.reshape(1, -1),
        w_pool_in,
        w_qlat.T,
        w_kvlat.T,
        w_krope.T,
        q_gain.reshape(1, -1),
        kv_gain.reshape(1, -1),
        w_q_content,
        w_q_rotary,
        w_key,
        w_value,
        pool_mix,
        pool_scale.reshape(1, -1),
        w_out_pool,
        w_out_attn,
        jnp.asarray(base_tab),
        jnp.asarray(rank_tab),
    )
    return out, logt.T


def solution(mesh):
    in_specs = (
        P("sp", "tp"),
        P(),
        P(None, "tp"),
        P(None, "tp"),
        P(None, "tp"),
        P(),
        P(),
        P(),
        P(None, "tp"),
        P(None, "tp"),
        P(None, "tp"),
        P(None, "tp"),
        P(),
        P(),
        P("tp", None),
        P("tp", None),
    )
    out_specs = (P(("sp", "tp"), None), P("sp", "tp"))
    return jax.shard_map(
        functools.partial(per_device, mesh.shape["sp"]),
        mesh=mesh,
        in_specs=in_specs,
        out_specs=out_specs,
        check_vma=False,
    )
```

```python
import functools
import math

import jax
import jax.numpy as jnp
import numpy as np
from jax import lax
from jax.experimental import pallas as pl
from jax.experimental.pallas import tpu as pltpu
from jax.sharding import PartitionSpec as P

NOPE = 128
ROPE = 64
VDIM = 128
GROUP_DIM = 128
SPAN = 16
CHIPS = 4
PEERS = 8

eps_norm = 1e-06
rope_base = 10000.0
masked_score = -1e30

MESH = pl.DeviceIdType.MESH
F32 = jnp.float32
BF16 = jnp.bfloat16
NT = (((1,), (1,)), ((), ()))


def event_list(ring):
    far = ring // 2
    timed = []
    for column in (0, 1):
        first, pace = (0.0, 4.5) if column == 0 else (10.0, 4.7)
        timed.append((first, (column, 0, 0)))
        for k in range(1, far):
            timed.append((first + pace * k, (column, 0, k)))
            timed.append((first + pace * k + 0.1, (column, 1, k)))
        timed.append((first + pace * far, (column, 2, far)))
    order = [e for _, e in sorted(timed)]
    at = {e: i for i, e in enumerate(order)}
    follow = {}
    for going in (0, 1):
        for which in (0, 1):
            entries = []
            for column, direction, k in order:
                entry = 0
                if k == 0 or direction == going:
                    if k + 1 < far:
                        entry = at[(column, going, k + 1)]
                    elif which == going:
                        entry = at[(column, 2, far)]
                entries.append(entry)
            follow[going, which] = entries
    shift = [k if direction == 1 else -k for _, direction, k in order]
    limit = ([], [])
    parent = ([], [])
    for which in (0, 1):
        for column, direction, k in order:
            bound = (ring - k, far - 1 + which, far)[direction]
            limit[which].append(bound)
            before = at[(column, direction if direction < 2 else which, k - 1)] if k > 1 else 0
            parent[which].append(at[(column, 0, 0)] if k == 1 else before)
    next_limit = {
        key: [limit[key[1]][e] if e else 0 for e in entries] for key, entries in follow.items()
    }
    when = {e: t for t, e in timed}
    pairs = []
    for above in (False, True):
        group = [e for e in order if (e[1] == 1) == above]
        pairs += list(zip(group[::2], group[1::2]))
    pairs.sort(key=lambda pair: when[pair[1]])
    pairs = [[at[e] for e in pair] for pair in pairs]
    return order, follow, shift, at[(1, 0, 0)], limit, next_limit, parent, pairs


def table(index, entries):
    if isinstance(index, int):
        return entries[index]
    out = jnp.int32(entries[0])
    for i, entry in enumerate(entries):
        if i > 0 and entry != entries[0]:
            out = jnp.where(index == i, jnp.int32(entry), out)
    return out


def remote(src, dst, send, recv, sp, tp):
    return pltpu.make_async_remote_copy(
        src_ref=src,
        dst_ref=dst,
        send_sem=send,
        recv_sem=recv,
        device_id={"sp": sp, "tp": tp},
        device_id_type=MESH,
    )


def dot(a, b, dims=(((1,), (0,)), ((), ()))):
    return lax.dot_general(a, b, dims, preferred_element_type=F32)


def kernel(
    sp_size,
    tokens,
    mix_gain,
    w_pool_in,
    w_qlat,
    w_kvlat,
    w_krope,
    q_gain,
    kv_gain,
    w_qc,
    w_qr,
    w_key,
    w_value,
    pool_mix,
    pool_scale,
    w_out_pool,
    w_out_attn,
    base_tab,
    rank_tab,
    out,
    logt,
    tok,
    wp,
    wl,
    wqc,
    wqr,
    wk,
    wv,
    mix,
    wo,
    tab,
    proj,
    pool_own,
    halo,
    pool_out,
    kvz,
    kvx,
    qbuf,
    qn,
    qs,
    wk2,
    wv2,
    gk,
    content_at,
    values_at,
    rotary_at,
    acc,
    stat,
    stat_in,
    most_at,
    sum_at,
    acc_in,
    part,
    rs,
    sem_local,
    sem_ws,
    sem_wr,
    sem_ts,
    sem_tr,
    sem_zs,
    sem_zr,
    sem_xs,
    sem_xr,
    sem_qs,
    sem_qr,
    sem_one_s,
    sem_one_r,
    sem_rs_s,
    sem_rs_r,
):
    sp = lax.axis_index("sp")
    tp = lax.axis_index("tp")
    count = sp_size // SPAN
    ring = SPAN // 2
    x, c = tp // 2, tp % 2
    rank = sp // count
    z, yh = rank // 2, rank % 2
    order, follow, shift, y_event, limit, next_limit, parent, pairs = event_list(ring)
    total_events = len(order)
    rows = tokens.shape[0]
    half = rows // 2
    width = tokens.shape[1]
    quarter = half // 4
    own_half = pl.multiple_of(half * c, half)
    other_half = pl.multiple_of(half * (1 - c), half)

    def tp_of(chip, core):
        return lax.rem(chip + CHIPS, CHIPS) * 2 + core

    partner = tp_of(x, 1 - c)
    right, left, across = tp_of(x + 1, c), tp_of(x - 1, c), tp_of(x + 2, c)
    ring_step = 2 * count
    above = lax.rem(sp + ring_step, sp_size)
    below = lax.rem(sp + sp_size - ring_step, sp_size)
    beside = sp + count * (1 - 2 * yh)
    halo_sp = lax.rem(sp + count * c, sp_size)
    halo_greet = lax.rem(sp + sp_size + count * (2 * c - 1), sp_size)

    core64 = pl.multiple_of(64 * c, 64)
    wl_q, wl_kv = core64, pl.multiple_of(128 + 64 * c, 64)
    wo_pool = pl.multiple_of(128 * c, 128)
    wo_attn = pl.multiple_of(256 + 256 * c, 256)
    shared = [
        (w_pool_in, lambda: wp.at[c]),
        (w_qlat, lambda: wl.at[pl.ds(wl_q, 64)]),
        (w_kvlat, lambda: wl.at[pl.ds(wl_kv, 64)]),
        (w_key, lambda: wk.at[c]),
        (w_value, lambda: wv.at[c]),
        (w_qc, lambda: wqc.at[c]),
        (w_qr, lambda: wqr.at[c]),
        (w_out_pool, lambda: wo.at[pl.ds(wo_pool, 128)]),
        (w_out_attn, lambda: wo.at[pl.ds(wo_attn, 256)]),
    ]
    n_shared = len(shared)
    local = [(src, dst()) for src, dst in shared]
    local += [
        (tokens.at[pl.ds(own_half, half)], tok.at[tp]),
        (w_krope, wl.at[pl.ds(256, 64)]),
        (w_krope, wl.at[pl.ds(320, 64)]),
        (base_tab, tab),
        (pool_mix.at[pl.ds(2 * x, 2)], mix),
    ]
    local = [pltpu.make_async_copy(s, d, sem_local.at[i]) for i, (s, d) in enumerate(local)]
    given = [
        remote(s, d(), sem_ws.at[i], sem_wr.at[i], sp, partner) for i, (s, d) in enumerate(shared)
    ]
    for i in [9, 10, 11, 0, 1, 2, 12, 3, 4, 5, 6, 13, 7, 8]:
        local[i].start()

    barrier = pltpu.get_barrier_semaphore()
    for i in range(1, PEERS):
        pl.semaphore_signal(
            barrier, inc=1, device_id={"sp": sp, "tp": lax.rem(tp + i, PEERS)}, device_id_type=MESH
        )
    for other_sp, other_tp in (
        (beside, tp),
        (above, tp),
        (below, tp),
        (halo_greet, partner),
    ):
        pl.semaphore_signal(
            barrier, inc=1, device_id={"sp": other_sp, "tp": other_tp}, device_id_type=MESH
        )
    pl.semaphore_wait(barrier, PEERS - 1 + 4)

    def token_copy(i):
        chip = x + (2, 2, 1, 1, 3, 3, 0)[i]
        core = (0, 1, 0, 1, 0, 1, 1 - c)[i]
        start = pl.multiple_of(half * core, half) if i == 6 else half * core
        return remote(
            tokens.at[pl.ds(start, half)],
            tok.at[tp],
            sem_ts.at[i],
            sem_tr.at[tp],
            sp,
            tp_of(chip, core),
        )

    token_copies = [token_copy(i) for i in range(7)]
    for i in (2, 4, 3, 5, 0, 1, 6):
        token_copies[i].start()
    for g in given:
        g.start()

    local[12].wait()
    lane = lax.broadcasted_iota(jnp.int32, (1, 128), 1)
    low_part = (lane % 64) < 32
    sign = jnp.where(low_part, -1.0, 1.0).astype(F32)
    cos_rank = rank_tab[0, pl.ds(rank, 1), :]
    sin_rank = rank_tab[1, pl.ds(rank, 1), :]
    cos_row, sin_row = tab[0], tab[1]
    tab[0] = cos_row * cos_rank - sin_row * sin_rank
    tab[1] = (sin_row * cos_rank + cos_row * sin_rank) * sign

    def rotate(v, cosine, signed_sine):
        swapped = jnp.where(low_part, pltpu.roll(v, 96, 1), pltpu.roll(v, 32, 1))
        return v * cosine + swapped * signed_sine

    for i in (0, 1, 2, 9, 10, 11):
        local[i].wait()
    for i in (0, 1, 2):
        given[i].wait_recv()

    def slab(j, squares):
        hop = j // 2
        chip = x + jnp.where(hop == 2, 3, jnp.where(hop == 3, 2, hop))
        source = tp_of(chip, (c + j) % 2)

        @pl.when(j > 0)
        def _():
            remote(tok.at[source], tok.at[source], sem_ts.at[0], sem_tr.at[source], sp, partner).wait_recv()

        at = pl.ds(pl.multiple_of(source * width, width), width)
        raw = tok[source].astype(F32)
        scaled = (raw * mix_gain[:, at]).astype(BF16)
        raw = raw * raw
        new = jnp.concatenate(
            [dot(scaled, wp[0, at, :]), dot(scaled, wp[1, at, :]), dot(scaled, wl[:, at], NT)],
            axis=1,
        )

        @pl.when(j == 0)
        def _():
            proj[...] = new

        @pl.when(j > 0)
        def _():
            proj[...] += new

        return squares + raw[:, :128] + raw[:, 128:]

    squares = lax.fori_loop(0, PEERS, slab, jnp.zeros((half, 128), F32))
    inverse = lax.rsqrt(jnp.sum(squares, axis=1, keepdims=True) / (width * PEERS) + eps_norm)
    done = (proj[...] * inverse).astype(BF16)
    own = kvz.at[rank]
    own[:half, :] = done[:, 384:512]
    qbuf[x] = done[:, 256:384]
    pool_own[...] = done[:, :256]
    rope = done[:, 512:640].astype(F32)
    rope = rotate(rope, tab[0, pl.ds(own_half, half), :], tab[1, pl.ds(own_half, half), :])
    rope = jnp.where(lane < 64, rope[: half // 2], rope[half // 2 :])
    own[half : half + half // 2, :] = rope.astype(BF16)

    first_part = pl.ds(0, half + half // 2)
    second = pl.ds(half + half // 2, half)

    def block_copy(event, which, block, to):
        piece = kvz.at[block, first_part if which == 0 else second]
        return remote(piece, piece, sem_zs.at[event, which], sem_zr.at[event, which], to, tp)

    def start_own(which):
        for going, to in ((0, above), (1, below)):
            if follow[going, which][0]:

                @pl.when(z < next_limit[going, which][0])
                def _():
                    block_copy(follow[going, which][0], which, rank, to).start()

        block_copy(y_event, which, rank, beside).start()

    first = own.at[pl.ds(0, half)]
    to_left = remote(first, own.at[second], sem_zs.at[0, 1], sem_zr.at[0, 1], sp, left)
    to_right = remote(first, kvx.at[rank, 1], sem_xs.at[0, 1], sem_xr.at[0, 1], sp, right)
    to_across = remote(first, kvx.at[rank, 0], sem_xs.at[0, 0], sem_xr.at[0, 0], sp, across)
    q_copies = [
        remote(qbuf.at[x], qbuf.at[x], sem_qs.at[i], sem_qr.at[i], sp, who)
        for i, who in enumerate((left, right, across))
    ]
    q_from = [lax.rem(x + 1, CHIPS), lax.rem(x + 3, CHIPS), lax.rem(x + 2, CHIPS)]
    to_left.start()
    start_own(0)
    to_right.start()
    to_across.start()
    for q_copy in q_copies:
        q_copy.start()
    halo_copy = remote(
        pool_own.at[pl.ds(half - 16, 16)],
        halo,
        sem_one_s.at[0],
        sem_one_r.at[0],
        halo_sp,
        partner,
    )
    halo_copy.start()

    for i in (3, 4, 5, 6):
        local[i].wait()
        given[i].wait_recv()
    for r in range(CHIPS):
        at = pl.ds(pl.multiple_of(lax.rem(x + r, CHIPS) * 128, 128), 128)
        gk[:, 128 * r : 128 * r + 128] = kv_gain[:, at]
        for core in (0, 1):
            wk2[128 * r : 128 * r + 128, 256 * core : 256 * core + 256] = wk[core, at, :]
            wv2[128 * r : 128 * r + 128, 256 * core : 256 * core + 256] = wv[core, at, :]

    def rank_of(t):
        column = table(t, [e[0] for e in order])
        moved = table(t, shift)
        return lax.rem(z + moved + ring, ring) * 2 + lax.rem(yh + column, 2)

    def x_copy(t, block, which):
        piece = kvz.at[block, second if which == 0 else pl.ds(0, half)]
        return remote(
            piece,
            kvx.at[block, which],
            sem_xs.at[t, which],
            sem_xr.at[t, which],
            sp,
            left if which == 0 else right,
        )

    def forward(t, parts=(0, 1)):
        block = rank_of(t)
        place = block // 2
        for which in parts:

            @pl.when(place < table(t, limit[which]))
            def _():
                block_copy(t, which, block, above).wait_recv()

            for going, to in ((0, above), (1, below)):

                @pl.when(place < table(t, next_limit[going, which]))
                def _():
                    entry = table(t, follow[going, which])
                    block_copy(entry, which, block, to).start()

            @pl.when(block < rank)
            def _():
                x_copy(t, block, 1 - which).start()


    def arrived(t, block):
        @pl.when(block <= rank)
        def _():
            x_copy(t, block, 0).wait_recv()
            x_copy(t, block, 1).wait_recv()

    to_left.wait_recv()
    start_own(1)

    forward(jnp.int32(1))
    forward(jnp.int32(2))
    for i, piece in enumerate(q_from):
        remote(
            qbuf.at[piece], qbuf.at[piece], sem_qs.at[i], sem_qr.at[i], sp, left
        ).wait_recv()
    latent = [qbuf[i].astype(F32) for i in range(CHIPS)]
    squares = latent[0] * latent[0]
    for i in range(1, CHIPS):
        squares = squares + latent[i] * latent[i]
    inverse = lax.rsqrt(jnp.sum(squares, axis=1, keepdims=True) / (128 * CHIPS) + eps_norm)
    for i in range(CHIPS):
        gain = q_gain[:, 128 * i : 128 * i + 128]
        qn[pl.ds(own_half, half), 128 * i : 128 * i + 128] = (latent[i] * inverse * gain).astype(BF16)
    qn_copy = remote(
        qn.at[pl.ds(own_half, half)],
        qn.at[pl.ds(own_half, half)],
        sem_one_s.at[1],
        sem_one_r.at[1],
        sp,
        partner,
    )
    qn_copy.start()
    qn_other = qn.at[pl.ds(other_half, half)]
    remote(qn_other, qn_other, sem_one_s.at[1], sem_one_r.at[1], sp, partner).wait_recv()
    normed = qn[...]
    to_log2 = (NOPE + ROPE) ** (-0.5) * math.log2(math.e)
    for core in (0, 1):
        content = (dot(normed, wqc[core]) * to_log2).astype(BF16)
        rotary = rotate(dot(normed, wqr[core]), tab[0], tab[1]) * to_log2
        for h in (0, 1):
            qs[2 * core + h, :, :128] = content[:, 128 * h : 128 * h + 128]
            turned = rotary if h == 0 else pltpu.roll(rotary, 64, 1)
            spare = jnp.where(lane == 64, 1.0, 0.0)
            qs[2 * core + h, :, 128:] = jnp.where(lane < 64, turned, spare).astype(BF16)

    most_at[...] = jnp.full(most_at.shape, masked_score, F32)
    sum_at[...] = jnp.zeros_like(sum_at)
    acc[...] = jnp.zeros_like(acc)

    def expand(blocks):
        parts = (pl.ds(0, half), second)
        def shown(b, value):
            return jnp.where(b <= rank, value.astype(F32), 0.0)

        piece = [
            jnp.concatenate([shown(b, kvz[b, at, :]) for b in blocks], axis=0) for at in parts
        ]
        piece += [jnp.concatenate([shown(b, kvx[b, i]) for b in blocks], axis=0) for i in (0, 1)]
        squares = piece[0] * piece[0]
        for i in range(1, CHIPS):
            squares = squares + piece[i] * piece[i]
        inverse = lax.rsqrt(jnp.sum(squares, axis=1, keepdims=True) / (128 * CHIPS) + eps_norm)
        normed = jnp.concatenate(
            [
                (piece[i] * inverse * gk[:, 128 * i : 128 * i + 128]).astype(BF16)
                for i in range(CHIPS)
            ],
            axis=1,
        )
        content = dot(normed, wk2[...]).astype(BF16)
        values = dot(normed, wv2[...]).astype(BF16)
        rotary = []
        for b in blocks:
            packed = shown(b, kvz[b, half : half + half // 2, :])
            hidden = jnp.where(b <= rank, 0.0, masked_score).astype(F32)
            spare = jnp.where(lane == 64, hidden, 0.0)
            rotary.append(jnp.where(lane < 64, packed, spare))
            rotary.append(jnp.where(lane < 64, pltpu.roll(packed, 64, 1), spare))
        rotary = jnp.concatenate(rotary, axis=0).astype(BF16)
        content_at[...] = content
        values_at[...] = values
        rotary_at[...] = rotary

    def attend_heads(heads, masked):
        if masked:
            column = lax.broadcasted_iota(jnp.int32, (rows, rows), 1)
            row = lax.broadcasted_iota(jnp.int32, (rows, rows), 0)
            allowed = jnp.logical_or(column >= half, column + half * c <= row)
        for h in heads:
            at = slice(128 * h, 128 * h + 128)
            keys = jnp.concatenate([content_at[:, at], rotary_at[...]], axis=1)
            scores = dot(qs[h], keys, NT)
            if masked:
                scores = jnp.where(allowed, scores, masked_score)
            old = most_at[h]
            new = jnp.maximum(old, jnp.max(scores, axis=1, keepdims=True))
            factor = jnp.exp2(old - new)
            expo = [jnp.exp2(scores[:, i : i + 128] - new) for i in range(0, rows, 128)]
            most_at[h] = new
            sum_at[h] = sum_at[h] * factor + sum(expo[1:], expo[0])
            expo = jnp.concatenate([e.astype(BF16) for e in expo], axis=1)
            acc[h] = acc[h] * factor + dot(expo, values_at[:, at])

    def pooling():
        remote(halo, halo, sem_one_s.at[0], sem_one_r.at[0], sp, partner).wait_recv()
        local[13].wait()
        before = halo[...].astype(F32)
        before = jnp.where(jnp.logical_and(rank == 0, c == 0), 0.0, before)
        row = lax.broadcasted_iota(jnp.int32, (half, 128), 0) + (rank * rows + own_half)
        odd = x % 2
        for g in (0, 1):
            at = slice(128 * g, 128 * g + 128)
            values = pool_own[:, at].astype(F32)
            extended = jnp.concatenate([before[:, at], values], axis=0)
            sums = [extended]
            for step in (1, 2, 4, 8):
                sums.append(sums[-1] + pltpu.roll(sums[-1], step, 0))
            window = jnp.where(odd == 1, (8, 16)[g], (2, 4)[g])
            chosen = jnp.where(odd == 1, sums[3 + g][16:], sums[1 + g][16:])
            counts = jnp.minimum(row + 1, window).astype(F32)
            pooled = (chosen / counts - values).astype(BF16)
            scale = pool_scale[:, pl.ds(pl.multiple_of(256 * x + 128 * g, 128), 128)]
            pool_out[:, at] = (dot(pooled, mix[g]) * scale).astype(BF16)

    forward(jnp.int32(3))
    forward(jnp.int32(4))
    arrived(0, rank)
    arrived(1, rank_of(jnp.int32(1)))
    expand([rank, rank_of(jnp.int32(1))])
    attend_heads((0, 1), True)
    forward(jnp.int32(5))
    attend_heads((2, 3), True)

    def visit(i, carry):
        first, then = 2 * i + 4, 2 * i + 5
        events = [table(i, [pair[n] for pair in pairs]) for n in (0, 1)]
        earlier = [rank_of(t) for t in events]
        seen = jnp.logical_or(earlier[0] < rank, earlier[1] < rank)

        @pl.when(first < total_events)
        def _():
            forward(first)

        arrived(events[0], earlier[0])
        arrived(events[1], earlier[1])

        @pl.when(seen)
        def _():
            expand(earlier)
            attend_heads((0, 1), False)


        @pl.when(then < total_events)
        def _():
            forward(then)


        @pl.when(seen)
        def _():
            attend_heads((2, 3), False)

        @pl.when(i == 1)
        def _():
            pooling()

        return carry

    lax.fori_loop(1, total_events // 2, visit, 0)

    acc_copy = remote(
        acc.at[:, pl.ds(other_half, half), :], acc_in, sem_one_s.at[2], sem_one_r.at[2], sp, partner
    )
    acc_copy.start()
    packed = jnp.zeros((rows, 128), F32)
    for h in range(4):
        packed = jnp.where(lane == h, most_at[h], packed)
        packed = jnp.where(lane == 8 + h, jnp.sum(sum_at[h], axis=1, keepdims=True), packed)
    stat[...] = packed
    stat_copy = remote(stat, stat_in, sem_one_s.at[3], sem_one_r.at[3], sp, partner)
    stat_copy.start()
    for i in (7, 8):
        local[i].wait()
        given[i].wait_recv()
    stat_copy.wait_recv()
    acc_copy.wait_recv()
    own_rows = pl.ds(own_half, half)
    mine_now, other_now = stat[...], stat_in[...]
    most = jnp.maximum(mine_now, other_now)
    sum_at[0] = jnp.exp2(mine_now - most)
    sum_at[1] = jnp.exp2(other_now - most)
    sums = pltpu.roll(mine_now, 120, 1) * sum_at[0] + pltpu.roll(other_now, 120, 1) * sum_at[1]
    sums = jnp.where(lane < 4, sums, 1.0)
    logs = jnp.where(lane < 4, most, 0.0) * math.log(2.0) + jnp.log(sums)
    logs = logs.T
    logt[...] = jnp.where(c == 0, logs[0:2, :], logs[2:4, :])
    most_at[0] = 1.0 / sums
    mixed = [pool_out[...]]
    for h in range(4):
        share = most_at[0, own_rows, h : h + 1]
        own_share = sum_at[0, own_rows, h : h + 1] * share
        other_share = sum_at[1, own_rows, h : h + 1] * share
        mixed.append((acc[h, own_rows, :] * own_share + acc_in[h] * other_share).astype(BF16))
    mixed = jnp.concatenate(mixed, axis=1)

    columns = wo.shape[1]
    chunks = sem_rs_s.shape[1]
    chunk = columns // chunks
    mine = x // 2 == c

    def part_copy(i, n):
        at = pl.ds(n * chunk, chunk)
        return remote(
            part.at[pl.ds(quarter * i, quarter), at],
            rs.at[x, :, at],
            sem_rs_s.at[i, n],
            sem_rs_r.at[x, n],
            sp,
            4 * c + i,
        )

    own_at = pl.multiple_of(quarter * lax.rem(tp, 4), quarter)

    def part_keep(n):
        at = pl.ds(n * chunk, chunk)
        return pltpu.make_async_copy(
            part.at[pl.ds(own_at, quarter), at], rs.at[x, :, at], sem_local.at[14 + n]
        )

    for n in range(chunks):
        at = slice(n * chunk, (n + 1) * chunk)
        part[:, at] = dot(mixed, wo[:, at]).astype(BF16)
        for i in range(4):

            @pl.when(4 * c + i != tp)
            def _():
                part_copy(i, n).start()

        @pl.when(mine)
        def _():
            part_keep(n).start()

    for n in range(chunks):
        at = slice(n * chunk, (n + 1) * chunk)
        for chip in range(CHIPS):

            @pl.when(jnp.logical_and(mine, x == chip))
            def _():
                part_keep(n).wait()

            @pl.when(jnp.logical_not(jnp.logical_and(mine, x == chip)))
            def _():
                ref = rs.at[chip, :, pl.ds(n * chunk, chunk)]
                remote(ref, ref, sem_rs_s.at[0, n], sem_rs_r.at[chip, n], sp, partner).wait_recv()

        out[:, at] = (
            rs[0, :, at].astype(F32)
            + rs[1, :, at].astype(F32)
            + rs[2, :, at].astype(F32)
            + rs[3, :, at].astype(F32)
        ).astype(BF16)

    for cp in token_copies + given + q_copies:
        cp.wait_send()
    to_left.wait_send()
    to_right.wait_send()
    to_across.wait_send()
    for cp in (halo_copy, qn_copy, acc_copy, stat_copy):
        cp.wait_send()

    for t in range(1, total_events):
        for which in (0, 1):
            held = lax.rem(z + shift[parent[which][t]] + ring, ring)

            @pl.when(held < limit[which][t])
            def _():
                block_copy(t, which, 0, above).wait_send()

        @pl.when(rank_of(t) < rank)
        def _():
            x_copy(t, 0, 0).wait_send()
            x_copy(t, 0, 1).wait_send()

    for n in range(chunks):
        for i in range(4):

            @pl.when(4 * c + i != tp)
            def _():
                part_copy(i, n).wait_send()


def rotary_tables(rows, ranks):
    frequency = rope_base ** (-np.arange(ROPE // 2, dtype=np.float64) * 2.0 / ROPE)
    frequency = np.tile(frequency, 128 // (ROPE // 2))
    by_row = np.arange(rows)[:, None] * frequency[None, :]
    by_rank = (np.arange(ranks) * rows)[:, None] * frequency[None, :]
    return (
        np.stack([np.cos(by_row), np.sin(by_row)]).astype(np.float32),
        np.stack([np.cos(by_rank), np.sin(by_rank)]).astype(np.float32),
    )


def per_device(
    sp_size,
    tokens,
    mix_gain,
    w_pool_in,
    w_qlat,
    w_kvlat,
    w_krope,
    q_gain,
    kv_gain,
    w_q_content,
    w_q_rotary,
    w_key,
    w_value,
    pool_mix,
    pool_scale,
    w_out_pool,
    w_out_attn,
):
    rows, width = tokens.shape
    half = rows // 2
    columns = w_out_attn.shape[1]
    features = width * PEERS
    base_tab, rank_tab = rotary_tables(rows, SPAN)
    total_events = len(event_list(SPAN // 2)[0])
    chunks = 2
    anywhere = pl.BlockSpec(memory_space=pl.ANY)
    near = pl.BlockSpec(memory_space=pltpu.VMEM)
    dma = lambda *shape: pltpu.SemaphoreType.DMA(shape)
    vmem = pltpu.VMEM
    out, logt = pl.pallas_call(
        functools.partial(kernel, sp_size),
        out_shape=(
            jax.ShapeDtypeStruct((rows // PEERS, columns), BF16),
            jax.ShapeDtypeStruct((2, rows), F32),
        ),
        in_specs=[
            anywhere,
            near,
            anywhere,
            anywhere,
            anywhere,
            anywhere,
            near,
            near,
            anywhere,
            anywhere,
            anywhere,
            anywhere,
            anywhere,
            near,
            anywhere,
            anywhere,
            anywhere,
            near,
        ],
        out_specs=(near, near),
        scratch_shapes=[
            vmem((PEERS, half, width), BF16),
            vmem((2, features, 128), BF16),
            vmem((384, features), BF16),
            vmem((2, 512, 256), BF16),
            vmem((2, 512, 128), BF16),
            vmem((2, 512, 256), BF16),
            vmem((2, 512, 256), BF16),
            vmem((2, 128, 128), BF16),
            vmem((768, columns), BF16),
            vmem((2, rows, 128), F32),
            vmem((half, 640), F32),
            vmem((half, 256), BF16),
            vmem((16, 256), BF16),
            vmem((half, 256), BF16),
            vmem((SPAN, 2 * half + half // 2, 128), BF16),
            vmem((SPAN, 2, half, 128), BF16),
            vmem((CHIPS, half, 128), BF16),
            vmem((rows, 512), BF16),
            vmem((4, rows, 256), BF16),
            vmem((512, 512), BF16),
            vmem((512, 512), BF16),
            vmem((1, 512), F32),
            vmem((rows, 512), BF16),
            vmem((rows, 512), BF16),
            vmem((rows, 128), BF16),
            vmem((4, rows, 128), F32),
            vmem((rows, 128), F32),
            vmem((rows, 128), F32),
            vmem((4, rows, 128), F32),
            vmem((4, rows, 128), F32),
            vmem((4, half, 128), F32),
            vmem((half, columns), BF16),
            vmem((CHIPS, rows // PEERS, columns), BF16),
            dma(14 + chunks),
            dma(9),
            dma(9),
            dma(7),
            dma(PEERS),
            dma(total_events, 2),
            dma(total_events, 2),
            dma(total_events, 2),
            dma(total_events, 2),
            dma(3),
            dma(3),
            dma(4),
            dma(4),
            dma(4, chunks),
            dma(CHIPS, chunks),
        ],
        compiler_params=pltpu.CompilerParams(
            collective_id=0, has_side_effects=True, vmem_limit_bytes=56 * 1024 * 1024
        ),
    )(
        tokens,
        mix_gain.reshape(1, -1),
        w_pool_in,
        w_qlat.T,
        w_kvlat.T,
        w_krope.T,
        q_gain.reshape(1, -1),
        kv_gain.reshape(1, -1),
        w_q_content,
        w_q_rotary,
        w_key,
        w_value,
        pool_mix,
        pool_scale.reshape(1, -1),
        w_out_pool,
        w_out_attn,
        jnp.asarray(base_tab),
        jnp.asarray(rank_tab),
    )
    return out, logt.T


def solution(mesh):
    in_specs = (
        P("sp", "tp"),
        P(),
        P(None, "tp"),
        P(None, "tp"),
        P(None, "tp"),
        P(),
        P(),
        P(),
        P(None, "tp"),
        P(None, "tp"),
        P(None, "tp"),
        P(None, "tp"),
        P(),
        P(),
        P("tp", None),
        P("tp", None),
    )
    out_specs = (P(("sp", "tp"), None), P("sp", "tp"))
    return jax.shard_map(
        functools.partial(per_device, mesh.shape["sp"]),
        mesh=mesh,
        in_specs=in_specs,
        out_specs=out_specs,
        check_vma=False,
    )
```

```python
import functools
import math

import jax
import jax.numpy as jnp
import numpy as np
from jax import lax
from jax.experimental import pallas as pl
from jax.experimental.pallas import tpu as pltpu
from jax.sharding import PartitionSpec as P

NOPE = 128
ROPE = 64
VDIM = 128
GROUP_DIM = 128
SPAN = 16
CHIPS = 4
PEERS = 8

eps_norm = 1e-06
rope_base = 10000.0
masked_score = -1e30

MESH = pl.DeviceIdType.MESH
F32 = jnp.float32
BF16 = jnp.bfloat16
NT = (((1,), (1,)), ((), ()))


def event_list(ring):
    far = ring // 2
    timed = []
    for column in (0, 1):
        first, pace = (0.0, 4.5) if column == 0 else (10.0, 4.7)
        timed.append((first, (column, 0, 0)))
        for k in range(1, far):
            timed.append((first + pace * k, (column, 0, k)))
            timed.append((first + pace * k + 0.1, (column, 1, k)))
        timed.append((first + pace * far, (column, 2, far)))
    order = [e for _, e in sorted(timed)]
    at = {e: i for i, e in enumerate(order)}
    follow = {}
    for going in (0, 1):
        for which in (0, 1):
            entries = []
            for column, direction, k in order:
                entry = 0
                if k == 0 or direction == going:
                    if k + 1 < far:
                        entry = at[(column, going, k + 1)]
                    elif going == 0 or which == 1:
                        entry = at[(column, 2, far)]
                entries.append(entry)
            follow[going, which] = entries
    shift = [k if direction == 1 else -k for _, direction, k in order]
    limit = ([], [])
    for which in (0, 1):
        for column, direction, k in order:
            bound = (ring - k, far - 1 + which, far)[direction]
            limit[which].append(bound)
    next_limit, next_least = {}, {}
    for (going, which), entries in follow.items():
        to_far = [e > 0 and order[e][1] == 2 and which == 1 for e in entries]
        next_limit[going, which] = [
            (far - 1 if f and going == 0 else limit[which][e]) if e else 0
            for e, f in zip(entries, to_far)
        ]
        next_least[going, which] = [far - 1 if f and going == 1 else 0 for f in to_far]
    when = {e: t for t, e in timed}
    pairs = []
    for above in (False, True):
        group = [e for e in order if (e[1] == 1) == above]
        pairs += list(zip(group[::2], group[1::2]))
    pairs.sort(key=lambda pair: when[pair[1]])
    pairs = [[at[e] for e in pair] for pair in pairs]
    return order, follow, shift, at[(1, 0, 0)], limit, next_limit, next_least, pairs


def table(index, entries):
    if isinstance(index, int):
        return jnp.int32(entries[index])
    out = jnp.int32(entries[0])
    for i, entry in enumerate(entries):
        if i > 0 and entry != entries[0]:
            out = jnp.where(index == i, jnp.int32(entry), out)
    return out


def remote(src, dst, send, recv, sp, tp):
    return pltpu.make_async_remote_copy(
        src_ref=src,
        dst_ref=dst,
        send_sem=send,
        recv_sem=recv,
        device_id={"sp": sp, "tp": tp},
        device_id_type=MESH,
    )


def dot(a, b, dims=(((1,), (0,)), ((), ()))):
    return lax.dot_general(a, b, dims, preferred_element_type=F32)


def kernel(
    sp_size,
    tokens,
    mix_gain_in,
    w_pool_in,
    w_qlat,
    w_kvlat,
    w_krope,
    q_gain_in,
    kv_gain_in,
    w_qc,
    w_qr,
    w_key,
    w_value,
    pool_mix,
    pool_scale_in,
    w_out_pool,
    w_out_attn,
    base_tab,
    rank_tab_in,
    out,
    logt,
    mix_gain,
    q_gain,
    kv_gain,
    pool_scale,
    rank_tab,
    tok,
    wp,
    wl,
    wqc,
    wqr,
    wk,
    wv,
    mix,
    wo,
    tab,
    proj,
    pool_own,
    halo,
    pool_out,
    kvz,
    kvx,
    qbuf,
    qn,
    qs,
    wk2,
    wv2,
    gk,
    content_at,
    values_at,
    rotary_at,
    acc,
    stat,
    stat_in,
    most_at,
    sum_at,
    acc_in,
    part,
    rs,
    sem_local,
    sem_ws,
    sem_wr,
    sem_ts,
    sem_tr,
    sem_zs,
    sem_zr,
    sem_xs,
    sem_xr,
    sem_qs,
    sem_qr,
    sem_one_s,
    sem_one_r,
    sem_rs_s,
    sem_rs_r,
    sem_relay_s,
    sem_ready,
):
    sp = lax.axis_index("sp")
    tp = lax.axis_index("tp")
    count = sp_size // SPAN
    ring = SPAN // 2
    x, c = tp // 2, tp % 2
    rank = sp // count
    z, yh = rank // 2, rank % 2
    order, follow, shift, y_event, limit, next_limit, next_least, pairs = event_list(ring)

    def goes(t, going, which, place):
        least = table(t, next_least[going, which])
        return jnp.logical_and(place >= least, place < table(t, next_limit[going, which]))

    total_events = len(order)
    rows = tokens.shape[0]
    half = rows // 2
    width = tokens.shape[1]
    quarter = half // 4
    own_half = pl.multiple_of(half * c, half)
    other_half = pl.multiple_of(half * (1 - c), half)

    def tp_of(chip, core):
        return lax.rem(chip + CHIPS, CHIPS) * 2 + core

    partner = tp_of(x, 1 - c)
    right, left, across = tp_of(x + 1, c), tp_of(x - 1, c), tp_of(x + 2, c)
    ring_step = 2 * count
    above = lax.rem(sp + ring_step, sp_size)
    below = lax.rem(sp + sp_size - ring_step, sp_size)
    beside = sp + count * (1 - 2 * yh)
    halo_sp = lax.rem(sp + count * c, sp_size)

    core64 = pl.multiple_of(64 * c, 64)
    wl_q, wl_kv = core64, pl.multiple_of(128 + 64 * c, 64)
    wo_pool = pl.multiple_of(128 * c, 128)
    wo_attn = pl.multiple_of(256 + 256 * c, 256)
    shared = [
        (w_pool_in, lambda: wp.at[c]),
        (w_qlat, lambda: wl.at[pl.ds(wl_q, 64)]),
        (w_kvlat, lambda: wl.at[pl.ds(wl_kv, 64)]),
        (w_key, lambda: wk.at[c]),
        (w_value, lambda: wv.at[c]),
        (w_qc, lambda: wqc.at[c]),
        (w_qr, lambda: wqr.at[c]),
        (w_out_pool, lambda: wo.at[pl.ds(wo_pool, 128)]),
        (w_out_attn, lambda: wo.at[pl.ds(wo_attn, 256)]),
    ]
    n_shared = len(shared)
    local = [(src, dst()) for src, dst in shared]
    local += [
        (tokens.at[pl.ds(own_half, half)], tok.at[tp]),
        (w_krope, wl.at[pl.ds(256, 64)]),
        (w_krope, wl.at[pl.ds(320, 64)]),
        (base_tab, tab),
        (pool_mix.at[pl.ds(2 * x, 2)], mix),
        (mix_gain_in, mix_gain),
        (q_gain_in, q_gain),
        (kv_gain_in, kv_gain),
        (pool_scale_in, pool_scale),
        (rank_tab_in, rank_tab),
    ]
    local = [pltpu.make_async_copy(s, d, sem_local.at[i]) for i, (s, d) in enumerate(local)]
    given = [
        remote(s, d(), sem_ws.at[i], sem_wr.at[i], sp, partner) for i, (s, d) in enumerate(shared)
    ]
    for i in [9, 14, 18, 12, 10, 11, 0, 1, 2, 15, 16, 17, 3, 4, 5, 6, 13, 7, 8]:
        local[i].start()

    barrier = pltpu.get_barrier_semaphore()
    for i in range(1, PEERS):
        pl.semaphore_signal(
            barrier, inc=1, device_id={"sp": sp, "tp": lax.rem(tp + i, PEERS)}, device_id_type=MESH
        )
    def greet(other_sp, other_tp):
        pl.semaphore_signal(
            barrier, inc=1, device_id={"sp": other_sp, "tp": other_tp}, device_id_type=MESH
        )

    def answer(which, other_sp, other_tp):
        pl.semaphore_signal(
            sem_ready.at[which],
            inc=1,
            device_id={"sp": other_sp, "tp": other_tp},
            device_id_type=MESH,
        )

    last_place = z == ring - 1
    sends_halo = jnp.logical_and(c == 1, rank < SPAN - 1)
    takes_halo = jnp.logical_and(c == 0, rank > 0)
    greet(beside, tp)

    @pl.when(jnp.logical_not(last_place))
    def _():
        greet(above, tp)

    @pl.when(z == 0)
    def _():
        greet(below, tp)

    @pl.when(sends_halo)
    def _():
        greet(halo_sp, partner)

    greeters = PEERS + jnp.where(z > 0, 1, 0) + jnp.where(last_place, 1, 0)
    pl.semaphore_wait(barrier, greeters + jnp.where(takes_halo, 1, 0))

    @pl.when(z > 0)
    def _():
        answer(0, below, tp)

    @pl.when(last_place)
    def _():
        answer(1, above, tp)

    @pl.when(takes_halo)
    def _():
        answer(2, lax.rem(sp + sp_size - count, sp_size), partner)

    def token_copy(i, part):
        chip, core = x + (1, 1, 3, 3)[i], i % 2
        at = pl.ds(part * (half // 2), half // 2)
        return remote(
            tokens.at[pl.ds(half * core + part * (half // 2), half // 2)],
            tok.at[tp, at],
            sem_ts.at[i, part],
            sem_tr.at[tp, part],
            sp,
            tp_of(chip, core),
        )

    def token_wait(source, part):
        piece = tok.at[source, pl.ds(part * (half // 2), half // 2)]
        remote(piece, piece, sem_ts.at[0, 0], sem_tr.at[source, part], sp, partner).wait_recv()

    def token_relay(source, part, index, to):
        piece = tok.at[source, pl.ds(part * (half // 2), half // 2)]
        return remote(piece, piece, sem_relay_s.at[index], sem_tr.at[source, part], sp, to)

    token_copies = [token_copy(i, part) for part in (0, 1) for i in (0, 1)]
    token_copies += [token_copy(i, part) for part in (1, 0) for i in (2, 3)]
    token_copies = [token_copies[i] for i in (0, 4, 1, 5, 2, 6, 3, 7)]
    token_copies.append(
        remote(
            tokens.at[pl.ds(other_half, half)], tok.at[tp], sem_one_s.at[4], sem_one_r.at[4], sp, partner
        )
    )
    for cp in token_copies:
        cp.start()
    for g in given:
        g.start()

    local[12].wait()
    local[18].wait()
    lane = lax.broadcasted_iota(jnp.int32, (1, 128), 1)
    low_part = (lane % 64) < 32
    sign = jnp.where(low_part, -1.0, 1.0).astype(F32)
    cos_rank = rank_tab[0, pl.ds(rank, 1), :]
    sin_rank = rank_tab[1, pl.ds(rank, 1), :]
    cos_row, sin_row = tab[0], tab[1]
    tab[0] = cos_row * cos_rank - sin_row * sin_rank
    tab[1] = (sin_row * cos_rank + cos_row * sin_rank) * sign

    def rotate(v, cosine, signed_sine):
        swapped = jnp.where(low_part, pltpu.roll(v, 96, 1), pltpu.roll(v, 32, 1))
        return v * cosine + swapped * signed_sine

    relayed = []
    for i, core in ((0, c), (1, 1 - c)):
        for chip, piece, onward in ((1, 1, left), (3, 0, right)):
            source = tp_of(x + chip, core)
            token_wait(source, piece)
            relay = token_relay(source, piece, len(relayed), onward)
            relay.start()
            relayed.append(relay)
    for i in (0, 1, 2, 9, 10, 11, 14, 15, 16, 17):
        local[i].wait()
    for i in (0, 1, 2):
        given[i].wait_recv()

    def slab(j, squares):
        hop = j // 2
        chip = x + jnp.where(hop == 2, 3, jnp.where(hop == 3, 2, hop))
        source = tp_of(chip, (c + j) % 2)

        @pl.when(j == 1)
        def _():
            remote(tok.at[source], tok.at[source], sem_one_s.at[4], sem_one_r.at[4], sp, partner).wait_recv()

        @pl.when(jnp.logical_or(jnp.logical_and(j >= 2, j < 4), j >= 6))
        def _():
            token_wait(source, 0)

        @pl.when(j >= 4)
        def _():
            token_wait(source, 1)

        at = pl.ds(pl.multiple_of(source * width, width), width)
        raw = tok[source].astype(F32)
        scaled = (raw * mix_gain[:, at]).astype(BF16)
        raw = raw * raw
        new = jnp.concatenate(
            [dot(scaled, wp[0, at, :]), dot(scaled, wp[1, at, :]), dot(scaled, wl[:, at], NT)],
            axis=1,
        )

        @pl.when(j == 0)
        def _():
            proj[...] = new

        @pl.when(j > 0)
        def _():
            proj[...] += new

        return squares + raw[:, :128] + raw[:, 128:]

    squares = lax.fori_loop(0, PEERS, slab, jnp.zeros((half, 128), F32))
    inverse = lax.rsqrt(jnp.sum(squares, axis=1, keepdims=True) / (width * PEERS) + eps_norm)
    done = (proj[...] * inverse).astype(BF16)
    own = kvz.at[rank]
    own[:half, :] = done[:, 384:512]
    qbuf[x] = done[:, 256:384]
    pool_own[...] = done[:, :256]
    rope = done[:, 512:640].astype(F32)
    rope = rotate(rope, tab[0, pl.ds(own_half, half), :], tab[1, pl.ds(own_half, half), :])
    rope = jnp.where(lane < 64, rope[: half // 2], rope[half // 2 :])
    own[half : half + half // 2, :] = rope.astype(BF16)

    first_part = pl.ds(0, half + half // 2)
    second = pl.ds(half + half // 2, half)

    def block_copy(event, which, block, to):
        piece = kvz.at[block, first_part if which == 0 else second]
        return remote(piece, piece, sem_zs.at[event, which], sem_zr.at[event, which], to, tp)

    def start_own(which):
        for going, to in ((0, above), (1, below)):
            if follow[going, which][0]:

                @pl.when(goes(0, going, which, z))
                def _():
                    block_copy(follow[going, which][0], which, rank, to).start()

        block_copy(y_event, which, rank, beside).start()

    first = own.at[pl.ds(0, half)]
    to_left = remote(first, own.at[second], sem_zs.at[0, 1], sem_zr.at[0, 1], sp, left)
    to_right = remote(first, kvx.at[rank, 1], sem_xs.at[0, 1], sem_xr.at[0, 1], sp, right)
    to_across = remote(first, kvx.at[rank, 0], sem_xs.at[0, 0], sem_xr.at[0, 0], sp, across)
    q_copies = [
        remote(qbuf.at[x], qbuf.at[x], sem_qs.at[i], sem_qr.at[i], sp, who)
        for i, who in enumerate((left, right, across))
    ]
    q_from = [lax.rem(x + 1, CHIPS), lax.rem(x + 3, CHIPS), lax.rem(x + 2, CHIPS)]
    to_left.start()

    @pl.when(jnp.logical_not(last_place))
    def _():
        pl.semaphore_wait(sem_ready.at[0], 1)

    @pl.when(z == 0)
    def _():
        pl.semaphore_wait(sem_ready.at[1], 1)

    start_own(0)
    for q_copy in q_copies:
        q_copy.start()
    to_right.start()
    to_across.start()
    halo_copy = remote(
        pool_own.at[pl.ds(half - 16, 16)],
        halo,
        sem_one_s.at[0],
        sem_one_r.at[0],
        halo_sp,
        partner,
    )

    @pl.when(sends_halo)
    def _():
        pl.semaphore_wait(sem_ready.at[2], 1)

    halo_goes = jnp.logical_or(c == 0, sends_halo)
    halo_comes = jnp.logical_or(c == 1, takes_halo)

    @pl.when(halo_goes)
    def _():
        halo_copy.start()


    for i in (3, 4, 5, 6):
        local[i].wait()
        given[i].wait_recv()
    for r in range(CHIPS):
        at = pl.ds(pl.multiple_of(lax.rem(x + r, CHIPS) * 128, 128), 128)
        gk[:, 128 * r : 128 * r + 128] = kv_gain[:, at]
        for core in (0, 1):
            wk2[128 * r : 128 * r + 128, 256 * core : 256 * core + 256] = wk[core, at, :]
            wv2[128 * r : 128 * r + 128, 256 * core : 256 * core + 256] = wv[core, at, :]

    def rank_of(t):
        column = table(t, [e[0] for e in order])
        moved = table(t, shift)
        return lax.rem(z + moved + ring, ring) * 2 + lax.rem(yh + column, 2)

    def x_copy(t, block, which):
        piece = kvz.at[block, second if which == 0 else pl.ds(0, half)]
        return remote(
            piece,
            kvx.at[block, which],
            sem_xs.at[t, which],
            sem_xr.at[t, which],
            sp,
            left if which == 0 else right,
        )

    def forward(t, parts=(0, 1)):
        block = rank_of(t)
        place = block // 2
        for which in parts:

            @pl.when(place < table(t, limit[which]))
            def _():
                block_copy(t, which, block, above).wait_recv()

            for going, to in ((0, above), (1, below)):

                @pl.when(goes(t, going, which, place))
                def _():
                    entry = table(t, follow[going, which])
                    block_copy(entry, which, block, to).start()

            @pl.when(block < rank)
            def _():
                x_copy(t, block, 1 - which).start()


    def arrived(t, block):
        @pl.when(block <= rank)
        def _():
            x_copy(t, block, 0).wait_recv()
            x_copy(t, block, 1).wait_recv()

    to_left.wait_recv()
    start_own(1)

    forward(jnp.int32(1))
    forward(jnp.int32(2))
    for i, piece in enumerate(q_from):
        remote(
            qbuf.at[piece], qbuf.at[piece], sem_qs.at[i], sem_qr.at[i], sp, left
        ).wait_recv()
    latent = [qbuf[i].astype(F32) for i in range(CHIPS)]
    squares = latent[0] * latent[0]
    for i in range(1, CHIPS):
        squares = squares + latent[i] * latent[i]
    inverse = lax.rsqrt(jnp.sum(squares, axis=1, keepdims=True) / (128 * CHIPS) + eps_norm)
    for i in range(CHIPS):
        gain = q_gain[:, 128 * i : 128 * i + 128]
        qn[pl.ds(own_half, half), 128 * i : 128 * i + 128] = (latent[i] * inverse * gain).astype(BF16)
    qn_copy = remote(
        qn.at[pl.ds(own_half, half)],
        qn.at[pl.ds(own_half, half)],
        sem_one_s.at[1],
        sem_one_r.at[1],
        sp,
        partner,
    )
    qn_copy.start()
    qn_other = qn.at[pl.ds(other_half, half)]
    remote(qn_other, qn_other, sem_one_s.at[1], sem_one_r.at[1], sp, partner).wait_recv()
    normed = qn[...]
    to_log2 = (NOPE + ROPE) ** (-0.5) * math.log2(math.e)
    for core in (0, 1):
        content = (dot(normed, wqc[core]) * to_log2).astype(BF16)
        rotary = rotate(dot(normed, wqr[core]), tab[0], tab[1]) * to_log2
        for h in (0, 1):
            qs[2 * core + h, :, :128] = content[:, 128 * h : 128 * h + 128]
            turned = rotary if h == 0 else pltpu.roll(rotary, 64, 1)
            spare = jnp.where(lane == 64, 1.0, 0.0)
            qs[2 * core + h, :, 128:] = jnp.where(lane < 64, turned, spare).astype(BF16)

    most_at[...] = jnp.full(most_at.shape, masked_score, F32)
    sum_at[...] = jnp.zeros_like(sum_at)
    acc[...] = jnp.zeros_like(acc)

    def expand(blocks):
        parts = (pl.ds(0, half), second)
        def shown(b, value):
            return jnp.where(b <= rank, value.astype(F32), 0.0)

        piece = [
            jnp.concatenate([shown(b, kvz[b, at, :]) for b in blocks], axis=0) for at in parts
        ]
        piece += [jnp.concatenate([shown(b, kvx[b, i]) for b in blocks], axis=0) for i in (0, 1)]
        squares = piece[0] * piece[0]
        for i in range(1, CHIPS):
            squares = squares + piece[i] * piece[i]
        inverse = lax.rsqrt(jnp.sum(squares, axis=1, keepdims=True) / (128 * CHIPS) + eps_norm)
        normed = jnp.concatenate(
            [
                (piece[i] * inverse * gk[:, 128 * i : 128 * i + 128]).astype(BF16)
                for i in range(CHIPS)
            ],
            axis=1,
        )
        content = dot(normed, wk2[...]).astype(BF16)
        values = dot(normed, wv2[...]).astype(BF16)
        rotary = []
        for b in blocks:
            packed = shown(b, kvz[b, half : half + half // 2, :])
            hidden = jnp.where(b <= rank, 0.0, masked_score).astype(F32)
            spare = jnp.where(lane == 64, hidden, 0.0)
            rotary.append(jnp.where(lane < 64, packed, spare))
            rotary.append(jnp.where(lane < 64, pltpu.roll(packed, 64, 1), spare))
        rotary = jnp.concatenate(rotary, axis=0).astype(BF16)
        content_at[...] = content
        values_at[...] = values
        rotary_at[...] = rotary

    def attend_heads(heads, masked):
        if masked:
            column = lax.broadcasted_iota(jnp.int32, (rows, rows), 1)
            row = lax.broadcasted_iota(jnp.int32, (rows, rows), 0)
            allowed = jnp.logical_or(column >= half, column + half * c <= row)
        for h in heads:
            at = slice(128 * h, 128 * h + 128)
            keys = jnp.concatenate([content_at[:, at], rotary_at[...]], axis=1)
            scores = dot(qs[h], keys, NT)
            if masked:
                scores = jnp.where(allowed, scores, masked_score)
            old = most_at[h]
            new = jnp.maximum(old, jnp.max(scores, axis=1, keepdims=True))
            factor = jnp.exp2(old - new)
            expo = [jnp.exp2(scores[:, i : i + 128] - new) for i in range(0, rows, 128)]
            most_at[h] = new
            sum_at[h] = sum_at[h] * factor + sum(expo[1:], expo[0])
            expo = jnp.concatenate([e.astype(BF16) for e in expo], axis=1)
            acc[h] = acc[h] * factor + dot(expo, values_at[:, at])

    def pooling():
        @pl.when(halo_comes)
        def _():
            remote(halo, halo, sem_one_s.at[0], sem_one_r.at[0], sp, partner).wait_recv()

        local[13].wait()
        before = halo[...].astype(F32)
        before = jnp.where(halo_comes, before, 0.0)
        row = lax.broadcasted_iota(jnp.int32, (half, 128), 0) + (rank * rows + own_half)
        odd = x % 2
        for g in (0, 1):
            at = slice(128 * g, 128 * g + 128)
            values = pool_own[:, at].astype(F32)
            extended = jnp.concatenate([before[:, at], values], axis=0)
            sums = [extended]
            for step in (1, 2, 4, 8):
                sums.append(sums[-1] + pltpu.roll(sums[-1], step, 0))
            window = jnp.where(odd == 1, (8, 16)[g], (2, 4)[g])
            chosen = jnp.where(odd == 1, sums[3 + g][16:], sums[1 + g][16:])
            counts = jnp.minimum(row + 1, window).astype(F32)
            pooled = (chosen / counts - values).astype(BF16)
            scale = pool_scale[:, pl.ds(pl.multiple_of(256 * x + 128 * g, 128), 128)]
            pool_out[:, at] = (dot(pooled, mix[g]) * scale).astype(BF16)

    forward(jnp.int32(3))
    forward(jnp.int32(4))
    arrived(0, rank)
    arrived(1, rank_of(jnp.int32(1)))
    expand([rank, rank_of(jnp.int32(1))])
    attend_heads((0, 1), True)
    forward(jnp.int32(5))
    attend_heads((2, 3), True)

    def visit(i, carry):
        first, then = 2 * i + 4, 2 * i + 5
        events = [table(i, [pair[n] for pair in pairs]) for n in (0, 1)]
        earlier = [rank_of(t) for t in events]
        seen = jnp.logical_or(earlier[0] < rank, earlier[1] < rank)

        @pl.when(first < total_events)
        def _():
            forward(first)

        arrived(events[0], earlier[0])
        arrived(events[1], earlier[1])

        @pl.when(seen)
        def _():
            expand(earlier)
            attend_heads((0, 1), False)


        @pl.when(then < total_events)
        def _():
            forward(then)


        @pl.when(seen)
        def _():
            attend_heads((2, 3), False)

        @pl.when(i == 1)
        def _():
            pooling()

        return carry

    def visit_last(i, carry):
        events = [table(i, [pair[n] for pair in pairs]) for n in (0, 1)]
        earlier = [rank_of(t) for t in events]
        arrived(events[0], earlier[0])
        arrived(events[1], earlier[1])

        @pl.when(jnp.logical_or(earlier[0] < rank, earlier[1] < rank))
        def _():
            expand(earlier)
            attend_heads((0, 1, 2, 3), False)

        return carry

    all_sent = (total_events - 4) // 2
    lax.fori_loop(1, all_sent, visit, 0)
    lax.fori_loop(all_sent, total_events // 2, visit_last, 0)

    acc_copy = remote(
        acc.at[:, pl.ds(other_half, half), :], acc_in, sem_one_s.at[2], sem_one_r.at[2], sp, partner
    )
    acc_copy.start()
    packed = jnp.zeros((rows, 128), F32)
    for h in range(4):
        packed = jnp.where(lane == h, most_at[h], packed)
        packed = jnp.where(lane == 8 + h, jnp.sum(sum_at[h], axis=1, keepdims=True), packed)
    stat[...] = packed
    stat_copy = remote(stat, stat_in, sem_one_s.at[3], sem_one_r.at[3], sp, partner)
    stat_copy.start()
    for i in (7, 8):
        local[i].wait()
        given[i].wait_recv()
    stat_copy.wait_recv()
    acc_copy.wait_recv()
    own_rows = pl.ds(own_half, half)
    mine_now, other_now = stat[...], stat_in[...]
    most = jnp.maximum(mine_now, other_now)
    sum_at[0] = jnp.exp2(mine_now - most)
    sum_at[1] = jnp.exp2(other_now - most)
    sums = pltpu.roll(mine_now, 120, 1) * sum_at[0] + pltpu.roll(other_now, 120, 1) * sum_at[1]
    sums = jnp.where(lane < 4, sums, 1.0)
    logs = jnp.where(lane < 4, most, 0.0) * math.log(2.0) + jnp.log(sums)
    logs = logs.T
    logt[...] = jnp.where(c == 0, logs[0:2, :], logs[2:4, :])
    most_at[0] = 1.0 / sums
    mixed = [pool_out[...]]
    for h in range(4):
        share = most_at[0, own_rows, h : h + 1]
        own_share = sum_at[0, own_rows, h : h + 1] * share
        other_share = sum_at[1, own_rows, h : h + 1] * share
        mixed.append((acc[h, own_rows, :] * own_share + acc_in[h] * other_share).astype(BF16))
    mixed = jnp.concatenate(mixed, axis=1)

    columns = wo.shape[1]
    chunks = sem_rs_s.shape[1]
    chunk = columns // chunks
    mine = x // 2 == c

    def part_copy(i, n):
        at = pl.ds(n * chunk, chunk)
        return remote(
            part.at[pl.ds(quarter * i, quarter), at],
            rs.at[x, :, at],
            sem_rs_s.at[i, n],
            sem_rs_r.at[x, n],
            sp,
            4 * c + i,
        )

    own_at = pl.multiple_of(quarter * lax.rem(tp, 4), quarter)

    def part_keep(n):
        at = pl.ds(n * chunk, chunk)
        return pltpu.make_async_copy(
            part.at[pl.ds(own_at, quarter), at], rs.at[x, :, at], sem_local.at[19 + n]
        )

    for n in range(chunks):
        at = slice(n * chunk, (n + 1) * chunk)
        part[:, at] = dot(mixed, wo[:, at]).astype(BF16)
        for i in range(4):

            @pl.when(4 * c + i != tp)
            def _():
                part_copy(i, n).start()

        @pl.when(mine)
        def _():
            part_keep(n).start()

    for n in range(chunks):
        at = slice(n * chunk, (n + 1) * chunk)
        for chip in range(CHIPS):

            @pl.when(jnp.logical_and(mine, x == chip))
            def _():
                part_keep(n).wait()

            @pl.when(jnp.logical_not(jnp.logical_and(mine, x == chip)))
            def _():
                ref = rs.at[chip, :, pl.ds(n * chunk, chunk)]
                remote(ref, ref, sem_rs_s.at[0, n], sem_rs_r.at[chip, n], sp, partner).wait_recv()

        out[:, at] = (
            rs[0, :, at].astype(F32)
            + rs[1, :, at].astype(F32)
            + rs[2, :, at].astype(F32)
            + rs[3, :, at].astype(F32)
        ).astype(BF16)

    for cp in token_copies + given + q_copies:
        cp.wait_send()
    for relay in relayed:
        relay.wait_send()
    to_left.wait_send()
    to_right.wait_send()
    to_across.wait_send()
    for cp in (qn_copy, acc_copy, stat_copy):
        cp.wait_send()

    @pl.when(halo_goes)
    def _():
        halo_copy.wait_send()


    for which in (0, 1):
        block_copy(y_event, which, 0, beside).wait_send()
    for t in range(total_events):
        held = rank_of(t) // 2
        for which in (0, 1):
            for going, to in ((0, above), (1, below)):
                entry = follow[going, which][t]
                if entry:

                    @pl.when(goes(t, going, which, held))
                    def _():
                        block_copy(entry, which, 0, to).wait_send()

    for t in range(1, total_events):

        @pl.when(rank_of(t) < rank)
        def _():
            x_copy(t, 0, 0).wait_send()
            x_copy(t, 0, 1).wait_send()

    for n in range(chunks):
        for i in range(4):

            @pl.when(4 * c + i != tp)
            def _():
                part_copy(i, n).wait_send()


def rotary_tables(rows, ranks):
    frequency = rope_base ** (-np.arange(ROPE // 2, dtype=np.float64) * 2.0 / ROPE)
    frequency = np.tile(frequency, 128 // (ROPE // 2))
    by_row = np.arange(rows)[:, None] * frequency[None, :]
    by_rank = (np.arange(ranks) * rows)[:, None] * frequency[None, :]
    return (
        np.stack([np.cos(by_row), np.sin(by_row)]).astype(np.float32),
        np.stack([np.cos(by_rank), np.sin(by_rank)]).astype(np.float32),
    )


def per_device(
    sp_size,
    tokens,
    mix_gain,
    w_pool_in,
    w_qlat,
    w_kvlat,
    w_krope,
    q_gain,
    kv_gain,
    w_q_content,
    w_q_rotary,
    w_key,
    w_value,
    pool_mix,
    pool_scale,
    w_out_pool,
    w_out_attn,
):
    rows, width = tokens.shape
    half = rows // 2
    columns = w_out_attn.shape[1]
    features = width * PEERS
    base_tab, rank_tab = rotary_tables(rows, SPAN)
    total_events = len(event_list(SPAN // 2)[0])
    chunks = 2
    anywhere = pl.BlockSpec(memory_space=pl.ANY)
    near = pl.BlockSpec(memory_space=pltpu.VMEM)
    dma = lambda *shape: pltpu.SemaphoreType.DMA(shape)
    vmem = pltpu.VMEM
    out, logt = pl.pallas_call(
        functools.partial(kernel, sp_size),
        out_shape=(
            jax.ShapeDtypeStruct((rows // PEERS, columns), BF16),
            jax.ShapeDtypeStruct((2, rows), F32),
        ),
        in_specs=[anywhere] * 18,
        out_specs=(near, near),
        scratch_shapes=[
            vmem((1, features), F32),
            vmem((1, 512), F32),
            vmem((1, 512), F32),
            vmem((1, 1024), F32),
            vmem((2, SPAN, 128), F32),
            vmem((PEERS, half, width), BF16),
            vmem((2, features, 128), BF16),
            vmem((384, features), BF16),
            vmem((2, 512, 256), BF16),
            vmem((2, 512, 128), BF16),
            vmem((2, 512, 256), BF16),
            vmem((2, 512, 256), BF16),
            vmem((2, 128, 128), BF16),
            vmem((768, columns), BF16),
            vmem((2, rows, 128), F32),
            vmem((half, 640), F32),
            vmem((half, 256), BF16),
            vmem((16, 256), BF16),
            vmem((half, 256), BF16),
            vmem((SPAN, 2 * half + half // 2, 128), BF16),
            vmem((SPAN, 2, half, 128), BF16),
            vmem((CHIPS, half, 128), BF16),
            vmem((rows, 512), BF16),
            vmem((4, rows, 256), BF16),
            vmem((512, 512), BF16),
            vmem((512, 512), BF16),
            vmem((1, 512), F32),
            vmem((rows, 512), BF16),
            vmem((rows, 512), BF16),
            vmem((rows, 128), BF16),
            vmem((4, rows, 128), F32),
            vmem((rows, 128), F32),
            vmem((rows, 128), F32),
            vmem((4, rows, 128), F32),
            vmem((4, rows, 128), F32),
            vmem((4, half, 128), F32),
            vmem((half, columns), BF16),
            vmem((CHIPS, rows // PEERS, columns), BF16),
            dma(19 + chunks),
            dma(9),
            dma(9),
            dma(4, 2),
            dma(PEERS, 2),
            dma(total_events, 2),
            dma(total_events, 2),
            dma(total_events, 2),
            dma(total_events, 2),
            dma(3),
            dma(3),
            dma(5),
            dma(5),
            dma(4, chunks),
            dma(CHIPS, chunks),
            dma(4),
            pltpu.SemaphoreType.REGULAR((3,)),
        ],
        compiler_params=pltpu.CompilerParams(
            collective_id=0, has_side_effects=True, vmem_limit_bytes=56 * 1024 * 1024
        ),
    )(
        tokens,
        mix_gain.reshape(1, -1),
        w_pool_in,
        w_qlat.T,
        w_kvlat.T,
        w_krope.T,
        q_gain.reshape(1, -1),
        kv_gain.reshape(1, -1),
        w_q_content,
        w_q_rotary,
        w_key,
        w_value,
        pool_mix,
        pool_scale.reshape(1, -1),
        w_out_pool,
        w_out_attn,
        jnp.asarray(base_tab),
        jnp.asarray(rank_tab),
    )
    return out, logt.T


def solution(mesh):
    in_specs = (
        P("sp", "tp"),
        P(),
        P(None, "tp"),
        P(None, "tp"),
        P(None, "tp"),
        P(),
        P(),
        P(),
        P(None, "tp"),
        P(None, "tp"),
        P(None, "tp"),
        P(None, "tp"),
        P(),
        P(),
        P("tp", None),
        P("tp", None),
    )
    out_specs = (P(("sp", "tp"), None), P("sp", "tp"))
    return jax.shard_map(
        functools.partial(per_device, mesh.shape["sp"]),
        mesh=mesh,
        in_specs=in_specs,
        out_specs=out_specs,
        check_vma=False,
    )
```

```python
import functools
import math

import jax
import jax.numpy as jnp
import numpy as np
from jax import lax
from jax.experimental import pallas as pl
from jax.experimental.pallas import tpu as pltpu
from jax.sharding import PartitionSpec as P

NOPE = 128
ROPE = 64
VDIM = 128
GROUP_DIM = 128
SPAN = 16
CHIPS = 4
PEERS = 8

eps_norm = 1e-06
rope_base = 10000.0
masked_score = -1e30

MESH = pl.DeviceIdType.MESH
F32 = jnp.float32
BF16 = jnp.bfloat16
NT = (((1,), (1,)), ((), ()))


def event_list(ring):
    far = ring // 2
    timed = []
    for column in (0, 1):
        first, pace = (0.0, 4.5) if column == 0 else (10.0, 4.7)
        timed.append((first, (column, 0, 0)))
        for k in range(1, far):
            timed.append((first + pace * k, (column, 0, k)))
            late = 5.0 if column == 1 and k == far - 1 else 0.1
            timed.append((first + pace * k + late, (column, 1, k)))
        timed.append((first + pace * far, (column, 2, far)))
    order = [e for _, e in sorted(timed)]
    at = {e: i for i, e in enumerate(order)}
    follow = {}
    for going in (0, 1):
        for which in (0, 1):
            entries = []
            for column, direction, k in order:
                entry = 0
                if k == 0 or direction == going:
                    if k + 1 < far:
                        entry = at[(column, going, k + 1)]
                    elif going == 0 or which == 1:
                        entry = at[(column, 2, far)]
                entries.append(entry)
            follow[going, which] = entries
    shift = [k if direction == 1 else -k for _, direction, k in order]
    limit = ([], [])
    for which in (0, 1):
        for column, direction, k in order:
            bound = (ring - k, far - 1 + which, far)[direction]
            limit[which].append(bound)
    next_limit, next_least = {}, {}
    for (going, which), entries in follow.items():
        to_far = [e > 0 and order[e][1] == 2 and which == 1 for e in entries]
        next_limit[going, which] = [
            (far - 1 if f and going == 0 else limit[which][e]) if e else 0
            for e, f in zip(entries, to_far)
        ]
        next_least[going, which] = [far - 1 if f and going == 1 else 0 for f in to_far]
    when = {e: t for t, e in timed}
    pairs = []
    for above in (False, True):
        group = [e for e in order if (e[1] == 1) == above]
        pairs += list(zip(group[::2], group[1::2]))
    pairs.sort(key=lambda pair: when[pair[1]])
    pairs = [[at[e] for e in pair] for pair in pairs]
    return order, follow, shift, at[(1, 0, 0)], limit, next_limit, next_least, pairs


def table(index, entries):
    if isinstance(index, int):
        return jnp.int32(entries[index])
    out = jnp.int32(entries[0])
    for i, entry in enumerate(entries):
        if i > 0 and entry != entries[0]:
            out = jnp.where(index == i, jnp.int32(entry), out)
    return out


def remote(src, dst, send, recv, sp, tp):
    return pltpu.make_async_remote_copy(
        src_ref=src,
        dst_ref=dst,
        send_sem=send,
        recv_sem=recv,
        device_id={"sp": sp, "tp": tp},
        device_id_type=MESH,
    )


def dot(a, b, dims=(((1,), (0,)), ((), ()))):
    return lax.dot_general(a, b, dims, preferred_element_type=F32)


def kernel(
    sp_size,
    tokens,
    mix_gain_in,
    w_pool_in,
    w_qlat,
    w_kvlat,
    w_krope,
    q_gain_in,
    kv_gain_in,
    w_qc,
    w_qr,
    w_key,
    w_value,
    pool_mix,
    pool_scale_in,
    w_out_pool,
    w_out_attn,
    base_tab,
    rank_tab_in,
    rs,
    logt,
    mix_gain,
    q_gain,
    kv_gain,
    pool_scale,
    rank_tab,
    tok,
    wp,
    wl,
    wqc,
    wqr,
    wk,
    wv,
    mix,
    wo,
    tab,
    proj,
    pool_own,
    halo,
    pool_out,
    kvz,
    kvx,
    qbuf,
    qn,
    qs,
    wk2,
    wv2,
    gk,
    content_at,
    values_at,
    rotary_at,
    acc,
    stat,
    stat_in,
    most_at,
    sum_at,
    acc_in,
    part,
    sem_local,
    sem_ws,
    sem_wr,
    sem_ts,
    sem_tr,
    sem_zs,
    sem_zr,
    sem_xs,
    sem_xr,
    sem_qs,
    sem_qr,
    sem_one_s,
    sem_one_r,
    sem_rs_s,
    sem_rs_r,
    sem_relay_s,
    sem_ready,
):
    sp = lax.axis_index("sp")
    tp = lax.axis_index("tp")
    count = sp_size // SPAN
    ring = SPAN // 2
    x, c = tp // 2, tp % 2
    rank = sp // count
    z, yh = rank // 2, rank % 2
    order, follow, shift, y_event, limit, next_limit, next_least, pairs = event_list(ring)

    def goes(t, going, which, place):
        least = table(t, next_least[going, which])
        return jnp.logical_and(place >= least, place < table(t, next_limit[going, which]))

    total_events = len(order)
    rows = tokens.shape[0]
    half = rows // 2
    width = tokens.shape[1]
    quarter = half // 4
    own_half = pl.multiple_of(half * c, half)
    other_half = pl.multiple_of(half * (1 - c), half)

    def tp_of(chip, core):
        return lax.rem(chip + CHIPS, CHIPS) * 2 + core

    partner = tp_of(x, 1 - c)
    right, left, across = tp_of(x + 1, c), tp_of(x - 1, c), tp_of(x + 2, c)
    ring_step = 2 * count
    above = lax.rem(sp + ring_step, sp_size)
    below = lax.rem(sp + sp_size - ring_step, sp_size)
    beside = sp + count * (1 - 2 * yh)
    halo_sp = lax.rem(sp + count * c, sp_size)

    core64 = pl.multiple_of(64 * c, 64)
    wl_q, wl_kv = core64, pl.multiple_of(128 + 64 * c, 64)
    wo_pool = pl.multiple_of(128 * c, 128)
    wo_attn = pl.multiple_of(256 + 256 * c, 256)
    shared = [
        (w_pool_in, lambda: wp.at[c]),
        (w_qlat, lambda: wl.at[pl.ds(wl_q, 64)]),
        (w_kvlat, lambda: wl.at[pl.ds(wl_kv, 64)]),
        (w_key, lambda: wk.at[c]),
        (w_value, lambda: wv.at[c]),
        (w_qc, lambda: wqc.at[c]),
        (w_qr, lambda: wqr.at[c]),
        (w_out_pool, lambda: wo.at[pl.ds(wo_pool, 128)]),
        (w_out_attn, lambda: wo.at[pl.ds(wo_attn, 256)]),
    ]
    n_shared = len(shared)
    local = [(src, dst()) for src, dst in shared]
    local += [
        (tokens.at[pl.ds(own_half, half)], tok.at[tp]),
        (w_krope, wl.at[pl.ds(256, 64)]),
        (w_krope, wl.at[pl.ds(320, 64)]),
        (base_tab, tab),
        (pool_mix.at[pl.ds(2 * x, 2)], mix),
        (mix_gain_in, mix_gain),
        (q_gain_in, q_gain),
        (kv_gain_in, kv_gain),
        (pool_scale_in, pool_scale),
        (rank_tab_in, rank_tab),
    ]
    local = [pltpu.make_async_copy(s, d, sem_local.at[i]) for i, (s, d) in enumerate(local)]
    given = [
        remote(s, d(), sem_ws.at[i], sem_wr.at[i], sp, partner) for i, (s, d) in enumerate(shared)
    ]
    for i in [9, 14, 18, 12, 10, 11, 0, 1, 2, 15, 16, 17, 3, 4, 5, 6, 13, 7, 8]:
        local[i].start()

    barrier = pltpu.get_barrier_semaphore()
    for i in range(1, PEERS):
        pl.semaphore_signal(
            barrier, inc=1, device_id={"sp": sp, "tp": lax.rem(tp + i, PEERS)}, device_id_type=MESH
        )
    def greet(other_sp, other_tp):
        pl.semaphore_signal(
            barrier, inc=1, device_id={"sp": other_sp, "tp": other_tp}, device_id_type=MESH
        )

    def answer(which, other_sp, other_tp):
        pl.semaphore_signal(
            sem_ready.at[which],
            inc=1,
            device_id={"sp": other_sp, "tp": other_tp},
            device_id_type=MESH,
        )

    last_place = z == ring - 1
    sends_halo = jnp.logical_and(c == 1, rank < SPAN - 1)
    takes_halo = jnp.logical_and(c == 0, rank > 0)
    greet(beside, tp)

    @pl.when(jnp.logical_not(last_place))
    def _():
        greet(above, tp)

    @pl.when(z == 0)
    def _():
        greet(below, tp)

    @pl.when(sends_halo)
    def _():
        greet(halo_sp, partner)

    greeters = PEERS + jnp.where(z > 0, 1, 0) + jnp.where(last_place, 1, 0)
    pl.semaphore_wait(barrier, greeters + jnp.where(takes_halo, 1, 0))

    @pl.when(z > 0)
    def _():
        answer(0, below, tp)

    @pl.when(last_place)
    def _():
        answer(1, above, tp)

    @pl.when(takes_halo)
    def _():
        answer(2, lax.rem(sp + sp_size - count, sp_size), partner)

    def token_copy(i, part):
        chip, core = x + (1, 1, 3, 3)[i], i % 2
        at = pl.ds(part * (half // 2), half // 2)
        return remote(
            tokens.at[pl.ds(half * core + part * (half // 2), half // 2)],
            tok.at[tp, at],
            sem_ts.at[i, part],
            sem_tr.at[tp, part],
            sp,
            tp_of(chip, core),
        )

    def token_wait(source, part):
        piece = tok.at[source, pl.ds(part * (half // 2), half // 2)]
        remote(piece, piece, sem_ts.at[0, 0], sem_tr.at[source, part], sp, partner).wait_recv()

    def token_relay(source, part, index, to):
        piece = tok.at[source, pl.ds(part * (half // 2), half // 2)]
        return remote(piece, piece, sem_relay_s.at[index], sem_tr.at[source, part], sp, to)

    token_copies = [token_copy(i, part) for part in (0, 1) for i in (0, 1)]
    token_copies += [token_copy(i, part) for part in (1, 0) for i in (2, 3)]
    token_copies = [token_copies[i] for i in (0, 4, 1, 5, 2, 6, 3, 7)]
    token_copies.append(
        remote(
            tokens.at[pl.ds(other_half, half)], tok.at[tp], sem_one_s.at[4], sem_one_r.at[4], sp, partner
        )
    )
    for cp in token_copies:
        cp.start()
    for g in given:
        g.start()

    local[12].wait()
    local[18].wait()
    lane = lax.broadcasted_iota(jnp.int32, (1, 128), 1)
    low_part = (lane % 64) < 32
    sign = jnp.where(low_part, -1.0, 1.0).astype(F32)
    cos_rank = rank_tab[0, pl.ds(rank, 1), :]
    sin_rank = rank_tab[1, pl.ds(rank, 1), :]
    cos_row, sin_row = tab[0], tab[1]
    tab[0] = cos_row * cos_rank - sin_row * sin_rank
    tab[1] = (sin_row * cos_rank + cos_row * sin_rank) * sign

    def rotate(v, cosine, signed_sine):
        swapped = jnp.where(low_part, pltpu.roll(v, 96, 1), pltpu.roll(v, 32, 1))
        return v * cosine + swapped * signed_sine

    relayed = []
    for i, core in ((0, c), (1, 1 - c)):
        for chip, piece, onward in ((1, 1, left), (3, 0, right)):
            source = tp_of(x + chip, core)
            token_wait(source, piece)
            relay = token_relay(source, piece, len(relayed), onward)
            relay.start()
            relayed.append(relay)
    for i in (0, 1, 2, 9, 10, 11, 14, 15, 16, 17):
        local[i].wait()
    for i in (0, 1, 2):
        given[i].wait_recv()

    def slab(j, squares):
        hop = j // 2
        chip = x + jnp.where(hop == 2, 3, jnp.where(hop == 3, 2, hop))
        source = tp_of(chip, (c + j) % 2)

        @pl.when(j == 1)
        def _():
            remote(tok.at[source], tok.at[source], sem_one_s.at[4], sem_one_r.at[4], sp, partner).wait_recv()

        @pl.when(jnp.logical_or(jnp.logical_and(j >= 2, j < 4), j >= 6))
        def _():
            token_wait(source, 0)

        @pl.when(j >= 4)
        def _():
            token_wait(source, 1)

        at = pl.ds(pl.multiple_of(source * width, width), width)
        raw = tok[source].astype(F32)
        scaled = (raw * mix_gain[:, at]).astype(BF16)
        raw = raw * raw
        new = jnp.concatenate(
            [dot(scaled, wp[0, at, :]), dot(scaled, wp[1, at, :]), dot(scaled, wl[:, at], NT)],
            axis=1,
        )

        @pl.when(j == 0)
        def _():
            proj[...] = new

        @pl.when(j > 0)
        def _():
            proj[...] += new

        return squares + raw[:, :128] + raw[:, 128:]

    squares = lax.fori_loop(0, PEERS, slab, jnp.zeros((half, 128), F32))
    inverse = lax.rsqrt(jnp.sum(squares, axis=1, keepdims=True) / (width * PEERS) + eps_norm)
    done = (proj[...] * inverse).astype(BF16)
    own = kvz.at[rank]
    own[:half, :] = done[:, 384:512]
    qbuf[x] = done[:, 256:384]
    pool_own[...] = done[:, :256]
    rope = done[:, 512:640].astype(F32)
    rope = rotate(rope, tab[0, pl.ds(own_half, half), :], tab[1, pl.ds(own_half, half), :])
    rope = jnp.where(lane < 64, rope[: half // 2], rope[half // 2 :])
    own[half : half + half // 2, :] = rope.astype(BF16)

    first_part = pl.ds(0, half + half // 2)
    second = pl.ds(half + half // 2, half)

    def block_copy(event, which, block, to):
        piece = kvz.at[block, first_part if which == 0 else second]
        return remote(piece, piece, sem_zs.at[event, which], sem_zr.at[event, which], to, tp)

    def start_own(which):
        for going, to in ((0, above), (1, below)):
            if follow[going, which][0]:

                @pl.when(goes(0, going, which, z))
                def _():
                    block_copy(follow[going, which][0], which, rank, to).start()

        block_copy(y_event, which, rank, beside).start()

    first = own.at[pl.ds(0, half)]
    to_left = remote(first, own.at[second], sem_zs.at[0, 1], sem_zr.at[0, 1], sp, left)
    to_right = remote(first, kvx.at[rank, 1], sem_xs.at[0, 1], sem_xr.at[0, 1], sp, right)
    to_across = remote(first, kvx.at[rank, 0], sem_xs.at[0, 0], sem_xr.at[0, 0], sp, across)
    q_copies = [
        remote(qbuf.at[x], qbuf.at[x], sem_qs.at[i], sem_qr.at[i], sp, who)
        for i, who in enumerate((left, right, across))
    ]
    q_from = [lax.rem(x + 1, CHIPS), lax.rem(x + 3, CHIPS), lax.rem(x + 2, CHIPS)]
    to_left.start()

    @pl.when(jnp.logical_not(last_place))
    def _():
        pl.semaphore_wait(sem_ready.at[0], 1)

    @pl.when(z == 0)
    def _():
        pl.semaphore_wait(sem_ready.at[1], 1)

    start_own(0)
    for q_copy in q_copies:
        q_copy.start()
    to_right.start()
    to_across.start()
    halo_copy = remote(
        pool_own.at[pl.ds(half - 16, 16)],
        halo,
        sem_one_s.at[0],
        sem_one_r.at[0],
        halo_sp,
        partner,
    )

    @pl.when(sends_halo)
    def _():
        pl.semaphore_wait(sem_ready.at[2], 1)

    halo_goes = jnp.logical_or(c == 0, sends_halo)
    halo_comes = jnp.logical_or(c == 1, takes_halo)

    @pl.when(halo_goes)
    def _():
        halo_copy.start()


    for i in (3, 4, 5, 6):
        local[i].wait()
        given[i].wait_recv()
    for r in range(CHIPS):
        at = pl.ds(pl.multiple_of(lax.rem(x + r, CHIPS) * 128, 128), 128)
        gk[:, 128 * r : 128 * r + 128] = kv_gain[:, at]
        for core in (0, 1):
            wk2[128 * r : 128 * r + 128, 256 * core : 256 * core + 256] = wk[core, at, :]
            wv2[128 * r : 128 * r + 128, 256 * core : 256 * core + 256] = wv[core, at, :]

    def rank_of(t):
        column = table(t, [e[0] for e in order])
        moved = table(t, shift)
        return lax.rem(z + moved + ring, ring) * 2 + lax.rem(yh + column, 2)

    def x_copy(t, block, which):
        piece = kvz.at[block, second if which == 0 else pl.ds(0, half)]
        return remote(
            piece,
            kvx.at[block, which],
            sem_xs.at[t, which],
            sem_xr.at[t, which],
            sp,
            left if which == 0 else right,
        )

    def forward(t, parts=(0, 1)):
        block = rank_of(t)
        place = block // 2
        for which in parts:

            @pl.when(place < table(t, limit[which]))
            def _():
                block_copy(t, which, block, above).wait_recv()

            for going, to in ((0, above), (1, below)):

                @pl.when(goes(t, going, which, place))
                def _():
                    entry = table(t, follow[going, which])
                    block_copy(entry, which, block, to).start()

            @pl.when(block < rank)
            def _():
                x_copy(t, block, 1 - which).start()


    def arrived(t, block):
        @pl.when(block <= rank)
        def _():
            x_copy(t, block, 0).wait_recv()
            x_copy(t, block, 1).wait_recv()

    to_left.wait_recv()
    start_own(1)

    forward(jnp.int32(1), (0,))
    forward(jnp.int32(2), (0,))
    for i, piece in enumerate(q_from):
        remote(
            qbuf.at[piece], qbuf.at[piece], sem_qs.at[i], sem_qr.at[i], sp, left
        ).wait_recv()
    latent = [qbuf[i].astype(F32) for i in range(CHIPS)]
    squares = latent[0] * latent[0]
    for i in range(1, CHIPS):
        squares = squares + latent[i] * latent[i]
    inverse = lax.rsqrt(jnp.sum(squares, axis=1, keepdims=True) / (128 * CHIPS) + eps_norm)
    for i in range(CHIPS):
        gain = q_gain[:, 128 * i : 128 * i + 128]
        qn[pl.ds(own_half, half), 128 * i : 128 * i + 128] = (latent[i] * inverse * gain).astype(BF16)
    qn_copy = remote(
        qn.at[pl.ds(own_half, half)],
        qn.at[pl.ds(own_half, half)],
        sem_one_s.at[1],
        sem_one_r.at[1],
        sp,
        partner,
    )
    qn_copy.start()
    forward(jnp.int32(1), (1,))
    forward(jnp.int32(2), (1,))
    qn_other = qn.at[pl.ds(other_half, half)]
    remote(qn_other, qn_other, sem_one_s.at[1], sem_one_r.at[1], sp, partner).wait_recv()
    normed = qn[...]
    to_log2 = (NOPE + ROPE) ** (-0.5) * math.log2(math.e)
    for core in (0, 1):
        content = (dot(normed, wqc[core]) * to_log2).astype(BF16)
        rotary = rotate(dot(normed, wqr[core]), tab[0], tab[1]) * to_log2
        for h in (0, 1):
            qs[2 * core + h, :, :128] = content[:, 128 * h : 128 * h + 128]
            turned = rotary if h == 0 else pltpu.roll(rotary, 64, 1)
            spare = jnp.where(lane == 64, 1.0, 0.0)
            qs[2 * core + h, :, 128:] = jnp.where(lane < 64, turned, spare).astype(BF16)

    most_at[...] = jnp.full(most_at.shape, masked_score, F32)
    sum_at[...] = jnp.zeros_like(sum_at)
    acc[...] = jnp.zeros_like(acc)

    def expand(blocks):
        parts = (pl.ds(0, half), second)
        def shown(b, value):
            return jnp.where(b <= rank, value.astype(F32), 0.0)

        piece = [
            jnp.concatenate([shown(b, kvz[b, at, :]) for b in blocks], axis=0) for at in parts
        ]
        piece += [jnp.concatenate([shown(b, kvx[b, i]) for b in blocks], axis=0) for i in (0, 1)]
        squares = piece[0] * piece[0]
        for i in range(1, CHIPS):
            squares = squares + piece[i] * piece[i]
        inverse = lax.rsqrt(jnp.sum(squares, axis=1, keepdims=True) / (128 * CHIPS) + eps_norm)
        normed = jnp.concatenate(
            [
                (piece[i] * inverse * gk[:, 128 * i : 128 * i + 128]).astype(BF16)
                for i in range(CHIPS)
            ],
            axis=1,
        )
        content = dot(normed, wk2[...]).astype(BF16)
        values = dot(normed, wv2[...]).astype(BF16)
        rotary = []
        for b in blocks:
            packed = shown(b, kvz[b, half : half + half // 2, :])
            hidden = jnp.where(b <= rank, 0.0, masked_score).astype(F32)
            spare = jnp.where(lane == 64, hidden, 0.0)
            rotary.append(jnp.where(lane < 64, packed, spare))
            rotary.append(jnp.where(lane < 64, pltpu.roll(packed, 64, 1), spare))
        rotary = jnp.concatenate(rotary, axis=0).astype(BF16)
        content_at[...] = content
        values_at[...] = values
        rotary_at[...] = rotary

    def attend_heads(heads, masked):
        if masked:
            column = lax.broadcasted_iota(jnp.int32, (rows, rows), 1)
            row = lax.broadcasted_iota(jnp.int32, (rows, rows), 0)
            allowed = jnp.logical_or(column >= half, column + half * c <= row)
        for h in heads:
            at = slice(128 * h, 128 * h + 128)
            keys = jnp.concatenate([content_at[:, at], rotary_at[...]], axis=1)
            scores = dot(qs[h], keys, NT)
            if masked:
                scores = jnp.where(allowed, scores, masked_score)
            old = most_at[h]
            new = jnp.maximum(old, jnp.max(scores, axis=1, keepdims=True))
            factor = jnp.exp2(old - new)
            expo = [jnp.exp2(scores[:, i : i + 128] - new) for i in range(0, rows, 128)]
            most_at[h] = new
            sum_at[h] = sum_at[h] * factor + sum(expo[1:], expo[0])
            expo = jnp.concatenate([e.astype(BF16) for e in expo], axis=1)
            acc[h] = acc[h] * factor + dot(expo, values_at[:, at])

    def pooling():
        @pl.when(halo_comes)
        def _():
            remote(halo, halo, sem_one_s.at[0], sem_one_r.at[0], sp, partner).wait_recv()

        local[13].wait()
        before = halo[...].astype(F32)
        before = jnp.where(halo_comes, before, 0.0)
        row = lax.broadcasted_iota(jnp.int32, (half, 128), 0) + (rank * rows + own_half)
        odd = x % 2
        for g in (0, 1):
            at = slice(128 * g, 128 * g + 128)
            values = pool_own[:, at].astype(F32)
            extended = jnp.concatenate([before[:, at], values], axis=0)
            sums = [extended]
            for step in (1, 2, 4, 8):
                sums.append(sums[-1] + pltpu.roll(sums[-1], step, 0))
            window = jnp.where(odd == 1, (8, 16)[g], (2, 4)[g])
            chosen = jnp.where(odd == 1, sums[3 + g][16:], sums[1 + g][16:])
            counts = jnp.minimum(row + 1, window).astype(F32)
            pooled = (chosen / counts - values).astype(BF16)
            scale = pool_scale[:, pl.ds(pl.multiple_of(256 * x + 128 * g, 128), 128)]
            pool_out[:, at] = (dot(pooled, mix[g]) * scale).astype(BF16)

    pooling()
    forward(jnp.int32(3))
    forward(jnp.int32(4))
    arrived(0, rank)
    arrived(1, rank_of(jnp.int32(1)))
    expand([rank, rank_of(jnp.int32(1))])
    attend_heads((0, 1), True)
    forward(jnp.int32(5))
    attend_heads((2, 3), True)

    def visit(i, carry):
        first, then = 2 * i + 4, 2 * i + 5
        events = [table(i, [pair[n] for pair in pairs]) for n in (0, 1)]
        earlier = [rank_of(t) for t in events]
        seen = jnp.logical_or(earlier[0] < rank, earlier[1] < rank)

        @pl.when(first < total_events)
        def _():
            forward(first)

        arrived(events[0], earlier[0])
        arrived(events[1], earlier[1])

        @pl.when(seen)
        def _():
            expand(earlier)
            attend_heads((0, 1), False)


        @pl.when(then < total_events)
        def _():
            forward(then)


        @pl.when(seen)
        def _():
            attend_heads((2, 3), False)

        return carry

    def visit_last(i, carry):
        events = [table(i, [pair[n] for pair in pairs]) for n in (0, 1)]
        earlier = [rank_of(t) for t in events]
        arrived(events[0], earlier[0])
        arrived(events[1], earlier[1])

        @pl.when(jnp.logical_or(earlier[0] < rank, earlier[1] < rank))
        def _():
            expand(earlier)
            attend_heads((0, 1, 2, 3), False)

        return carry

    all_sent = (total_events - 4) // 2
    lax.fori_loop(1, all_sent, visit, 0)
    lax.fori_loop(all_sent, total_events // 2, visit_last, 0)

    acc_copy = remote(
        acc.at[:, pl.ds(other_half, half), :], acc_in, sem_one_s.at[2], sem_one_r.at[2], sp, partner
    )
    acc_copy.start()
    packed = jnp.zeros((rows, 128), F32)
    for h in range(4):
        packed = jnp.where(lane == h, most_at[h], packed)
        packed = jnp.where(lane == 8 + h, jnp.sum(sum_at[h], axis=1, keepdims=True), packed)
    stat[...] = packed
    stat_copy = remote(stat, stat_in, sem_one_s.at[3], sem_one_r.at[3], sp, partner)
    stat_copy.start()
    for i in (7, 8):
        local[i].wait()
        given[i].wait_recv()
    stat_copy.wait_recv()
    acc_copy.wait_recv()
    own_rows = pl.ds(own_half, half)
    mine_now, other_now = stat[...], stat_in[...]
    most = jnp.maximum(mine_now, other_now)
    sum_at[0] = jnp.exp2(mine_now - most)
    sum_at[1] = jnp.exp2(other_now - most)
    sums = pltpu.roll(mine_now, 120, 1) * sum_at[0] + pltpu.roll(other_now, 120, 1) * sum_at[1]
    sums = jnp.where(lane < 4, sums, 1.0)
    logs = jnp.where(lane < 4, most, 0.0) * math.log(2.0) + jnp.log(sums)
    logs = logs.T
    logt[...] = jnp.where(c == 0, logs[0:2, :], logs[2:4, :])
    most_at[0] = 1.0 / sums
    mixed = [pool_out[...]]
    for h in range(4):
        share = most_at[0, own_rows, h : h + 1]
        own_share = sum_at[0, own_rows, h : h + 1] * share
        other_share = sum_at[1, own_rows, h : h + 1] * share
        mixed.append((acc[h, own_rows, :] * own_share + acc_in[h] * other_share).astype(BF16))
    mixed = jnp.concatenate(mixed, axis=1)

    columns = wo.shape[1]
    chunks = sem_rs_s.shape[1]
    chunk = columns // chunks
    mine = x // 2 == c

    def part_copy(i, n):
        at = pl.ds(n * chunk, chunk)
        return remote(
            part.at[pl.ds(quarter * i, quarter), at],
            rs.at[x, :, at],
            sem_rs_s.at[i, n],
            sem_rs_r.at[x, n],
            sp,
            4 * c + i,
        )

    own_at = pl.multiple_of(quarter * lax.rem(tp, 4), quarter)

    def part_keep(n):
        at = pl.ds(n * chunk, chunk)
        return pltpu.make_async_copy(
            part.at[pl.ds(own_at, quarter), at], rs.at[x, :, at], sem_local.at[19 + n]
        )

    for n in range(chunks):
        at = slice(n * chunk, (n + 1) * chunk)
        part[:, at] = dot(mixed, wo[:, at]).astype(BF16)
        for i in range(4):

            @pl.when(4 * c + i != tp)
            def _():
                part_copy(i, n).start()

        @pl.when(mine)
        def _():
            part_keep(n).start()

    for n in range(chunks):
        at = slice(n * chunk, (n + 1) * chunk)
        for chip in range(CHIPS):

            @pl.when(jnp.logical_and(mine, x == chip))
            def _():
                part_keep(n).wait()

            @pl.when(jnp.logical_not(jnp.logical_and(mine, x == chip)))
            def _():
                ref = rs.at[chip, :, pl.ds(n * chunk, chunk)]
                remote(ref, ref, sem_rs_s.at[0, n], sem_rs_r.at[chip, n], sp, partner).wait_recv()

    for cp in token_copies + given + q_copies:
        cp.wait_send()
    for relay in relayed:
        relay.wait_send()
    to_left.wait_send()
    to_right.wait_send()
    to_across.wait_send()
    for cp in (qn_copy, acc_copy, stat_copy):
        cp.wait_send()

    @pl.when(halo_goes)
    def _():
        halo_copy.wait_send()


    for which in (0, 1):
        block_copy(y_event, which, 0, beside).wait_send()
    for t in range(total_events):
        held = rank_of(t) // 2
        for which in (0, 1):
            for going, to in ((0, above), (1, below)):
                entry = follow[going, which][t]
                if entry:

                    @pl.when(goes(t, going, which, held))
                    def _():
                        block_copy(entry, which, 0, to).wait_send()

    for t in range(1, total_events):

        @pl.when(rank_of(t) < rank)
        def _():
            x_copy(t, 0, 0).wait_send()
            x_copy(t, 0, 1).wait_send()

    for n in range(chunks):
        for i in range(4):

            @pl.when(4 * c + i != tp)
            def _():
                part_copy(i, n).wait_send()


def rotary_tables(rows, ranks):
    frequency = rope_base ** (-np.arange(ROPE // 2, dtype=np.float64) * 2.0 / ROPE)
    frequency = np.tile(frequency, 128 // (ROPE // 2))
    by_row = np.arange(rows)[:, None] * frequency[None, :]
    by_rank = (np.arange(ranks) * rows)[:, None] * frequency[None, :]
    return (
        np.stack([np.cos(by_row), np.sin(by_row)]).astype(np.float32),
        np.stack([np.cos(by_rank), np.sin(by_rank)]).astype(np.float32),
    )


def per_device(
    sp_size,
    tokens,
    mix_gain,
    w_pool_in,
    w_qlat,
    w_kvlat,
    w_krope,
    q_gain,
    kv_gain,
    w_q_content,
    w_q_rotary,
    w_key,
    w_value,
    pool_mix,
    pool_scale,
    w_out_pool,
    w_out_attn,
):
    rows, width = tokens.shape
    half = rows // 2
    columns = w_out_attn.shape[1]
    features = width * PEERS
    base_tab, rank_tab = rotary_tables(rows, SPAN)
    total_events = len(event_list(SPAN // 2)[0])
    chunks = 2
    anywhere = pl.BlockSpec(memory_space=pl.ANY)
    near = pl.BlockSpec(memory_space=pltpu.VMEM)
    dma = lambda *shape: pltpu.SemaphoreType.DMA(shape)
    vmem = pltpu.VMEM
    out, logt = pl.pallas_call(
        functools.partial(kernel, sp_size),
        out_shape=(
            pltpu.VMEM((CHIPS, rows // PEERS, columns), BF16),
            pltpu.VMEM((2, rows), F32),
        ),
        in_specs=[anywhere] * 18,
        out_specs=(anywhere, near),
        scratch_shapes=[
            vmem((1, features), F32),
            vmem((1, 512), F32),
            vmem((1, 512), F32),
            vmem((1, 1024), F32),
            vmem((2, SPAN, 128), F32),
            vmem((PEERS, half, width), BF16),
            vmem((2, features, 128), BF16),
            vmem((384, features), BF16),
            vmem((2, 512, 256), BF16),
            vmem((2, 512, 128), BF16),
            vmem((2, 512, 256), BF16),
            vmem((2, 512, 256), BF16),
            vmem((2, 128, 128), BF16),
            vmem((768, columns), BF16),
            vmem((2, rows, 128), F32),
            vmem((half, 640), F32),
            vmem((half, 256), BF16),
            vmem((16, 256), BF16),
            vmem((half, 256), BF16),
            vmem((SPAN, 2 * half + half // 2, 128), BF16),
            vmem((SPAN, 2, half, 128), BF16),
            vmem((CHIPS, half, 128), BF16),
            vmem((rows, 512), BF16),
            vmem((4, rows, 256), BF16),
            vmem((512, 512), BF16),
            vmem((512, 512), BF16),
            vmem((1, 512), F32),
            vmem((rows, 512), BF16),
            vmem((rows, 512), BF16),
            vmem((rows, 128), BF16),
            vmem((4, rows, 128), F32),
            vmem((rows, 128), F32),
            vmem((rows, 128), F32),
            vmem((4, rows, 128), F32),
            vmem((4, rows, 128), F32),
            vmem((4, half, 128), F32),
            vmem((half, columns), BF16),
            dma(19 + chunks),
            dma(9),
            dma(9),
            dma(4, 2),
            dma(PEERS, 2),
            dma(total_events, 2),
            dma(total_events, 2),
            dma(total_events, 2),
            dma(total_events, 2),
            dma(3),
            dma(3),
            dma(5),
            dma(5),
            dma(4, chunks),
            dma(CHIPS, chunks),
            dma(4),
            pltpu.SemaphoreType.REGULAR((3,)),
        ],
        compiler_params=pltpu.CompilerParams(
            collective_id=0, has_side_effects=True, vmem_limit_bytes=56 * 1024 * 1024
        ),
    )(
        tokens,
        mix_gain.reshape(1, -1),
        w_pool_in,
        w_qlat.T,
        w_kvlat.T,
        w_krope.T,
        q_gain.reshape(1, -1),
        kv_gain.reshape(1, -1),
        w_q_content,
        w_q_rotary,
        w_key,
        w_value,
        pool_mix,
        pool_scale.reshape(1, -1),
        w_out_pool,
        w_out_attn,
        jnp.asarray(base_tab),
        jnp.asarray(rank_tab),
    )
    wide = [out[i].astype(F32) for i in range(CHIPS)]
    return (wide[0] + wide[1] + wide[2] + wide[3]).astype(BF16), logt.T


def solution(mesh):
    in_specs = (
        P("sp", "tp"),
        P(),
        P(None, "tp"),
        P(None, "tp"),
        P(None, "tp"),
        P(),
        P(),
        P(),
        P(None, "tp"),
        P(None, "tp"),
        P(None, "tp"),
        P(None, "tp"),
        P(),
        P(),
        P("tp", None),
        P("tp", None),
    )
    out_specs = (P(("sp", "tp"), None), P("sp", "tp"))
    return jax.shard_map(
        functools.partial(per_device, mesh.shape["sp"]),
        mesh=mesh,
        in_specs=in_specs,
        out_specs=out_specs,
        check_vma=False,
    )
```

```python
import functools
import math

import jax
import jax.numpy as jnp
import numpy as np
from jax import lax
from jax.experimental import pallas as pl
from jax.experimental.pallas import tpu as pltpu
from jax.sharding import PartitionSpec as P

NOPE = 128
ROPE = 64
VDIM = 128
GROUP_DIM = 128
SPAN = 16
CHIPS = 4
PEERS = 8

eps_norm = 1e-06
rope_base = 10000.0
masked_score = -1e30

MESH = pl.DeviceIdType.MESH
F32 = jnp.float32
BF16 = jnp.bfloat16
NT = (((1,), (1,)), ((), ()))


def event_list(ring):
    far = ring // 2
    timed = []
    for column in (0, 1):
        first, pace = (0.0, 4.5) if column == 0 else (10.0, 4.7)
        timed.append((first, (column, 0, 0)))
        for k in range(1, far):
            timed.append((first + pace * k, (column, 0, k)))
            late = 5.0 if column == 1 and k == far - 1 else 0.1
            timed.append((first + pace * k + late, (column, 1, k)))
        timed.append((first + pace * far, (column, 2, far)))
    order = [e for _, e in sorted(timed)]
    at = {e: i for i, e in enumerate(order)}
    follow = {}
    for going in (0, 1):
        for which in (0, 1):
            entries = []
            for column, direction, k in order:
                entry = 0
                if k == 0 or direction == going:
                    if k + 1 < far:
                        entry = at[(column, going, k + 1)]
                    elif going == 0 or which == 1:
                        entry = at[(column, 2, far)]
                entries.append(entry)
            follow[going, which] = entries
    shift = [k if direction == 1 else -k for _, direction, k in order]
    limit = ([], [])
    for which in (0, 1):
        for column, direction, k in order:
            bound = (ring - k, far - 1 + which, far)[direction]
            limit[which].append(bound)
    next_limit, next_least = {}, {}
    for (going, which), entries in follow.items():
        to_far = [e > 0 and order[e][1] == 2 and which == 1 for e in entries]
        next_limit[going, which] = [
            (far - 1 if f and going == 0 else limit[which][e]) if e else 0
            for e, f in zip(entries, to_far)
        ]
        next_least[going, which] = [far - 1 if f and going == 1 else 0 for f in to_far]
    when = {e: t for t, e in timed}
    pairs = []
    for above in (False, True):
        group = [e for e in order if (e[1] == 1) == above]
        pairs += list(zip(group[::2], group[1::2]))
    pairs.sort(key=lambda pair: when[pair[1]])
    pairs = [[at[e] for e in pair] for pair in pairs]
    return order, follow, shift, at[(1, 0, 0)], limit, next_limit, next_least, pairs


def table(index, entries):
    if isinstance(index, int):
        return jnp.int32(entries[index])
    out = jnp.int32(entries[0])
    for i, entry in enumerate(entries):
        if i > 0 and entry != entries[0]:
            out = jnp.where(index == i, jnp.int32(entry), out)
    return out


def remote(src, dst, send, recv, sp, tp):
    return pltpu.make_async_remote_copy(
        src_ref=src,
        dst_ref=dst,
        send_sem=send,
        recv_sem=recv,
        device_id={"sp": sp, "tp": tp},
        device_id_type=MESH,
    )


def dot(a, b, dims=(((1,), (0,)), ((), ()))):
    return lax.dot_general(a, b, dims, preferred_element_type=F32)


def kernel(
    sp_size,
    tokens,
    mix_gain_in,
    w_pool_in,
    w_qlat,
    w_kvlat,
    w_krope,
    q_gain_in,
    kv_gain_in,
    w_qc,
    w_qr,
    w_key,
    w_value,
    pool_mix,
    pool_scale_in,
    w_out_pool,
    w_out_attn,
    base_tab,
    rank_tab_in,
    rs,
    logt,
    mix_gain,
    q_gain,
    kv_gain,
    pool_scale,
    rank_tab,
    tok,
    wp,
    wl,
    wqc,
    wqr,
    wk,
    wv,
    mix,
    wo,
    tab,
    proj,
    pool_own,
    halo,
    pool_out,
    kvz,
    kvx,
    qbuf,
    qn,
    qs,
    wk2,
    wv2,
    gk,
    content_at,
    values_at,
    rotary_at,
    acc,
    stat,
    stat_in,
    most_at,
    sum_at,
    acc_in,
    part,
    sem_local,
    sem_ws,
    sem_wr,
    sem_ts,
    sem_tr,
    sem_zs,
    sem_zr,
    sem_xs,
    sem_xr,
    sem_qs,
    sem_qr,
    sem_one_s,
    sem_one_r,
    sem_rs_s,
    sem_rs_r,
    sem_relay_s,
    sem_ready,
):
    sp = lax.axis_index("sp")
    tp = lax.axis_index("tp")
    count = sp_size // SPAN
    ring = SPAN // 2
    x, c = tp // 2, tp % 2
    rank = sp // count
    z, yh = rank // 2, rank % 2
    order, follow, shift, y_event, limit, next_limit, next_least, pairs = event_list(ring)

    def goes(t, going, which, place):
        least = table(t, next_least[going, which])
        return jnp.logical_and(place >= least, place < table(t, next_limit[going, which]))

    total_events = len(order)
    rows = tokens.shape[0]
    half = rows // 2
    width = tokens.shape[1]
    quarter = half // 4
    own_half = pl.multiple_of(half * c, half)
    other_half = pl.multiple_of(half * (1 - c), half)

    def tp_of(chip, core):
        return lax.rem(chip + CHIPS, CHIPS) * 2 + core

    partner = tp_of(x, 1 - c)
    right, left, across = tp_of(x + 1, c), tp_of(x - 1, c), tp_of(x + 2, c)
    ring_step = 2 * count
    above = lax.rem(sp + ring_step, sp_size)
    below = lax.rem(sp + sp_size - ring_step, sp_size)
    beside = sp + count * (1 - 2 * yh)
    halo_sp = lax.rem(sp + count * c, sp_size)

    core64 = pl.multiple_of(64 * c, 64)
    wl_q, wl_kv = core64, pl.multiple_of(128 + 64 * c, 64)
    wo_pool = pl.multiple_of(128 * c, 128)
    wo_attn = pl.multiple_of(256 + 256 * c, 256)
    shared = [
        (w_pool_in, lambda: wp.at[c]),
        (w_qlat, lambda: wl.at[pl.ds(wl_q, 64)]),
        (w_kvlat, lambda: wl.at[pl.ds(wl_kv, 64)]),
        (w_key, lambda: wk.at[c]),
        (w_value, lambda: wv.at[c]),
        (w_qc, lambda: wqc.at[c]),
        (w_qr, lambda: wqr.at[c]),
        (w_out_pool, lambda: wo.at[pl.ds(wo_pool, 128)]),
        (w_out_attn, lambda: wo.at[pl.ds(wo_attn, 256)]),
    ]
    n_shared = len(shared)
    local = [(src, dst()) for src, dst in shared]
    local += [
        (tokens.at[pl.ds(own_half, half)], tok.at[tp]),
        (w_krope, wl.at[pl.ds(256, 64)]),
        (w_krope, wl.at[pl.ds(320, 64)]),
        (base_tab, tab),
        (pool_mix.at[pl.ds(2 * x, 2)], mix),
        (mix_gain_in, mix_gain),
        (q_gain_in, q_gain),
        (kv_gain_in, kv_gain),
        (pool_scale_in, pool_scale),
        (rank_tab_in, rank_tab),
    ]
    local = [pltpu.make_async_copy(s, d, sem_local.at[i]) for i, (s, d) in enumerate(local)]
    given = [
        remote(s, d(), sem_ws.at[i], sem_wr.at[i], sp, partner) for i, (s, d) in enumerate(shared)
    ]
    for i in [9, 14, 18, 12, 10, 11, 0, 1, 2, 15, 16, 17, 3, 4, 5, 6, 13, 7, 8]:
        local[i].start()

    barrier = pltpu.get_barrier_semaphore()
    for i in range(1, PEERS):
        pl.semaphore_signal(
            barrier, inc=1, device_id={"sp": sp, "tp": lax.rem(tp + i, PEERS)}, device_id_type=MESH
        )
    def greet(other_sp, other_tp):
        pl.semaphore_signal(
            barrier, inc=1, device_id={"sp": other_sp, "tp": other_tp}, device_id_type=MESH
        )

    def answer(which, other_sp, other_tp):
        pl.semaphore_signal(
            sem_ready.at[which],
            inc=1,
            device_id={"sp": other_sp, "tp": other_tp},
            device_id_type=MESH,
        )

    last_place = z == ring - 1
    sends_halo = jnp.logical_and(c == 1, rank < SPAN - 1)
    takes_halo = jnp.logical_and(c == 0, rank > 0)
    @pl.when(yh == 0)
    def _():
        greet(beside, tp)

    @pl.when(jnp.logical_not(last_place))
    def _():
        greet(above, tp)

    @pl.when(z == 0)
    def _():
        greet(below, tp)

    before_sp = lax.rem(sp + sp_size - count, sp_size)

    @pl.when(jnp.logical_and(c == 1, yh == 0))
    def _():
        greet(halo_sp, partner)

    @pl.when(jnp.logical_and(takes_halo, yh == 0))
    def _():
        greet(before_sp, partner)

    greeters = PEERS - 1 + yh + jnp.where(z > 0, 1, 0) + jnp.where(last_place, 1, 0)
    of_halo = jnp.logical_and(yh == 1, jnp.logical_or(takes_halo, sends_halo))
    pl.semaphore_wait(barrier, greeters + jnp.where(of_halo, 1, 0))

    @pl.when(yh == 1)
    def _():
        answer(3, beside, tp)

    @pl.when(z > 0)
    def _():
        answer(0, below, tp)

    @pl.when(last_place)
    def _():
        answer(1, above, tp)

    @pl.when(jnp.logical_and(takes_halo, yh == 1))
    def _():
        answer(2, before_sp, partner)

    def token_copy(i, part):
        chip, core = x + (1, 1, 3, 3)[i], i % 2
        at = pl.ds(part * (half // 2), half // 2)
        return remote(
            tokens.at[pl.ds(half * core + part * (half // 2), half // 2)],
            tok.at[tp, at],
            sem_ts.at[i, part],
            sem_tr.at[tp, part],
            sp,
            tp_of(chip, core),
        )

    def token_wait(source, part):
        piece = tok.at[source, pl.ds(part * (half // 2), half // 2)]
        remote(piece, piece, sem_ts.at[0, 0], sem_tr.at[source, part], sp, partner).wait_recv()

    def token_relay(source, part, index, to):
        piece = tok.at[source, pl.ds(part * (half // 2), half // 2)]
        return remote(piece, piece, sem_relay_s.at[index], sem_tr.at[source, part], sp, to)

    token_copies = [token_copy(i, part) for part in (0, 1) for i in (0, 1)]
    token_copies += [token_copy(i, part) for part in (1, 0) for i in (2, 3)]
    token_copies = [token_copies[i] for i in (0, 4, 1, 5, 2, 6, 3, 7)]
    token_copies.append(
        remote(
            tokens.at[pl.ds(other_half, half)], tok.at[tp], sem_one_s.at[4], sem_one_r.at[4], sp, partner
        )
    )
    for cp in token_copies:
        cp.start()
    for g in given:
        g.start()

    local[12].wait()
    local[18].wait()
    lane = lax.broadcasted_iota(jnp.int32, (1, 128), 1)
    low_part = (lane % 64) < 32
    sign = jnp.where(low_part, -1.0, 1.0).astype(F32)
    cos_rank = rank_tab[0, pl.ds(rank, 1), :]
    sin_rank = rank_tab[1, pl.ds(rank, 1), :]
    cos_row, sin_row = tab[0], tab[1]
    tab[0] = cos_row * cos_rank - sin_row * sin_rank
    tab[1] = (sin_row * cos_rank + cos_row * sin_rank) * sign

    def rotate(v, cosine, signed_sine):
        swapped = jnp.where(low_part, pltpu.roll(v, 96, 1), pltpu.roll(v, 32, 1))
        return v * cosine + swapped * signed_sine

    relayed = []
    for i, core in ((0, c), (1, 1 - c)):
        for chip, piece, onward in ((1, 1, left), (3, 0, right)):
            source = tp_of(x + chip, core)
            token_wait(source, piece)
            relay = token_relay(source, piece, len(relayed), onward)
            relay.start()
            relayed.append(relay)
    for i in (0, 1, 2, 9, 10, 11, 14, 15, 16, 17):
        local[i].wait()
    for i in (0, 1, 2):
        given[i].wait_recv()

    def slab(j, squares):
        hop = j // 2
        chip = x + jnp.where(hop == 2, 3, jnp.where(hop == 3, 2, hop))
        source = tp_of(chip, (c + j) % 2)

        @pl.when(j == 1)
        def _():
            remote(tok.at[source], tok.at[source], sem_one_s.at[4], sem_one_r.at[4], sp, partner).wait_recv()

        @pl.when(jnp.logical_or(jnp.logical_and(j >= 2, j < 4), j >= 6))
        def _():
            token_wait(source, 0)

        @pl.when(j >= 4)
        def _():
            token_wait(source, 1)

        at = pl.ds(pl.multiple_of(source * width, width), width)
        raw = tok[source].astype(F32)
        scaled = (raw * mix_gain[:, at]).astype(BF16)
        raw = raw * raw
        new = jnp.concatenate(
            [dot(scaled, wp[0, at, :]), dot(scaled, wp[1, at, :]), dot(scaled, wl[:, at], NT)],
            axis=1,
        )

        @pl.when(j == 0)
        def _():
            proj[...] = new

        @pl.when(j > 0)
        def _():
            proj[...] += new

        return squares + raw[:, :128] + raw[:, 128:]

    squares = lax.fori_loop(0, PEERS, slab, jnp.zeros((half, 128), F32))
    inverse = lax.rsqrt(jnp.sum(squares, axis=1, keepdims=True) / (width * PEERS) + eps_norm)
    done = (proj[...] * inverse).astype(BF16)
    own = kvz.at[rank]
    own[:half, :] = done[:, 384:512]
    qbuf[x] = done[:, 256:384]
    pool_own[...] = done[:, :256]
    rope = done[:, 512:640].astype(F32)
    rope = rotate(rope, tab[0, pl.ds(own_half, half), :], tab[1, pl.ds(own_half, half), :])
    rope = jnp.where(lane < 64, rope[: half // 2], rope[half // 2 :])
    own[half : half + half // 2, :] = rope.astype(BF16)

    first_part = pl.ds(0, half + half // 2)
    second = pl.ds(half + half // 2, half)

    def block_copy(event, which, block, to):
        piece = kvz.at[block, first_part if which == 0 else second]
        return remote(piece, piece, sem_zs.at[event, which], sem_zr.at[event, which], to, tp)

    def start_own(which):
        for going, to in ((0, above), (1, below)):
            if follow[going, which][0]:

                @pl.when(goes(0, going, which, z))
                def _():
                    block_copy(follow[going, which][0], which, rank, to).start()

        block_copy(y_event, which, rank, beside).start()

    first = own.at[pl.ds(0, half)]
    to_left = remote(first, own.at[second], sem_zs.at[0, 1], sem_zr.at[0, 1], sp, left)
    to_right = remote(first, kvx.at[rank, 1], sem_xs.at[0, 1], sem_xr.at[0, 1], sp, right)
    to_across = remote(first, kvx.at[rank, 0], sem_xs.at[0, 0], sem_xr.at[0, 0], sp, across)
    q_copies = [
        remote(qbuf.at[x], qbuf.at[x], sem_qs.at[i], sem_qr.at[i], sp, who)
        for i, who in enumerate((left, right, across))
    ]
    q_from = [lax.rem(x + 1, CHIPS), lax.rem(x + 3, CHIPS), lax.rem(x + 2, CHIPS)]
    to_left.start()

    @pl.when(jnp.logical_not(last_place))
    def _():
        pl.semaphore_wait(sem_ready.at[0], 1)

    @pl.when(z == 0)
    def _():
        pl.semaphore_wait(sem_ready.at[1], 1)

    @pl.when(yh == 0)
    def _():
        pl.semaphore_wait(sem_ready.at[3], 1)

    start_own(0)
    for q_copy in q_copies:
        q_copy.start()
    to_right.start()
    to_across.start()
    halo_copy = remote(
        pool_own.at[pl.ds(half - 16, 16)],
        halo,
        sem_one_s.at[0],
        sem_one_r.at[0],
        halo_sp,
        partner,
    )

    @pl.when(jnp.logical_and(c == 1, yh == 0))
    def _():
        pl.semaphore_wait(sem_ready.at[2], 1)

    halo_goes = jnp.logical_or(c == 0, sends_halo)
    halo_comes = jnp.logical_or(c == 1, takes_halo)

    @pl.when(halo_goes)
    def _():
        halo_copy.start()


    for i in (3, 4, 5, 6):
        local[i].wait()
        given[i].wait_recv()
    for r in range(CHIPS):
        at = pl.ds(pl.multiple_of(lax.rem(x + r, CHIPS) * 128, 128), 128)
        gk[:, 128 * r : 128 * r + 128] = kv_gain[:, at]
        for core in (0, 1):
            wk2[128 * r : 128 * r + 128, 256 * core : 256 * core + 256] = wk[core, at, :]
            wv2[128 * r : 128 * r + 128, 256 * core : 256 * core + 256] = wv[core, at, :]

    def rank_of(t):
        column = table(t, [e[0] for e in order])
        moved = table(t, shift)
        return lax.rem(z + moved + ring, ring) * 2 + lax.rem(yh + column, 2)

    def x_copy(t, block, which):
        piece = kvz.at[block, second if which == 0 else pl.ds(0, half)]
        return remote(
            piece,
            kvx.at[block, which],
            sem_xs.at[t, which],
            sem_xr.at[t, which],
            sp,
            left if which == 0 else right,
        )

    def forward(t, parts=(0, 1)):
        block = rank_of(t)
        place = block // 2
        for which in parts:

            @pl.when(place < table(t, limit[which]))
            def _():
                block_copy(t, which, block, above).wait_recv()

            for going, to in ((0, above), (1, below)):

                @pl.when(goes(t, going, which, place))
                def _():
                    entry = table(t, follow[going, which])
                    block_copy(entry, which, block, to).start()

            @pl.when(block < rank)
            def _():
                x_copy(t, block, 1 - which).start()


    def arrived(t, block):
        @pl.when(block <= rank)
        def _():
            x_copy(t, block, 0).wait_recv()
            x_copy(t, block, 1).wait_recv()

    to_left.wait_recv()
    start_own(1)

    forward(jnp.int32(1), (0,))
    forward(jnp.int32(2), (0,))
    for i, piece in enumerate(q_from):
        remote(
            qbuf.at[piece], qbuf.at[piece], sem_qs.at[i], sem_qr.at[i], sp, left
        ).wait_recv()
    latent = [qbuf[i].astype(F32) for i in range(CHIPS)]
    squares = latent[0] * latent[0]
    for i in range(1, CHIPS):
        squares = squares + latent[i] * latent[i]
    inverse = lax.rsqrt(jnp.sum(squares, axis=1, keepdims=True) / (128 * CHIPS) + eps_norm)
    for i in range(CHIPS):
        gain = q_gain[:, 128 * i : 128 * i + 128]
        qn[pl.ds(own_half, half), 128 * i : 128 * i + 128] = (latent[i] * inverse * gain).astype(BF16)
    qn_copy = remote(
        qn.at[pl.ds(own_half, half)],
        qn.at[pl.ds(own_half, half)],
        sem_one_s.at[1],
        sem_one_r.at[1],
        sp,
        partner,
    )
    qn_copy.start()
    forward(jnp.int32(1), (1,))
    forward(jnp.int32(2), (1,))
    qn_other = qn.at[pl.ds(other_half, half)]
    remote(qn_other, qn_other, sem_one_s.at[1], sem_one_r.at[1], sp, partner).wait_recv()
    normed = qn[...]
    to_log2 = (NOPE + ROPE) ** (-0.5) * math.log2(math.e)
    for core in (0, 1):
        content = (dot(normed, wqc[core]) * to_log2).astype(BF16)
        rotary = rotate(dot(normed, wqr[core]), tab[0], tab[1]) * to_log2
        for h in (0, 1):
            qs[2 * core + h, :, :128] = content[:, 128 * h : 128 * h + 128]
            turned = rotary if h == 0 else pltpu.roll(rotary, 64, 1)
            spare = jnp.where(lane == 64, 1.0, 0.0)
            qs[2 * core + h, :, 128:] = jnp.where(lane < 64, turned, spare).astype(BF16)

    most_at[...] = jnp.full(most_at.shape, masked_score, F32)
    sum_at[...] = jnp.zeros_like(sum_at)
    acc[...] = jnp.zeros_like(acc)

    def expand(blocks):
        parts = (pl.ds(0, half), second)
        def shown(b, value):
            return jnp.where(b <= rank, value.astype(F32), 0.0)

        piece = [
            jnp.concatenate([shown(b, kvz[b, at, :]) for b in blocks], axis=0) for at in parts
        ]
        piece += [jnp.concatenate([shown(b, kvx[b, i]) for b in blocks], axis=0) for i in (0, 1)]
        squares = piece[0] * piece[0]
        for i in range(1, CHIPS):
            squares = squares + piece[i] * piece[i]
        inverse = lax.rsqrt(jnp.sum(squares, axis=1, keepdims=True) / (128 * CHIPS) + eps_norm)
        normed = jnp.concatenate(
            [
                (piece[i] * inverse * gk[:, 128 * i : 128 * i + 128]).astype(BF16)
                for i in range(CHIPS)
            ],
            axis=1,
        )
        content = dot(normed, wk2[...]).astype(BF16)
        values = dot(normed, wv2[...]).astype(BF16)
        rotary = []
        for b in blocks:
            packed = shown(b, kvz[b, half : half + half // 2, :])
            hidden = jnp.where(b <= rank, 0.0, masked_score).astype(F32)
            spare = jnp.where(lane == 64, hidden, 0.0)
            rotary.append(jnp.where(lane < 64, packed, spare))
            rotary.append(jnp.where(lane < 64, pltpu.roll(packed, 64, 1), spare))
        rotary = jnp.concatenate(rotary, axis=0).astype(BF16)
        content_at[...] = content
        values_at[...] = values
        rotary_at[...] = rotary

    def attend_heads(heads, masked):
        if masked:
            column = lax.broadcasted_iota(jnp.int32, (rows, rows), 1)
            row = lax.broadcasted_iota(jnp.int32, (rows, rows), 0)
            allowed = jnp.logical_or(column >= half, column + half * c <= row)
        for h in heads:
            at = slice(128 * h, 128 * h + 128)
            keys = jnp.concatenate([content_at[:, at], rotary_at[...]], axis=1)
            scores = dot(qs[h], keys, NT)
            if masked:
                scores = jnp.where(allowed, scores, masked_score)
            old = most_at[h]
            new = jnp.maximum(old, jnp.max(scores, axis=1, keepdims=True))
            factor = jnp.exp2(old - new)
            expo = [jnp.exp2(scores[:, i : i + 128] - new) for i in range(0, rows, 128)]
            most_at[h] = new
            sum_at[h] = sum_at[h] * factor + sum(expo[1:], expo[0])
            expo = jnp.concatenate([e.astype(BF16) for e in expo], axis=1)
            acc[h] = acc[h] * factor + dot(expo, values_at[:, at])

    def pooling():
        @pl.when(halo_comes)
        def _():
            remote(halo, halo, sem_one_s.at[0], sem_one_r.at[0], sp, partner).wait_recv()

        local[13].wait()
        before = halo[...].astype(F32)
        before = jnp.where(halo_comes, before, 0.0)
        row = lax.broadcasted_iota(jnp.int32, (half, 128), 0) + (rank * rows + own_half)
        odd = x % 2
        for g in (0, 1):
            at = slice(128 * g, 128 * g + 128)
            values = pool_own[:, at].astype(F32)
            extended = jnp.concatenate([before[:, at], values], axis=0)
            sums = [extended]
            for step in (1, 2, 4, 8):
                sums.append(sums[-1] + pltpu.roll(sums[-1], step, 0))
            window = jnp.where(odd == 1, (8, 16)[g], (2, 4)[g])
            chosen = jnp.where(odd == 1, sums[3 + g][16:], sums[1 + g][16:])
            counts = jnp.minimum(row + 1, window).astype(F32)
            pooled = (chosen / counts - values).astype(BF16)
            scale = pool_scale[:, pl.ds(pl.multiple_of(256 * x + 128 * g, 128), 128)]
            pool_out[:, at] = (dot(pooled, mix[g]) * scale).astype(BF16)

    pooling()
    forward(jnp.int32(3))
    forward(jnp.int32(4))
    arrived(0, rank)
    arrived(1, rank_of(jnp.int32(1)))
    expand([rank, rank_of(jnp.int32(1))])
    attend_heads((0, 1), True)
    forward(jnp.int32(5))
    attend_heads((2, 3), True)

    def visit(i, carry):
        first, then = 2 * i + 4, 2 * i + 5
        events = [table(i, [pair[n] for pair in pairs]) for n in (0, 1)]
        earlier = [rank_of(t) for t in events]
        seen = jnp.logical_or(earlier[0] < rank, earlier[1] < rank)

        @pl.when(first < total_events)
        def _():
            forward(first)

        arrived(events[0], earlier[0])
        arrived(events[1], earlier[1])

        @pl.when(seen)
        def _():
            expand(earlier)
            attend_heads((0, 1), False)


        @pl.when(then < total_events)
        def _():
            forward(then)


        @pl.when(seen)
        def _():
            attend_heads((2, 3), False)

        return carry

    def visit_last(i, carry):
        events = [table(i, [pair[n] for pair in pairs]) for n in (0, 1)]
        earlier = [rank_of(t) for t in events]
        arrived(events[0], earlier[0])
        arrived(events[1], earlier[1])

        @pl.when(jnp.logical_or(earlier[0] < rank, earlier[1] < rank))
        def _():
            expand(earlier)
            attend_heads((0, 1, 2, 3), False)

        return carry

    all_sent = (total_events - 4) // 2
    lax.fori_loop(1, all_sent, visit, 0)
    lax.fori_loop(all_sent, total_events // 2, visit_last, 0)

    acc_copy = remote(
        acc.at[:, pl.ds(other_half, half), :], acc_in, sem_one_s.at[2], sem_one_r.at[2], sp, partner
    )
    acc_copy.start()
    packed = jnp.zeros((rows, 128), F32)
    for h in range(4):
        packed = jnp.where(lane == h, most_at[h], packed)
        packed = jnp.where(lane == 8 + h, jnp.sum(sum_at[h], axis=1, keepdims=True), packed)
    stat[...] = packed
    stat_copy = remote(stat, stat_in, sem_one_s.at[3], sem_one_r.at[3], sp, partner)
    stat_copy.start()
    for i in (7, 8):
        local[i].wait()
        given[i].wait_recv()
    stat_copy.wait_recv()
    acc_copy.wait_recv()
    own_rows = pl.ds(own_half, half)
    mine_now, other_now = stat[...], stat_in[...]
    most = jnp.maximum(mine_now, other_now)
    sum_at[0] = jnp.exp2(mine_now - most)
    sum_at[1] = jnp.exp2(other_now - most)
    sums = pltpu.roll(mine_now, 120, 1) * sum_at[0] + pltpu.roll(other_now, 120, 1) * sum_at[1]
    sums = jnp.where(lane < 4, sums, 1.0)
    logs = jnp.where(lane < 4, most, 0.0) * math.log(2.0) + jnp.log(sums)
    logs = logs.T
    logt[...] = jnp.where(c == 0, logs[0:2, :], logs[2:4, :])
    most_at[0] = 1.0 / sums
    mixed = [pool_out[...]]
    for h in range(4):
        share = most_at[0, own_rows, h : h + 1]
        own_share = sum_at[0, own_rows, h : h + 1] * share
        other_share = sum_at[1, own_rows, h : h + 1] * share
        mixed.append((acc[h, own_rows, :] * own_share + acc_in[h] * other_share).astype(BF16))
    mixed = jnp.concatenate(mixed, axis=1)

    columns = wo.shape[1]
    chunks = sem_rs_s.shape[1]
    chunk = columns // chunks
    mine = x // 2 == c

    def part_copy(i, n):
        at = pl.ds(n * chunk, chunk)
        return remote(
            part.at[pl.ds(quarter * i, quarter), at],
            rs.at[x, :, at],
            sem_rs_s.at[i, n],
            sem_rs_r.at[x, n],
            sp,
            4 * c + i,
        )

    own_at = pl.multiple_of(quarter * lax.rem(tp, 4), quarter)

    def part_keep(n):
        at = pl.ds(n * chunk, chunk)
        return pltpu.make_async_copy(
            part.at[pl.ds(own_at, quarter), at], rs.at[x, :, at], sem_local.at[19 + n]
        )

    for n in range(chunks):
        at = slice(n * chunk, (n + 1) * chunk)
        part[:, at] = dot(mixed, wo[:, at]).astype(BF16)
        for i in range(4):

            @pl.when(4 * c + i != tp)
            def _():
                part_copy(i, n).start()

        @pl.when(mine)
        def _():
            part_keep(n).start()

    for n in range(chunks):
        at = slice(n * chunk, (n + 1) * chunk)
        for chip in range(CHIPS):

            @pl.when(jnp.logical_and(mine, x == chip))
            def _():
                part_keep(n).wait()

            @pl.when(jnp.logical_not(jnp.logical_and(mine, x == chip)))
            def _():
                ref = rs.at[chip, :, pl.ds(n * chunk, chunk)]
                remote(ref, ref, sem_rs_s.at[0, n], sem_rs_r.at[chip, n], sp, partner).wait_recv()

    for cp in token_copies + given + q_copies:
        cp.wait_send()
    for relay in relayed:
        relay.wait_send()
    to_left.wait_send()
    to_right.wait_send()
    to_across.wait_send()
    for cp in (qn_copy, acc_copy, stat_copy):
        cp.wait_send()

    @pl.when(halo_goes)
    def _():
        halo_copy.wait_send()


    for which in (0, 1):
        block_copy(y_event, which, 0, beside).wait_send()
    for t in range(total_events):
        held = rank_of(t) // 2
        for which in (0, 1):
            for going, to in ((0, above), (1, below)):
                entry = follow[going, which][t]
                if entry:

                    @pl.when(goes(t, going, which, held))
                    def _():
                        block_copy(entry, which, 0, to).wait_send()

    for t in range(1, total_events):

        @pl.when(rank_of(t) < rank)
        def _():
            x_copy(t, 0, 0).wait_send()
            x_copy(t, 0, 1).wait_send()

    for n in range(chunks):
        for i in range(4):

            @pl.when(4 * c + i != tp)
            def _():
                part_copy(i, n).wait_send()


def rotary_tables(rows, ranks):
    frequency = rope_base ** (-np.arange(ROPE // 2, dtype=np.float64) * 2.0 / ROPE)
    frequency = np.tile(frequency, 128 // (ROPE // 2))
    by_row = np.arange(rows)[:, None] * frequency[None, :]
    by_rank = (np.arange(ranks) * rows)[:, None] * frequency[None, :]
    return (
        np.stack([np.cos(by_row), np.sin(by_row)]).astype(np.float32),
        np.stack([np.cos(by_rank), np.sin(by_rank)]).astype(np.float32),
    )


def per_device(
    sp_size,
    tokens,
    mix_gain,
    w_pool_in,
    w_qlat,
    w_kvlat,
    w_krope,
    q_gain,
    kv_gain,
    w_q_content,
    w_q_rotary,
    w_key,
    w_value,
    pool_mix,
    pool_scale,
    w_out_pool,
    w_out_attn,
):
    rows, width = tokens.shape
    half = rows // 2
    columns = w_out_attn.shape[1]
    features = width * PEERS
    base_tab, rank_tab = rotary_tables(rows, SPAN)
    total_events = len(event_list(SPAN // 2)[0])
    chunks = 2
    anywhere = pl.BlockSpec(memory_space=pl.ANY)
    near = pl.BlockSpec(memory_space=pltpu.VMEM)
    dma = lambda *shape: pltpu.SemaphoreType.DMA(shape)
    vmem = pltpu.VMEM
    out, logt = pl.pallas_call(
        functools.partial(kernel, sp_size),
        out_shape=(
            pltpu.VMEM((CHIPS, rows // PEERS, columns), BF16),
            pltpu.VMEM((2, rows), F32),
        ),
        in_specs=[anywhere] * 18,
        out_specs=(anywhere, near),
        scratch_shapes=[
            vmem((1, features), F32),
            vmem((1, 512), F32),
            vmem((1, 512), F32),
            vmem((1, 1024), F32),
            vmem((2, SPAN, 128), F32),
            vmem((PEERS, half, width), BF16),
            vmem((2, features, 128), BF16),
            vmem((384, features), BF16),
            vmem((2, 512, 256), BF16),
            vmem((2, 512, 128), BF16),
            vmem((2, 512, 256), BF16),
            vmem((2, 512, 256), BF16),
            vmem((2, 128, 128), BF16),
            vmem((768, columns), BF16),
            vmem((2, rows, 128), F32),
            vmem((half, 640), F32),
            vmem((half, 256), BF16),
            vmem((16, 256), BF16),
            vmem((half, 256), BF16),
            vmem((SPAN, 2 * half + half // 2, 128), BF16),
            vmem((SPAN, 2, half, 128), BF16),
            vmem((CHIPS, half, 128), BF16),
            vmem((rows, 512), BF16),
            vmem((4, rows, 256), BF16),
            vmem((512, 512), BF16),
            vmem((512, 512), BF16),
            vmem((1, 512), F32),
            vmem((rows, 512), BF16),
            vmem((rows, 512), BF16),
            vmem((rows, 128), BF16),
            vmem((4, rows, 128), F32),
            vmem((rows, 128), F32),
            vmem((rows, 128), F32),
            vmem((4, rows, 128), F32),
            vmem((4, rows, 128), F32),
            vmem((4, half, 128), F32),
            vmem((half, columns), BF16),
            dma(19 + chunks),
            dma(9),
            dma(9),
            dma(4, 2),
            dma(PEERS, 2),
            dma(total_events, 2),
            dma(total_events, 2),
            dma(total_events, 2),
            dma(total_events, 2),
            dma(3),
            dma(3),
            dma(5),
            dma(5),
            dma(4, chunks),
            dma(CHIPS, chunks),
            dma(4),
            pltpu.SemaphoreType.REGULAR((4,)),
        ],
        compiler_params=pltpu.CompilerParams(
            collective_id=0, has_side_effects=True, vmem_limit_bytes=56 * 1024 * 1024
        ),
    )(
        tokens,
        mix_gain.reshape(1, -1),
        w_pool_in,
        w_qlat.T,
        w_kvlat.T,
        w_krope.T,
        q_gain.reshape(1, -1),
        kv_gain.reshape(1, -1),
        w_q_content,
        w_q_rotary,
        w_key,
        w_value,
        pool_mix,
        pool_scale.reshape(1, -1),
        w_out_pool,
        w_out_attn,
        jnp.asarray(base_tab),
        jnp.asarray(rank_tab),
    )
    wide = [out[i].astype(F32) for i in range(CHIPS)]
    return (wide[0] + wide[1] + wide[2] + wide[3]).astype(BF16), logt.T


def solution(mesh):
    in_specs = (
        P("sp", "tp"),
        P(),
        P(None, "tp"),
        P(None, "tp"),
        P(None, "tp"),
        P(),
        P(),
        P(),
        P(None, "tp"),
        P(None, "tp"),
        P(None, "tp"),
        P(None, "tp"),
        P(),
        P(),
        P("tp", None),
        P("tp", None),
    )
    out_specs = (P(("sp", "tp"), None), P("sp", "tp"))
    return jax.shard_map(
        functools.partial(per_device, mesh.shape["sp"]),
        mesh=mesh,
        in_specs=in_specs,
        out_specs=out_specs,
        check_vma=False,
    )
```
